32 devices in a mesh: grp: 2 (over y), fs: 4 (over z), tp: 4 (over x, core).
Axes of the slice: x: 2, y: 2, z: 4, core: 2. Of those that a mesh axis runs over, the one named last changes fastest.
Arguments:
- tokens: bfloat16 [4096, 2048], P(('grp', 'fs', 'tp')), parts along dimension 0, may hold values from -6 to 6
- mix_weight_in: bfloat16 [2048, 1024], P('fs', 'tp'), may hold values from -0.125 to 0.125
- pool_scale: float32 [1024], P('tp'), may hold values from 0.1 to 1.9
- mix_weight_out: bfloat16 [1024, 2048], P('tp', 'fs'), may hold values from -0.1875 to 0.1875
- up_weight: bfloat16 [2048, 8192], P('fs', 'tp'), may hold values from -0.125 to 0.125
- down_weight: bfloat16 [8192, 2048], P('tp', 'fs'), may hold values from -0.0625 to 0.0625
- gains: float32 [4, 2048], replicated, may hold values from 0.1 to 1.9
Outputs:
- result: bfloat16 [4096, 2048], P(('grp', 'fs', 'tp')), parts along dimension 0
The draws below stay inside these ranges and needn't reach their ends.
There are 2 independent parts, one for each index of `grp`. The reference program is written for one: setup_inputs(seed, part) draws one part's arguments, and reference() takes and returns one part's arrays. A program takes and returns all parts, laid end to end along the dimension named above; an argument that names none is the same for every part. Nothing has to cross between parts.
All inputs are finite; a program needn't handle non-finite values.
Results may differ from the reference program's by a relative error of at most 0.02.
Values may be sent and summed in bfloat16 or wider, within the bound.
A program may use at most 64 MiB of HBM per device.

```python
import jax
import jax.numpy as jnp
from jax import lax

D = 2048
PW = 1024
GROUPS = 4
FF = 8192
ROWS = 128
TOKENS = 2048
N_FS = 4
N_TP = 4


def level_of(own_key, extent, split, least, top_value):
    factor_of, own = 1.0, jax.random.fold_in(own_key, 6)
    for dim, blocks in split:
        heights = jnp.exp(jax.random.uniform(jax.random.fold_in(own, dim), (blocks,), jnp.float32, least / len(split), top_value / len(split)))
        factor_of = factor_of * jnp.repeat(heights, extent[dim] // blocks).reshape([-1 if axis == dim else 1 for axis in range(len(extent))])
    return factor_of


def scatter_about(key, shape, spread, reach, shards=(), kind=jnp.bfloat16):
    level = level_of(key, shape, shards, -0.22, 0.18) if shards else 1.0
    entries = jax.random.normal(key, shape, jnp.float32) * spread * level
    return jnp.minimum(jnp.maximum(entries, -reach), reach).astype(kind)


def setup_inputs(seed: int = 0, part: int = 0) -> dict:
    keys = jax.random.split(jax.random.key(seed), 8)
    own_keys = jax.random.split(jax.random.fold_in(keys[7], part), 8)
    return {
        "tokens": scatter_about(own_keys[0], (TOKENS, D), 1.0, 6.0, ((0, 16),)),
        "mix_weight_in": scatter_about(keys[1], (D, PW), D ** -0.5, 0.125, ((0, 4), (1, 4))),
        "pool_scale": jnp.clip(1.0 + 0.18 * jax.random.normal(keys[2], (PW,), jnp.float32), 0.1, 1.9),
        "mix_weight_out": scatter_about(keys[3], (PW, D), PW ** -0.5, 0.1875, ((0, 4), (1, 4))),
        "up_weight": scatter_about(keys[4], (D, FF), D ** -0.5, 0.125, ((0, 4), (1, 4))),
        "down_weight": scatter_about(keys[5], (FF, D), FF ** -0.5, 0.0625, ((0, 4), (1, 4))),
        "gains": jnp.clip(1.0 + 0.18 * jax.random.normal(keys[6], (4, D), jnp.float32), 0.1, 1.9),
    }


norm_eps = 1e-06
pool_spans = (2, 4, 8, 16)

def normalize(values, gain):
    upcast = values.astype(jnp.float32)
    return upcast * lax.rsqrt(lax.optimization_barrier(jnp.mean(upcast * upcast, axis=-1, keepdims=True)) + norm_eps) * gain

def pooling(mixed_in):
    length = mixed_in.shape[0]
    upcast = mixed_in.astype(jnp.float32)
    running = jnp.cumsum(upcast, axis=0)
    position = jnp.arange(1, length + 1, dtype=jnp.float32)[:, None]
    group_of = (jnp.arange(PW) // (PW // GROUPS))[None, :]
    average = jnp.zeros_like(upcast)
    for index, span in enumerate(pool_spans):
        lagged = jnp.pad(running, ((span, 0), (0, 0)))[:length]
        window_mean = (running - lagged) / jnp.minimum(position, float(span))
        average = jnp.where(group_of == index, window_mean, average)
    return average - upcast

def split_sum(left, right, width):
    total = jnp.zeros((left.shape[0], right.shape[1]), jnp.float32)
    for block in range(N_TP):
        partial_value = jnp.dot(left[:, block * width:(block + 1) * width], right[block * width:(block + 1) * width], preferred_element_type=jnp.float32)
        total = total + lax.optimization_barrier(partial_value.astype(jnp.bfloat16)).astype(jnp.float32)
    return total.astype(jnp.bfloat16)

def reference(tokens, mix_weight_in, pool_scale, mix_weight_out, up_weight, down_weight, gains):

    def one_sequence(sequence):
        normed = normalize(sequence, gains[0]).astype(jnp.bfloat16)
        mixed_in = jnp.dot(normed, mix_weight_in, preferred_element_type=jnp.float32).astype(jnp.bfloat16)
        scaled = (pooling(mixed_in) * pool_scale).astype(jnp.bfloat16)
        mixer_out = split_sum(scaled, mix_weight_out, PW // N_TP)
        middle = (sequence.astype(jnp.float32) + normalize(mixer_out, gains[1])).astype(jnp.bfloat16)
        normed_two = normalize(middle, gains[2]).astype(jnp.bfloat16)
        hidden_pre = jax.nn.relu(jnp.dot(normed_two, up_weight, preferred_element_type=jnp.float32))
        squared = (hidden_pre * hidden_pre).astype(jnp.bfloat16)
        channel_out = split_sum(squared, down_weight, FF // N_TP)
        return (middle.astype(jnp.float32) + normalize(channel_out, gains[3])).astype(jnp.bfloat16)
    sequences = tokens.reshape(N_FS, ROWS * N_TP, D)
    return lax.map(one_sequence, sequences).reshape(TOKENS, D)
```

```python
import functools

import jax
import jax.numpy as jnp
from jax import lax
from jax.experimental import pallas as pl
from jax.experimental.pallas import tpu as pltpu
from jax.sharding import PartitionSpec as P

GROUPS = 4
EPS = 1e-06
MESH = pl.DeviceIdType.MESH


def normalize(values, gain):
    upcast = values.astype(jnp.float32)
    return upcast * lax.rsqrt(jnp.mean(upcast * upcast, axis=-1, keepdims=True) + EPS) * gain


def pooling(mixed_in, first_channel, group_width):
    length, width = mixed_in.shape
    upcast = mixed_in.astype(jnp.float32)
    row = lax.broadcasted_iota(jnp.int32, (length, width), 0)
    group = (first_channel + lax.broadcasted_iota(jnp.int32, (length, width), 1)) // group_width
    position = (row + 1).astype(jnp.float32)
    total, average = upcast, jnp.zeros_like(upcast)
    for index in range(GROUPS):
        step = 1 << index
        total = total + jnp.where(row >= step, pltpu.roll(total, step, axis=0), 0.0)
        mean = total / jnp.minimum(position, float(2 * step))
        average = jnp.where(group == index, mean, average)
    return average - upcast


def kernel(dims, tok_h, gains_h, scale_h, mi_h, mo_h, up_h, dn_h, out,
           tok, gains, scale, mi, mo, up, dn, g1, g2, hid, sp1, rq1, rp1, sp2, rq2, rp2, mid,
           lsem, zs, zr, ys, yr, gs, g1r, g2r, g3r, es, er,
           w1s, w1r, w2s, w2r, p1s, p1r, p2s, p2r, p3s):
    G, F, T, R, D, K, PWt, Ht, NU, ND = dims
    g, f, t = lax.axis_index("grp"), lax.axis_index("fs"), lax.axis_index("tp")
    cu, cd = Ht // NU, K // ND
    off = F >= 4
    far = F - 2 if off else F - 1
    first, last = (1, F - 2) if off else (0, F - 1)
    mid_plane = (f >= first) & (f <= last)
    end = (f < first) | (f > last)
    helper = (f == 1) | (f == F - 2) if off else f < 0
    helped = jnp.where(f == 1, 0, F - 1)
    inner = jnp.where(f == 0, 1, F - 2)
    sibling = t + 1 - 2 * lax.rem(t, 2)
    place, half_t = lax.rem(t, 2), T // 2
    step = D // 4

    def to_right_ok(w):
        return f + 1 < F if w in ("mi", "mo") else (f + 1 <= last)

    def to_left_ok(w):
        return f > 0 if w in ("mi", "mo") else (f - 1 >= first)

    def shared(w, s):
        return True if w in ("mi", "mo") or not off else ~(helper & (s == helped))
    pieces = {"mi": (0, 1), "mo": (1, 1), "up": (2, NU), "dn": (2 + NU, ND)}
    kinds = {"mi": 0, "mo": 0, "up": 1, "dn": 1}
    bufs = {"mi": (mi_h, mi), "mo": (mo_h, mo), "up": (up_h, up), "dn": (dn_h, dn)}

    def mult(value, by):
        return pl.multiple_of(value, by)

    def span(w, s, c, half):
        base = 0 if s is None else s * K
        if w == "mi":
            return pl.ds(mult(base + half * (K // G), K // G), K // G), pl.ds(0, PWt)
        if w == "mo":
            return pl.ds(mult(half * (PWt // G), PWt // G), PWt // G), pl.ds(mult(base, 128), K)
        if w == "up":
            return pl.ds(mult(base + half * (K // G), K // G), K // G), pl.ds(mult(c * cu, cu), cu)
        return pl.ds(mult(half * (Ht // G), Ht // G), Ht // G), pl.ds(mult(base + c * cd, cd), cd)

    def view(w, s, c, half):
        return bufs[w][1].at[span(w, s, c, half)]

    def z_copy(w, s, c, to_right, own=False):
        p = pieces[w][0] + c
        src = bufs[w][0].at[span(w, None, c, g)] if own else view(w, s, c, g)
        target = f + 1 if to_right else f - 1
        side = 0 if to_right else 1
        return pltpu.make_async_remote_copy(
            src_ref=src, dst_ref=view(w, s, c, g), send_sem=zs.at[side, kinds[w], s], recv_sem=zr.at[s, p],
            device_id=(g, target, t), device_id_type=MESH)

    def y_copy(w, s, c, k, half=None):
        p = pieces[w][0] + c
        half = g if half is None else half
        return pltpu.make_async_remote_copy(
            src_ref=view(w, s, c, half), dst_ref=view(w, s, c, half),
            send_sem=ys.at[k - 1, kinds[w], s], recv_sem=yr.at[k - 1, s, p],
            device_id=(lax.rem(g + k, G), f, t), device_id_type=MESH)

    def send_own(w, c):
        @pl.when(to_right_ok(w))
        def _():
            z_copy(w, f, c, True, own=True).start()

        @pl.when(to_left_ok(w))
        def _():
            z_copy(w, f, c, False, own=True).start()

    def whole_copy(w, c, k):
        p = pieces[w][0] + c
        half = lax.rem(g - k + G, G)
        return pltpu.make_async_remote_copy(
            src_ref=bufs[w][0].at[span(w, None, c, half)], dst_ref=view(w, f, c, half),
            send_sem=ys.at[k - 1, kinds[w], f], recv_sem=yr.at[k - 1, f, p],
            device_id=(g, inner, t), device_id_type=MESH)

    def send_whole(w):
        if off:
            @pl.when(end)
            def _():
                for c in range(pieces[w][1]):
                    for k in range(1, G):
                        whole_copy(w, c, k).start()

    def pump(w, d, c):
        for to_right in (True, False):
            s = f - d if to_right else f + d
            more = to_right_ok(w) if to_right else to_left_ok(w)
            here = (s >= 0) & (s < F)
            if w in ("up", "dn"):
                here = here & mid_plane

            @pl.when(here)
            def _():
                z_copy(w, s, c, to_right).wait_recv()

                @pl.when(more)
                def _():
                    z_copy(w, s, c, to_right).start()

                @pl.when(shared(w, s))
                def _():
                    for k in range(1, G):
                        y_copy(w, s, c, k).start()

    def y_wait(w, s, c):
        for k in range(1, G):
            y_copy(w, s, c, k, lax.rem(g - k + G, G)).wait_recv()

    def y_wait_all(w):
        def body(i, _):
            s, c = i // pieces[w][1], lax.rem(i, pieces[w][1])

            @pl.when(s != f)
            def _():
                y_wait(w, s, c)
            return 0
        lax.fori_loop(0, F * pieces[w][1], body, 0)

    def local(w, index):
        cols, rows = pl.ds(mult(f * K, K), K), pl.ds(mult(f * K, K), K)
        dst = bufs[w][1].at[rows, :] if w in ("mi", "up") else bufs[w][1].at[:, cols]
        return pltpu.make_async_copy(bufs[w][0], dst, lsem.at[index])

    def peer(k):
        return lax.rem(t + k, T)

    def tp_copy(src, dst, send, recv, k):
        return pltpu.make_async_remote_copy(
            src_ref=src, dst_ref=dst, send_sem=send, recv_sem=recv,
            device_id=(g, f, peer(k)), device_id_type=MESH)

    def gather_copy(buf, sems, block, target):
        return pltpu.make_async_remote_copy(
            src_ref=buf.at[block], dst_ref=buf.at[block], send_sem=gs.at[sems[0]],
            recv_sem=sems[1].at[block], device_id=(g, f, target), device_id_type=MESH)

    def gather_start(buf, sems):
        for k in range(2, T, 2):
            gather_copy(buf, sems, t, peer(k)).start()
        gather_copy(buf, sems, t, sibling).start()

    def gather_finish(buf, sems):
        for k in range(2, T, 2):
            block = lax.rem(t - k + T, T)
            gather_copy(buf, sems, block, sibling).wait_recv()
            gather_copy(buf, sems, block, sibling).start()
        for k in range(0, T, 2):
            block = lax.rem(sibling - k + T, T)
            gather_copy(buf, sems, block, sibling).wait_recv()

    def gather_drain(buf, sems):
        sent = buf.at[pl.ds(0, T - 1)]
        pltpu.make_async_remote_copy(
            src_ref=sent, dst_ref=sent, send_sem=gs.at[sems[0]], recv_sem=sems[1].at[0],
            device_id=(g, f, sibling), device_id_type=MESH).wait_send()

    own_rows, end_rows = g2.at[0], g2.at[1]
    sems1, sems2, sems3 = (0, g1r), (1, g2r), (2, g3r)

    def end_copy():
        return pltpu.make_async_remote_copy(
            src_ref=g2.at[0, t], dst_ref=g2.at[1, t], send_sem=es.at[0], recv_sem=er.at[0],
            device_id=(g, inner, t), device_id_type=MESH)

    def swap1(j):
        cols = pl.ds(j * step, step)
        return pltpu.make_async_remote_copy(
            src_ref=sp1.at[1 - place, :, :, cols], dst_ref=rq1.at[:, :, cols],
            send_sem=w1s.at[0], recv_sem=w1r.at[j], device_id=(g, f, sibling), device_id_type=MESH)

    def part1(k):
        return tp_copy(sp1.at[place, peer(k) // 2], rp1.at[k // 2 - 1],
                       p1s.at[k // 2 - 1], p1r.at[k // 2 - 1], k)

    def columns(s, c):
        return pl.ds(mult(s * K + c * cd, cd), cd)

    def swap2(i, s, c):
        return pltpu.make_async_remote_copy(
            src_ref=sp2.at[i, 1 - place, :, :, columns(s, c)], dst_ref=rq2.at[i, :, :, columns(s, c)],
            send_sem=w2s.at[i], recv_sem=w2r.at[i, s, c],
            device_id=(g, f, sibling), device_id_type=MESH)

    def part2(s, c, k):
        return tp_copy(sp2.at[0, place, peer(k) // 2, :, columns(s, c)], rp2.at[k // 2, :, columns(s, c)],
                       p2s.at[k // 2 - 1], p2r.at[k // 2], k)

    def part3(s, c, k):
        return pltpu.make_async_remote_copy(
            src_ref=sp2.at[1, place, peer(k) // 2, :, columns(s, c)], dst_ref=rp2.at[k // 2, :, columns(s, c)],
            send_sem=p3s.at[k // 2], recv_sem=p2r.at[k // 2],
            device_id=(g, helped, peer(k)), device_id_type=MESH)

    def merge(a, b):
        return (a.astype(jnp.float32) + b.astype(jnp.float32)).astype(jnp.bfloat16)

    loads = [pltpu.make_async_copy(a, b, lsem.at[4 + i])
             for i, (a, b) in enumerate(((tok_h, tok), (gains_h, gains), (scale_h, scale)))]
    for load in loads:
        load.start()
    for index, w in enumerate(("mi", "mo", "up", "dn")):
        local(w, index).start()

    barrier = pltpu.get_barrier_semaphore()

    @pl.when(f + 1 < F)
    def _():
        pl.semaphore_signal(barrier, inc=1, device_id=(g, f + 1, t), device_id_type=MESH)

    @pl.when(f > 0)
    def _():
        pl.semaphore_signal(barrier, inc=1, device_id=(g, f - 1, t), device_id_type=MESH)

    for k in range(1, G):
        pl.semaphore_signal(barrier, inc=1, device_id=(lax.rem(g + k, G), f, t), device_id_type=MESH)
    for k in range(1, T):
        pl.semaphore_signal(barrier, inc=1, device_id=(g, f, peer(k)), device_id_type=MESH)
    greeted = jnp.where(f + 1 < F, 1, 0) + jnp.where(f > 0, 1, 0) + (G - 1 + T - 1)
    if off:
        @pl.when(helper)
        def _():
            for k in range(1, T):
                pl.semaphore_signal(barrier, inc=1, device_id=(g, helped, peer(k)), device_id_type=MESH)

        @pl.when(end)
        def _():
            for k in range(1, T):
                pl.semaphore_signal(barrier, inc=1, device_id=(g, inner, peer(k)), device_id_type=MESH)
        greeted = greeted + jnp.where(helper | end, T - 1, 0)
    pl.semaphore_wait(barrier, greeted)

    send_own("mi", 0)
    send_own("mo", 0)
    send_own("up", 0)
    for load in loads:
        load.wait()
    g1[t] = normalize(tok[...], gains[0:1, :]).astype(jnp.bfloat16)
    gather_start(g1, sems1)

    for d in range(1, F):
        pump("mi", d, 0)
        pump("mo", d, 0)
        if d < NU:
            send_own("up", d)
    for c in range(F, NU):
        send_own("up", c)
    send_whole("up")

    for c in range(NU // 2):
        pump("up", 1, c)

    y_wait_all("mi")
    local("mi", 0).wait()
    gather_finish(g1, sems1)
    mixed_in = jnp.dot(g1[...].reshape(T * R, D), mi[...],
                       preferred_element_type=jnp.float32).astype(jnp.bfloat16)
    scaled = (pooling(mixed_in, t * PWt, PWt * T // GROUPS) * scale[...]).astype(jnp.bfloat16)
    y_wait_all("mo")
    local("mo", 1).wait()
    for j in range(4):
        cols = pl.ds(j * step, step)
        value = jnp.dot(scaled, mo[:, cols], preferred_element_type=jnp.float32
                        ).astype(jnp.bfloat16).reshape(half_t, 2, R, step)
        for q in range(2):
            sp1[q, :, :, cols] = value[:, q]
        swap1(j).start()
    for j in range(4):
        cols = pl.ds(j * step, step)
        swap1(j).wait_recv()
        sp1[place, :, :, cols] = merge(sp1[place, :, :, cols], rq1[:, :, cols])
    for k in range(2, T, 2):
        part1(k).start()

    def pump_all(w, d, start=0):
        def body(c, _):
            pump(w, d, c)
            return 0
        lax.fori_loop(start, pieces[w][1], body, 0)

    pump_all("up", 1, NU // 2)
    early = far <= 2

    @pl.when(mid_plane & early)
    def _():
        for c in range(ND):
            send_own("dn", c)

    total = sp1[place, t // 2].astype(jnp.float32)
    for k in range(2, T, 2):
        part1(k).wait_recv()
        total = total + rp1[k // 2 - 1].astype(jnp.float32)
    mixer_out = total.astype(jnp.bfloat16)
    middle = (tok[...].astype(jnp.float32) + normalize(mixer_out, gains[1:2, :])).astype(jnp.bfloat16)
    mid[...] = middle
    g2[0, t] = normalize(middle, gains[2:3, :]).astype(jnp.bfloat16)

    @pl.when(mid_plane)
    def _():
        gather_start(own_rows, sems2)
    if off:
        @pl.when(end)
        def _():
            end_copy().start()

    def pump_mid(d, _):
        pump_all("up", d)
        return 0
    lax.fori_loop(2, far, pump_mid, 0)

    @pl.when(~(mid_plane & early))
    def _():
        for c in range(ND):
            send_own("dn", c)
    send_whole("dn")
    if far > 1:
        pump_all("up", far)

    width = 256

    def up_project(i):
        def up_step(j, _):
            cols = pl.ds(mult(j * width, width), width)
            pre = jnp.dot(g2[i].reshape(T * R, D), up[:, cols], preferred_element_type=jnp.float32)
            pre = jnp.maximum(pre, 0.0)
            hid[i, :, cols] = (pre * pre).astype(jnp.bfloat16)
            return 0
        lax.fori_loop(0, Ht // width, up_step, 0)

    local("up", 2).wait()
    local("dn", 3).wait()

    @pl.when(mid_plane)
    def _():
        gather_finish(own_rows, sems2)
        if off:
            @pl.when(helper)
            def _():
                end_copy().wait_recv()
                gather_start(end_rows, sems3)
        y_wait_all("up")
        up_project(0)
        for c in range(ND // 2):
            pump("dn", 1, c)
        if off:
            @pl.when(helper)
            def _():
                gather_finish(end_rows, sems3)
                up_project(1)

    def dn_compute(s, c):
        @pl.when(s != f)
        def _():
            y_wait("dn", s, c)
        cols = columns(s, c)

        def project(i):
            value = jnp.dot(hid[i], dn[:, cols], preferred_element_type=jnp.float32
                            ).astype(jnp.bfloat16).reshape(half_t, 2, R, cd)
            for q in range(2):
                sp2[i, q, :, :, cols] = value[:, q]
            swap2(i, s, c).start()
        if off:
            @pl.when(helper)
            def _():
                project(1)
        project(0)

    def dn_merge(s, c):
        cols = columns(s, c)

        def finish(i):
            swap2(i, s, c).wait_recv()
            sp2[i, place, :, :, cols] = merge(sp2[i, place, :, :, cols], rq2[i, :, :, cols])
        if off:
            @pl.when(helper)
            def _():
                finish(1)
                for k in range(0, T, 2):
                    part3(s, c, k).start()
        finish(0)
        for k in range(2, T, 2):
            part2(s, c, k).start()

    def dn_step(e, _):
        d, c = e // ND, lax.rem(e, ND)

        @pl.when((d <= far) & (e >= ND + ND // 2))
        def _():
            pump("dn", d, c)

        def one(j, _):
            now = j // 4
            late = lax.rem(j, 4) // 2
            side = lax.rem(j, 2)
            ev = e - 1 + now - ND + late * (ND - 1)
            dd, cc = ev // ND, lax.rem(ev, ND)
            s = f + (2 * side - 1) * dd
            right_turn = jnp.where(late == 1, dd == far, dd < far)
            once = (dd > 0) | (side == 0)
            wanted = (ev >= 0) & right_turn & once & (s >= 0) & (s < F)

            @pl.when(wanted & (now == 0))
            def _():
                dn_merge(s, cc)

            @pl.when(wanted & (now == 1))
            def _():
                dn_compute(s, cc)
            return 0
        lax.fori_loop(0, 8, one, 0)
        return 0

    @pl.when(mid_plane)
    def _():
        lax.fori_loop(ND, (far + 1) * ND + 2, dn_step, 0)

    def landed(k):
        return tp_copy(rp2.at[k // 2], rp2.at[k // 2], p2s.at[0], p2r.at[k // 2], 2)

    for k in range(2, T, 2):
        landed(k).wait_recv()
    if off:
        @pl.when(end)
        def _():
            landed(0).wait_recv()

    @pl.when(mid_plane)
    def _():
        rp2[0] = sp2[0, place, t // 2]
    total = jnp.zeros((R, D), jnp.float32)
    for k in range(half_t):
        total = total + rp2[k].astype(jnp.float32)
    channel_out = total.astype(jnp.bfloat16)
    out[...] = (mid[...].astype(jnp.float32) + normalize(channel_out, gains[3:4, :])).astype(jnp.bfloat16)

    def sent(kind, sem):
        rows = (mi if kind == 0 else up).at[pl.ds(0, 2 * (K // G)), :]
        pltpu.make_async_remote_copy(
            src_ref=rows, dst_ref=rows, send_sem=sem, recv_sem=zr.at[0, 0],
            device_id=(g, f, sibling), device_id_type=MESH).wait_send()

    for kind, w in ((0, "mi"), (1, "up")):
        def drain(s, _):
            moved = True if kind == 0 else (mid_plane | (s == f))

            @pl.when((s <= f) & to_right_ok(w) & moved)
            def _():
                sent(kind, zs.at[0, kind, s])

            @pl.when((s >= f) & to_left_ok(w) & moved)
            def _():
                sent(kind, zs.at[1, kind, s])

            @pl.when((s != f) & moved & shared(w, s))
            def _():
                for k in range(1, G):
                    sent(kind, ys.at[k - 1, kind, s])
            if off and kind == 1:
                @pl.when((s == f) & end)
                def _():
                    for k in range(1, G):
                        sent(kind, ys.at[k - 1, kind, s])
            return 0
        lax.fori_loop(0, F, drain, 0)

    def swapped(buf, sem):
        pltpu.make_async_remote_copy(
            src_ref=buf, dst_ref=buf, send_sem=sem, recv_sem=w1r.at[0],
            device_id=(g, f, sibling), device_id_type=MESH).wait_send()

    @pl.when(mid_plane)
    def _():
        swapped(rq2.at[0], w2s.at[0])
        for k in range(2, T, 2):
            swapped(rp2.at[0], p2s.at[k // 2 - 1])
        gather_drain(own_rows, sems2)
        if off:
            @pl.when(helper)
            def _():
                gather_drain(end_rows, sems3)
                swapped(rq2.at[1], w2s.at[1])
                for k in range(0, T, 2):
                    swapped(rp2.at[0], p3s.at[k // 2])
    if off:
        @pl.when(end)
        def _():
            end_copy().wait_send()
    gather_drain(g1, sems1)
    swapped(rq1, w1s.at[0])
    for k in range(2, T, 2):
        part1(k).wait_send()


def local_layer(sizes, tokens, mix_in, scale, mix_out, up_w, down_w, gains):
    G, F, T = sizes
    R, D = tokens.shape
    K, PWt = mix_in.shape
    Ht = up_w.shape[1]
    NU = max(1, min(4, Ht // 256))
    ND = max(1, min(4, K // 128))
    dims = (G, F, T, R, D, K, PWt, Ht, NU, ND)
    NP = 2 + NU + ND
    H = T // 2
    vmem, hbm = pl.BlockSpec(memory_space=pltpu.VMEM), pl.BlockSpec(memory_space=pl.ANY)
    bf, dma = jnp.bfloat16, pltpu.SemaphoreType.DMA
    return pl.pallas_call(
        functools.partial(kernel, dims),
        out_shape=pltpu.VMEM((R, D), bf),
        in_specs=[hbm] * 7,
        out_specs=vmem,
        scratch_shapes=[
            pltpu.VMEM((R, D), bf), pltpu.VMEM(gains.shape, jnp.float32), pltpu.VMEM((1, PWt), jnp.float32),
            pltpu.VMEM((D, PWt), bf), pltpu.VMEM((PWt, D), bf),
            pltpu.VMEM((D, Ht), bf), pltpu.VMEM((Ht, D), bf),
            pltpu.VMEM((T, R, D), bf), pltpu.VMEM((2, T, R, D), bf),
            pltpu.VMEM((2, T * R, Ht), bf),
            pltpu.VMEM((2, H, R, D), bf), pltpu.VMEM((H, R, D), bf), pltpu.VMEM((H - 1, R, D), bf),
            pltpu.VMEM((2, 2, H, R, D), bf), pltpu.VMEM((2, H, R, D), bf), pltpu.VMEM((H, R, D), bf),
            pltpu.VMEM((R, D), bf),
            dma((7,)), dma((2, 2, F)), dma((F, NP)),
            dma((G - 1, 2, F)), dma((G - 1, F, NP)),
            dma((3,)), dma((T,)), dma((T,)), dma((T,)),
            dma((1,)), dma((1,)),
            dma((1,)), dma((4,)), dma((2,)), dma((2, F, ND)),
            dma((H - 1,)), dma((H - 1,)),
            dma((H - 1,)), dma((H,)), dma((H,)),
        ],
        compiler_params=pltpu.CompilerParams(
            collective_id=0, has_side_effects=True, vmem_limit_bytes=63 * 1024 * 1024),
    )(tokens, gains, scale.reshape(1, PWt), mix_in, mix_out, up_w, down_w)


def solution(mesh):
    sizes = tuple(mesh.shape[name] for name in ("grp", "fs", "tp"))
    return jax.shard_map(
        functools.partial(local_layer, sizes),
        mesh=mesh,
        in_specs=(
            P(("grp", "fs", "tp"), None),
            P("fs", "tp"),
            P("tp"),
            P("tp", "fs"),
            P("fs", "tp"),
            P("tp", "fs"),
            P(),
        ),
        out_specs=P(("grp", "fs", "tp"), None),
        check_vma=False,
    )
```

```python
import functools

import jax
import jax.numpy as jnp
from jax import lax
from jax.experimental import pallas as pl
from jax.experimental.pallas import tpu as pltpu
from jax.sharding import PartitionSpec as P

GROUPS = 4
EPS = 1e-06
MESH = pl.DeviceIdType.MESH


def normalize(values, gain):
    upcast = values.astype(jnp.float32)
    return upcast * lax.rsqrt(jnp.mean(upcast * upcast, axis=-1, keepdims=True) + EPS) * gain


def pooling(mixed_in, first_channel, group_width):
    length, width = mixed_in.shape
    upcast = mixed_in.astype(jnp.float32)
    row = lax.broadcasted_iota(jnp.int32, (length, width), 0)
    group = (first_channel + lax.broadcasted_iota(jnp.int32, (length, width), 1)) // group_width
    position = (row + 1).astype(jnp.float32)
    total, average = upcast, jnp.zeros_like(upcast)
    for index in range(GROUPS):
        step = 1 << index
        total = total + jnp.where(row >= step, pltpu.roll(total, step, axis=0), 0.0)
        mean = total / jnp.minimum(position, float(2 * step))
        average = jnp.where(group == index, mean, average)
    return average - upcast


def kernel(dims, tok_h, gains_h, scale_h, mi_h, mo_h, up_h, dn_h, out,
           tok, gains, scale, mi, mo, up, dn, g1, g2, hid, sp1, rq1, rp1, sp2, rq2, rp2, mid,
           lsem, zs, zr, ys, yr, gs, g1r, g2r, g3r, es, er,
           w1s, w1r, w2s, w2r, p1s, p1r, p2s, p2r, p3s):
    G, F, T, R, D, K, PWt, Ht, NU, ND = dims
    g, f, t = lax.axis_index("grp"), lax.axis_index("fs"), lax.axis_index("tp")
    cu, cd = Ht // NU, K // ND
    UD = 1 if ND % 2 else 2
    NB = ND // UD
    cw = UD * cd
    off = F >= 4
    far = F - 2 if off else F - 1
    first, last = (1, F - 2) if off else (0, F - 1)
    mid_plane = (f >= first) & (f <= last)
    end = (f < first) | (f > last)
    helper = (f == 1) | (f == F - 2) if off else f < 0
    helped = jnp.where(f == 1, 0, F - 1)
    inner = jnp.where(f == 0, 1, F - 2)
    sibling = t + 1 - 2 * lax.rem(t, 2)
    place, half_t = lax.rem(t, 2), T // 2
    step = D // 4

    def to_right_ok(w):
        return f + 1 < F if w in ("mi", "mo") else (f + 1 <= last)

    def to_left_ok(w):
        return f > 0 if w in ("mi", "mo") else (f - 1 >= first)

    def shared(w, s):
        return True if w in ("mi", "mo") or not off else ~(helper & (s == helped))
    pieces = {"mi": (0, 1), "mo": (1, 1), "up": (2, NU), "dn": (2 + NU, ND)}
    kinds = {"mi": 0, "mo": 0, "up": 1, "dn": 1}
    bufs = {"mi": (mi_h, mi), "mo": (mo_h, mo), "up": (up_h, up), "dn": (dn_h, dn)}

    def mult(value, by):
        return pl.multiple_of(value, by)

    def span(w, s, c, half):
        base = 0 if s is None else s * K
        if w == "mi":
            return pl.ds(mult(base + half * (K // G), K // G), K // G), pl.ds(0, PWt)
        if w == "mo":
            return pl.ds(mult(half * (PWt // G), PWt // G), PWt // G), pl.ds(mult(base, 128), K)
        if w == "up":
            return pl.ds(mult(base + half * (K // G), K // G), K // G), pl.ds(mult(c * cu, cu), cu)
        return pl.ds(mult(half * (Ht // G), Ht // G), Ht // G), pl.ds(mult(base + c * cd, cd), cd)

    def view(w, s, c, half):
        return bufs[w][1].at[span(w, s, c, half)]

    def z_copy(w, s, c, to_right, own=False):
        p = pieces[w][0] + c
        src = bufs[w][0].at[span(w, None, c, g)] if own else view(w, s, c, g)
        target = f + 1 if to_right else f - 1
        side = 0 if to_right else 1
        return pltpu.make_async_remote_copy(
            src_ref=src, dst_ref=view(w, s, c, g), send_sem=zs.at[side, kinds[w], s], recv_sem=zr.at[s, p],
            device_id=(g, target, t), device_id_type=MESH)

    def y_copy(w, s, c, k, half=None):
        p = pieces[w][0] + c
        half = g if half is None else half
        return pltpu.make_async_remote_copy(
            src_ref=view(w, s, c, half), dst_ref=view(w, s, c, half),
            send_sem=ys.at[k - 1, kinds[w], s], recv_sem=yr.at[k - 1, s, p],
            device_id=(lax.rem(g + k, G), f, t), device_id_type=MESH)

    def send_own(w, c):
        @pl.when(to_right_ok(w))
        def _():
            z_copy(w, f, c, True, own=True).start()

        @pl.when(to_left_ok(w))
        def _():
            z_copy(w, f, c, False, own=True).start()

    def whole_copy(w, c, k):
        p = pieces[w][0] + c
        half = lax.rem(g - k + G, G)
        return pltpu.make_async_remote_copy(
            src_ref=bufs[w][0].at[span(w, None, c, half)], dst_ref=view(w, f, c, half),
            send_sem=ys.at[k - 1, kinds[w], f], recv_sem=yr.at[k - 1, f, p],
            device_id=(g, inner, t), device_id_type=MESH)

    def send_whole(w):
        if off:
            @pl.when(end)
            def _():
                for c in range(pieces[w][1]):
                    for k in range(1, G):
                        whole_copy(w, c, k).start()

    def pump(w, d, c):
        for to_right in (True, False):
            s = f - d if to_right else f + d
            more = to_right_ok(w) if to_right else to_left_ok(w)
            here = (s >= 0) & (s < F)
            if w in ("up", "dn"):
                here = here & mid_plane

            @pl.when(here)
            def _():
                z_copy(w, s, c, to_right).wait_recv()

                @pl.when(more)
                def _():
                    z_copy(w, s, c, to_right).start()

                @pl.when(shared(w, s))
                def _():
                    for k in range(1, G):
                        y_copy(w, s, c, k).start()

    def y_wait(w, s, c):
        for k in range(1, G):
            y_copy(w, s, c, k, lax.rem(g - k + G, G)).wait_recv()

    def y_wait_all(w):
        def body(i, _):
            s, c = i // pieces[w][1], lax.rem(i, pieces[w][1])

            @pl.when(s != f)
            def _():
                y_wait(w, s, c)
            return 0
        lax.fori_loop(0, F * pieces[w][1], body, 0)

    def local(w, index):
        cols, rows = pl.ds(mult(f * K, K), K), pl.ds(mult(f * K, K), K)
        dst = bufs[w][1].at[rows, :] if w in ("mi", "up") else bufs[w][1].at[:, cols]
        return pltpu.make_async_copy(bufs[w][0], dst, lsem.at[index])

    def peer(k):
        return lax.rem(t + k, T)

    def tp_copy(src, dst, send, recv, k):
        return pltpu.make_async_remote_copy(
            src_ref=src, dst_ref=dst, send_sem=send, recv_sem=recv,
            device_id=(g, f, peer(k)), device_id_type=MESH)

    def gather_copy(buf, sems, block, target):
        return pltpu.make_async_remote_copy(
            src_ref=buf.at[block], dst_ref=buf.at[block], send_sem=gs.at[sems[0]],
            recv_sem=sems[1].at[block], device_id=(g, f, target), device_id_type=MESH)

    def gather_start(buf, sems):
        for k in range(2, T, 2):
            gather_copy(buf, sems, t, peer(k)).start()
        gather_copy(buf, sems, t, sibling).start()

    def gather_finish(buf, sems):
        for k in range(2, T, 2):
            block = lax.rem(t - k + T, T)
            gather_copy(buf, sems, block, sibling).wait_recv()
            gather_copy(buf, sems, block, sibling).start()
        for k in range(0, T, 2):
            block = lax.rem(sibling - k + T, T)
            gather_copy(buf, sems, block, sibling).wait_recv()

    def gather_drain(buf, sems):
        sent = buf.at[pl.ds(0, T - 1)]
        pltpu.make_async_remote_copy(
            src_ref=sent, dst_ref=sent, send_sem=gs.at[sems[0]], recv_sem=sems[1].at[0],
            device_id=(g, f, sibling), device_id_type=MESH).wait_send()

    own_rows, end_rows = g2.at[0], g2.at[1]
    sems1, sems2, sems3 = (0, g1r), (1, g2r), (2, g3r)

    def end_copy():
        return pltpu.make_async_remote_copy(
            src_ref=g2.at[0, t], dst_ref=g2.at[1, t], send_sem=es.at[0], recv_sem=er.at[0],
            device_id=(g, inner, t), device_id_type=MESH)

    def swap1(j):
        cols = pl.ds(j * step, step)
        return pltpu.make_async_remote_copy(
            src_ref=sp1.at[1 - place, :, :, cols], dst_ref=rq1.at[:, :, cols],
            send_sem=w1s.at[0], recv_sem=w1r.at[j], device_id=(g, f, sibling), device_id_type=MESH)

    def part1(k):
        return tp_copy(sp1.at[place, peer(k) // 2], rp1.at[k // 2 - 1],
                       p1s.at[k // 2 - 1], p1r.at[k // 2 - 1], k)

    def columns(s, u):
        return pl.ds(mult(s * K + u * cw, cw), cw)

    def swap2(i, s, u):
        return pltpu.make_async_remote_copy(
            src_ref=sp2.at[i, 1 - place, :, :, columns(s, u)], dst_ref=rq2.at[i, :, :, columns(s, u)],
            send_sem=w2s.at[i], recv_sem=w2r.at[i, s, u],
            device_id=(g, f, sibling), device_id_type=MESH)

    def part2(s, u, k):
        return tp_copy(sp2.at[0, place, peer(k) // 2, :, columns(s, u)], rp2.at[k // 2, :, columns(s, u)],
                       p2s.at[k // 2 - 1], p2r.at[k // 2], k)

    def part3(s, u, k):
        return pltpu.make_async_remote_copy(
            src_ref=sp2.at[1, place, peer(k) // 2, :, columns(s, u)], dst_ref=rp2.at[k // 2, :, columns(s, u)],
            send_sem=p3s.at[k // 2], recv_sem=p2r.at[k // 2],
            device_id=(g, helped, peer(k)), device_id_type=MESH)

    def merge(a, b):
        return (a.astype(jnp.float32) + b.astype(jnp.float32)).astype(jnp.bfloat16)

    loads = [pltpu.make_async_copy(a, b, lsem.at[4 + i])
             for i, (a, b) in enumerate(((tok_h, tok), (gains_h, gains), (scale_h, scale)))]
    for load in loads:
        load.start()
    for index, w in enumerate(("mi", "mo", "up", "dn")):
        local(w, index).start()

    barrier = pltpu.get_barrier_semaphore()

    @pl.when(f + 1 < F)
    def _():
        pl.semaphore_signal(barrier, inc=1, device_id=(g, f + 1, t), device_id_type=MESH)

    @pl.when(f > 0)
    def _():
        pl.semaphore_signal(barrier, inc=1, device_id=(g, f - 1, t), device_id_type=MESH)

    for k in range(1, G):
        pl.semaphore_signal(barrier, inc=1, device_id=(lax.rem(g + k, G), f, t), device_id_type=MESH)
    for k in range(1, T):
        pl.semaphore_signal(barrier, inc=1, device_id=(g, f, peer(k)), device_id_type=MESH)
    greeted = jnp.where(f + 1 < F, 1, 0) + jnp.where(f > 0, 1, 0) + (G - 1 + T - 1)
    if off:
        @pl.when(helper)
        def _():
            for k in range(1, T):
                pl.semaphore_signal(barrier, inc=1, device_id=(g, helped, peer(k)), device_id_type=MESH)

        @pl.when(end)
        def _():
            for k in range(1, T):
                pl.semaphore_signal(barrier, inc=1, device_id=(g, inner, peer(k)), device_id_type=MESH)
        greeted = greeted + jnp.where(helper | end, T - 1, 0)
    pl.semaphore_wait(barrier, greeted)

    send_own("mi", 0)
    send_own("mo", 0)
    send_own("up", 0)
    for load in loads:
        load.wait()
    g1[t] = normalize(tok[...], gains[0:1, :]).astype(jnp.bfloat16)
    gather_start(g1, sems1)

    for d in range(1, F):
        pump("mi", d, 0)
        pump("mo", d, 0)
        if d < NU:
            send_own("up", d)
    for c in range(F, NU):
        send_own("up", c)
    send_whole("up")

    for c in range(NU // 2):
        pump("up", 1, c)

    y_wait_all("mi")
    local("mi", 0).wait()
    gather_finish(g1, sems1)
    mixed_in = jnp.dot(g1[...].reshape(T * R, D), mi[...],
                       preferred_element_type=jnp.float32).astype(jnp.bfloat16)
    scaled = (pooling(mixed_in, t * PWt, PWt * T // GROUPS) * scale[...]).astype(jnp.bfloat16)
    y_wait_all("mo")
    local("mo", 1).wait()
    for j in range(4):
        cols = pl.ds(j * step, step)
        value = jnp.dot(scaled, mo[:, cols], preferred_element_type=jnp.float32
                        ).astype(jnp.bfloat16).reshape(half_t, 2, R, step)
        for q in range(2):
            sp1[q, :, :, cols] = value[:, q]
        swap1(j).start()
    for j in range(4):
        cols = pl.ds(j * step, step)
        swap1(j).wait_recv()
        sp1[place, :, :, cols] = merge(sp1[place, :, :, cols], rq1[:, :, cols])
    for k in range(2, T, 2):
        part1(k).start()

    def pump_all(w, d, start=0):
        def body(c, _):
            pump(w, d, c)
            return 0
        lax.fori_loop(start, pieces[w][1], body, 0)

    pump_all("up", 1, NU // 2)
    early = far <= 2

    @pl.when(mid_plane & early)
    def _():
        for c in range(ND):
            send_own("dn", c)

    total = sp1[place, t // 2].astype(jnp.float32)
    for k in range(2, T, 2):
        part1(k).wait_recv()
        total = total + rp1[k // 2 - 1].astype(jnp.float32)
    mixer_out = total.astype(jnp.bfloat16)
    middle = (tok[...].astype(jnp.float32) + normalize(mixer_out, gains[1:2, :])).astype(jnp.bfloat16)
    mid[...] = middle
    g2[0, t] = normalize(middle, gains[2:3, :]).astype(jnp.bfloat16)

    @pl.when(mid_plane)
    def _():
        gather_start(own_rows, sems2)
    if off:
        @pl.when(end)
        def _():
            end_copy().start()

    def pump_mid(d, _):
        pump_all("up", d)
        return 0
    lax.fori_loop(2, far, pump_mid, 0)

    @pl.when(~(mid_plane & early))
    def _():
        for c in range(ND):
            send_own("dn", c)
    send_whole("dn")
    if far > 1:
        pump_all("up", far)

    def up_project(i, c):
        cols = pl.ds(mult(c * cu, cu), cu)
        pre = jnp.dot(g2[i].reshape(T * R, D), up[:, cols], preferred_element_type=jnp.float32)
        pre = jnp.maximum(pre, 0.0)
        hid[i, :, cols] = (pre * pre).astype(jnp.bfloat16)

    half_u, half_d = NU // 2, (ND + 1) // 2
    turn = max(half_u - 1, 0)
    soon = [c for c in range(half_d) if half_u + c < NU]
    if off and half_d < ND:
        soon.append(half_d)
    later = [c for c in range(ND) if c not in soon]

    def up_step(j, _):
        i, c = j // NU, lax.rem(j, NU)

        @pl.when(i == 0)
        def _():
            def landed_rows(s, _):
                @pl.when(s != f)
                def _():
                    y_wait("up", s, c)
                return 0
            lax.fori_loop(0, F, landed_rows, 0)
        if off:
            @pl.when(helper & (i == 1) & (c == 0))
            def _():
                gather_finish(end_rows, sems3)

        @pl.when((i == 0) | helper)
        def _():
            up_project(i, c)
        if off:
            @pl.when(helper & (i == 0) & (c == turn))
            def _():
                end_copy().wait_recv()
                gather_start(end_rows, sems3)
        first_pass = (i == 0) & (c >= half_u) & (c - half_u < half_d)
        second_pass = (i == 1) & (c == turn) & (half_d < ND)

        @pl.when(first_pass | second_pass)
        def _():
            pump("dn", 1, jnp.where(i == 0, c - half_u, half_d))
        return 0

    local("up", 2).wait()
    local("dn", 3).wait()

    def dn_compute(s, u):
        @pl.when(s != f)
        def _():
            for c in range(UD):
                y_wait("dn", s, u * UD + c)
        cols = columns(s, u)

        def project(i):
            value = jnp.dot(hid[i], dn[:, cols], preferred_element_type=jnp.float32
                            ).astype(jnp.bfloat16).reshape(half_t, 2, R, cw)
            for q in range(2):
                sp2[i, q, :, :, cols] = value[:, q]
            swap2(i, s, u).start()
        if off:
            @pl.when(helper)
            def _():
                project(1)
        project(0)

    def dn_merge(s, u):
        cols = columns(s, u)

        def finish(i):
            swap2(i, s, u).wait_recv()
            sp2[i, place, :, :, cols] = merge(sp2[i, place, :, :, cols], rq2[i, :, :, cols])
        if off:
            @pl.when(helper)
            def _():
                finish(1)
                for k in range(0, T, 2):
                    part3(s, u, k).start()
        finish(0)
        for k in range(2, T, 2):
            part2(s, u, k).start()

    slots = (far + 1) * NB

    def dn_step(n, _):
        def one(j, _):
            now, which = j // 3, lax.rem(j, 3)
            slot = n - 1 + now
            d, u = slot // NB, lax.rem(slot, NB)
            s = jnp.where(which == 0, helped, jnp.where(which == 1, f - d, f + d))
            theirs = helper & (s == helped)
            side = (s >= 0) & (s < F) & ~theirs & ((which == 1) | (d > 0))
            wanted = (slot >= 0) & (slot < slots) & jnp.where(which == 0, helper & (d == far), side)

            @pl.when(wanted & (now == 0))
            def _():
                dn_merge(s, u)

            @pl.when(wanted & (now == 1))
            def _():
                dn_compute(s, u)
            return 0
        lax.fori_loop(0, 6, one, 0)

        @pl.when(n == NB - 1)
        def _():
            for c in later:
                pump("dn", 1, c)

        @pl.when((n >= NB) & (n < far * NB))
        def _():
            for c in range(UD):
                pump("dn", n // NB + 1, lax.rem(n, NB) * UD + c)
        return 0

    @pl.when(mid_plane)
    def _():
        gather_finish(own_rows, sems2)
        lax.fori_loop(0, (2 if off else 1) * NU, up_step, 0)
        lax.fori_loop(0, slots + 1, dn_step, 0)

    def landed(k):
        return tp_copy(rp2.at[k // 2], rp2.at[k // 2], p2s.at[0], p2r.at[k // 2], 2)

    for k in range(2, T, 2):
        landed(k).wait_recv()
    if off:
        @pl.when(end)
        def _():
            landed(0).wait_recv()

    @pl.when(mid_plane)
    def _():
        rp2[0] = sp2[0, place, t // 2]
    total = jnp.zeros((R, D), jnp.float32)
    for k in range(half_t):
        total = total + rp2[k].astype(jnp.float32)
    channel_out = total.astype(jnp.bfloat16)
    out[...] = (mid[...].astype(jnp.float32) + normalize(channel_out, gains[3:4, :])).astype(jnp.bfloat16)

    def sent(kind, sem):
        rows = (mi if kind == 0 else up).at[pl.ds(0, 2 * (K // G)), :]
        pltpu.make_async_remote_copy(
            src_ref=rows, dst_ref=rows, send_sem=sem, recv_sem=zr.at[0, 0],
            device_id=(g, f, sibling), device_id_type=MESH).wait_send()

    for kind, w in ((0, "mi"), (1, "up")):
        def drain(s, _):
            moved = True if kind == 0 else (mid_plane | (s == f))

            @pl.when((s <= f) & to_right_ok(w) & moved)
            def _():
                sent(kind, zs.at[0, kind, s])

            @pl.when((s >= f) & to_left_ok(w) & moved)
            def _():
                sent(kind, zs.at[1, kind, s])

            @pl.when((s != f) & moved & shared(w, s))
            def _():
                for k in range(1, G):
                    sent(kind, ys.at[k - 1, kind, s])
            if off and kind == 1:
                @pl.when((s == f) & end)
                def _():
                    for k in range(1, G):
                        sent(kind, ys.at[k - 1, kind, s])
            return 0
        lax.fori_loop(0, F, drain, 0)

    def swapped(buf, sem):
        pltpu.make_async_remote_copy(
            src_ref=buf, dst_ref=buf, send_sem=sem, recv_sem=w1r.at[0],
            device_id=(g, f, sibling), device_id_type=MESH).wait_send()

    @pl.when(mid_plane)
    def _():
        swapped(rq2.at[0], w2s.at[0])
        for k in range(2, T, 2):
            swapped(rp2.at[0], p2s.at[k // 2 - 1])
        gather_drain(own_rows, sems2)
        if off:
            @pl.when(helper)
            def _():
                gather_drain(end_rows, sems3)
                swapped(rq2.at[1], w2s.at[1])
                for k in range(0, T, 2):
                    swapped(rp2.at[0], p3s.at[k // 2])
    if off:
        @pl.when(end)
        def _():
            end_copy().wait_send()
    gather_drain(g1, sems1)
    swapped(rq1, w1s.at[0])
    for k in range(2, T, 2):
        part1(k).wait_send()


def local_layer(sizes, tokens, mix_in, scale, mix_out, up_w, down_w, gains):
    G, F, T = sizes
    R, D = tokens.shape
    K, PWt = mix_in.shape
    Ht = up_w.shape[1]
    NU = max(1, min(4, Ht // 256))
    ND = max(1, min(4, K // 128))
    dims = (G, F, T, R, D, K, PWt, Ht, NU, ND)
    NP = 2 + NU + ND
    H = T // 2
    vmem, hbm = pl.BlockSpec(memory_space=pltpu.VMEM), pl.BlockSpec(memory_space=pl.ANY)
    bf, dma = jnp.bfloat16, pltpu.SemaphoreType.DMA
    return pl.pallas_call(
        functools.partial(kernel, dims),
        out_shape=pltpu.VMEM((R, D), bf),
        in_specs=[hbm] * 7,
        out_specs=vmem,
        scratch_shapes=[
            pltpu.VMEM((R, D), bf), pltpu.VMEM(gains.shape, jnp.float32), pltpu.VMEM((1, PWt), jnp.float32),
            pltpu.VMEM((D, PWt), bf), pltpu.VMEM((PWt, D), bf),
            pltpu.VMEM((D, Ht), bf), pltpu.VMEM((Ht, D), bf),
            pltpu.VMEM((T, R, D), bf), pltpu.VMEM((2, T, R, D), bf),
            pltpu.VMEM((2, T * R, Ht), bf),
            pltpu.VMEM((2, H, R, D), bf), pltpu.VMEM((H, R, D), bf), pltpu.VMEM((H - 1, R, D), bf),
            pltpu.VMEM((2, 2, H, R, D), bf), pltpu.VMEM((2, H, R, D), bf), pltpu.VMEM((H, R, D), bf),
            pltpu.VMEM((R, D), bf),
            dma((7,)), dma((2, 2, F)), dma((F, NP)),
            dma((G - 1, 2, F)), dma((G - 1, F, NP)),
            dma((3,)), dma((T,)), dma((T,)), dma((T,)),
            dma((1,)), dma((1,)),
            dma((1,)), dma((4,)), dma((2,)), dma((2, F, ND if ND % 2 else ND // 2)),
            dma((H - 1,)), dma((H - 1,)),
            dma((H - 1,)), dma((H,)), dma((H,)),
        ],
        compiler_params=pltpu.CompilerParams(
            collective_id=0, has_side_effects=True, vmem_limit_bytes=63 * 1024 * 1024),
    )(tokens, gains, scale.reshape(1, PWt), mix_in, mix_out, up_w, down_w)


def solution(mesh):
    sizes = tuple(mesh.shape[name] for name in ("grp", "fs", "tp"))
    return jax.shard_map(
        functools.partial(local_layer, sizes),
        mesh=mesh,
        in_specs=(
            P(("grp", "fs", "tp"), None),
            P("fs", "tp"),
            P("tp"),
            P("tp", "fs"),
            P("fs", "tp"),
            P("tp", "fs"),
            P(),
        ),
        out_specs=P(("grp", "fs", "tp"), None),
        check_vma=False,
    )
```

```python
import functools

import jax
import jax.numpy as jnp
from jax import lax
from jax.experimental import pallas as pl
from jax.experimental.pallas import tpu as pltpu
from jax.sharding import PartitionSpec as P

GROUPS = 4
EPS = 1e-06
MESH = pl.DeviceIdType.MESH


def normalize(values, gain):
    upcast = values.astype(jnp.float32)
    return upcast * lax.rsqrt(jnp.mean(upcast * upcast, axis=-1, keepdims=True) + EPS) * gain


def pooling(mixed_in, first_channel, group_width):
    length, width = mixed_in.shape
    upcast = mixed_in.astype(jnp.float32)
    row = lax.broadcasted_iota(jnp.int32, (length, width), 0)
    group = (first_channel + lax.broadcasted_iota(jnp.int32, (length, width), 1)) // group_width
    position = (row + 1).astype(jnp.float32)
    total, average = upcast, jnp.zeros_like(upcast)
    for index in range(GROUPS):
        step = 1 << index
        total = total + jnp.where(row >= step, pltpu.roll(total, step, axis=0), 0.0)
        mean = total / jnp.minimum(position, float(2 * step))
        average = jnp.where(group == index, mean, average)
    return average - upcast


def kernel(dims, tok_h, gains_h, scale_h, mi_h, mo_h, up_h, dn_h, out,
           tok, gains, scale, mi, mo, up, dn, g1, g2, hid, sp1, rq1, rp1, sp2, rq2, rp2, mid,
           lsem, zs, zr, ys, yr, gs, g1r, g2r, g3r, es, er,
           w1s, w1r, w2s, w2r, p1s, p1r, p2s, p2r, p3s):
    G, F, T, R, D, K, PWt, Ht, NU, ND = dims
    g, f, t = lax.axis_index("grp"), lax.axis_index("fs"), lax.axis_index("tp")
    cu, cd = Ht // NU, K // ND
    UD = 1 if ND % 2 else 2
    NB = ND // UD
    cw = UD * cd
    off = F >= 4
    tuned = F == 4 and NU == 4 and ND == 4
    far = F - 2 if off else F - 1
    first, last = (1, F - 2) if off else (0, F - 1)
    mid_plane = (f >= first) & (f <= last)
    end = (f < first) | (f > last)
    helper = (f == 1) | (f == F - 2) if off else f < 0
    helped = jnp.where(f == 1, 0, F - 1)
    inner = jnp.where(f == 0, 1, F - 2)
    sibling = t + 1 - 2 * lax.rem(t, 2)
    place, half_t = lax.rem(t, 2), T // 2
    step = D // 4

    def to_right_ok(w):
        return f + 1 < F if w in ("mi", "mo") else (f + 1 <= last)

    def to_left_ok(w):
        return f > 0 if w in ("mi", "mo") else (f - 1 >= first)

    def shared(w, s):
        return True if w in ("mi", "mo") or not off else ~(helper & (s == helped))
    pieces = {"mi": (0, 1), "mo": (1, 1), "up": (2, NU), "dn": (2 + NU, ND)}
    kinds = {"mi": 0, "mo": 0, "up": 1, "dn": 1}
    bufs = {"mi": (mi_h, mi), "mo": (mo_h, mo), "up": (up_h, up), "dn": (dn_h, dn)}

    def mult(value, by):
        return pl.multiple_of(value, by)

    def span(w, s, c, half):
        base = 0 if s is None else s * K
        if w == "mi":
            return pl.ds(mult(base + half * (K // G), K // G), K // G), pl.ds(0, PWt)
        if w == "mo":
            return pl.ds(mult(half * (PWt // G), PWt // G), PWt // G), pl.ds(mult(base, 128), K)
        if w == "up":
            return pl.ds(mult(base + half * (K // G), K // G), K // G), pl.ds(mult(c * cu, cu), cu)
        return pl.ds(mult(half * (Ht // G), Ht // G), Ht // G), pl.ds(mult(base + c * cd, cd), cd)

    def view(w, s, c, half):
        return bufs[w][1].at[span(w, s, c, half)]

    def z_copy(w, s, c, to_right, own=False):
        p = pieces[w][0] + c
        src = bufs[w][0].at[span(w, None, c, g)] if own else view(w, s, c, g)
        target = f + 1 if to_right else f - 1
        side = 0 if to_right else 1
        return pltpu.make_async_remote_copy(
            src_ref=src, dst_ref=view(w, s, c, g), send_sem=zs.at[side, kinds[w], s], recv_sem=zr.at[s, p],
            device_id=(g, target, t), device_id_type=MESH)

    def y_copy(w, s, c, k, half=None):
        p = pieces[w][0] + c
        half = g if half is None else half
        return pltpu.make_async_remote_copy(
            src_ref=view(w, s, c, half), dst_ref=view(w, s, c, half),
            send_sem=ys.at[k - 1, kinds[w], s], recv_sem=yr.at[k - 1, s, p],
            device_id=(lax.rem(g + k, G), f, t), device_id_type=MESH)

    def send_own(w, c):
        @pl.when(to_right_ok(w))
        def _():
            z_copy(w, f, c, True, own=True).start()

        @pl.when(to_left_ok(w))
        def _():
            z_copy(w, f, c, False, own=True).start()

    def whole_copy(w, c, k):
        p = pieces[w][0] + c
        half = lax.rem(g - k + G, G)
        return pltpu.make_async_remote_copy(
            src_ref=bufs[w][0].at[span(w, None, c, half)], dst_ref=view(w, f, c, half),
            send_sem=ys.at[k - 1, kinds[w], f], recv_sem=yr.at[k - 1, f, p],
            device_id=(g, inner, t), device_id_type=MESH)

    def send_whole(w):
        if off:
            order = list(range(pieces[w][1]))
            if tuned and w == "dn":
                order = order[-1:] + order[:-1]

            @pl.when(end)
            def _():
                for c in order:
                    for k in range(1, G):
                        whole_copy(w, c, k).start()

    def pass_on(k):
        half = lax.rem(g - k + G, G)
        p = pieces["dn"][0] + ND - 1
        block = view("dn", helped, ND - 1, half)
        return pltpu.make_async_remote_copy(
            src_ref=block, dst_ref=block, send_sem=ys.at[k - 1, 1, helped], recv_sem=yr.at[k - 1, helped, p],
            device_id=(g, F - 1 - f, t), device_id_type=MESH)

    def pump(w, d, c, kind=None):
        for to_right in (True, False):
            s = f - d if to_right else f + d
            more = to_right_ok(w) if to_right else to_left_ok(w)
            here = (s >= 0) & (s < F)
            if w in ("up", "dn"):
                here = here & mid_plane
            theirs = helper & (s == helped)
            if kind is not None:
                here = here & (theirs if kind == "relay" else ~theirs)
            spread = shared(w, s)
            if tuned and w == "dn" and c == ND - 1:
                spread = spread & (s > 0) & (s < F - 1)

            @pl.when(here)
            def _():
                z_copy(w, s, c, to_right).wait_recv()

                @pl.when(more)
                def _():
                    z_copy(w, s, c, to_right).start()

                @pl.when(spread)
                def _():
                    for k in range(1, G):
                        y_copy(w, s, c, k).start()

    def y_wait(w, s, c):
        for k in range(1, G):
            y_copy(w, s, c, k, lax.rem(g - k + G, G)).wait_recv()

    def y_wait_all(w):
        def body(i, _):
            s, c = i // pieces[w][1], lax.rem(i, pieces[w][1])

            @pl.when(s != f)
            def _():
                y_wait(w, s, c)
            return 0
        lax.fori_loop(0, F * pieces[w][1], body, 0)

    def local(w, index):
        cols, rows = pl.ds(mult(f * K, K), K), pl.ds(mult(f * K, K), K)
        dst = bufs[w][1].at[rows, :] if w in ("mi", "up") else bufs[w][1].at[:, cols]
        return pltpu.make_async_copy(bufs[w][0], dst, lsem.at[index])

    def peer(k):
        return lax.rem(t + k, T)

    def tp_copy(src, dst, send, recv, k):
        return pltpu.make_async_remote_copy(
            src_ref=src, dst_ref=dst, send_sem=send, recv_sem=recv,
            device_id=(g, f, peer(k)), device_id_type=MESH)

    def gather_copy(buf, sems, block, target):
        return pltpu.make_async_remote_copy(
            src_ref=buf.at[block], dst_ref=buf.at[block], send_sem=gs.at[sems[0]],
            recv_sem=sems[1].at[block], device_id=(g, f, target), device_id_type=MESH)

    def gather_start(buf, sems):
        for k in range(2, T, 2):
            gather_copy(buf, sems, t, peer(k)).start()
        gather_copy(buf, sems, t, sibling).start()

    def gather_finish(buf, sems):
        for k in range(2, T, 2):
            block = lax.rem(t - k + T, T)
            gather_copy(buf, sems, block, sibling).wait_recv()
            gather_copy(buf, sems, block, sibling).start()
        for k in range(0, T, 2):
            block = lax.rem(sibling - k + T, T)
            gather_copy(buf, sems, block, sibling).wait_recv()

    def gather_drain(buf, sems):
        sent = buf.at[pl.ds(0, T - 1)]
        pltpu.make_async_remote_copy(
            src_ref=sent, dst_ref=sent, send_sem=gs.at[sems[0]], recv_sem=sems[1].at[0],
            device_id=(g, f, sibling), device_id_type=MESH).wait_send()

    own_rows, end_rows = g2.at[0], g2.at[1]
    sems1, sems2, sems3 = (0, g1r), (1, g2r), (2, g3r)

    def end_copy():
        return pltpu.make_async_remote_copy(
            src_ref=g2.at[0, t], dst_ref=g2.at[1, t], send_sem=es.at[0], recv_sem=er.at[0],
            device_id=(g, inner, t), device_id_type=MESH)

    def swap1(j):
        cols = pl.ds(j * step, step)
        return pltpu.make_async_remote_copy(
            src_ref=sp1.at[1 - place, :, :, cols], dst_ref=rq1.at[:, :, cols],
            send_sem=w1s.at[0], recv_sem=w1r.at[j], device_id=(g, f, sibling), device_id_type=MESH)

    def part1(k):
        return tp_copy(sp1.at[place, peer(k) // 2], rp1.at[k // 2 - 1],
                       p1s.at[k // 2 - 1], p1r.at[k // 2 - 1], k)

    def columns(s, u):
        return pl.ds(mult(s * K + u * cw, cw), cw)

    def swap2(i, s, u):
        return pltpu.make_async_remote_copy(
            src_ref=sp2.at[i, 1 - place, :, :, columns(s, u)], dst_ref=rq2.at[i, :, :, columns(s, u)],
            send_sem=w2s.at[i], recv_sem=w2r.at[i, s, u],
            device_id=(g, f, sibling), device_id_type=MESH)

    def part2(s, u, k):
        return tp_copy(sp2.at[0, place, peer(k) // 2, :, columns(s, u)], rp2.at[k // 2, :, columns(s, u)],
                       p2s.at[k // 2 - 1], p2r.at[k // 2], k)

    def part3(s, u, k):
        return pltpu.make_async_remote_copy(
            src_ref=sp2.at[1, place, peer(k) // 2, :, columns(s, u)], dst_ref=rp2.at[k // 2, :, columns(s, u)],
            send_sem=p3s.at[k // 2], recv_sem=p2r.at[k // 2],
            device_id=(g, helped, peer(k)), device_id_type=MESH)

    def merge(a, b):
        return (a.astype(jnp.float32) + b.astype(jnp.float32)).astype(jnp.bfloat16)

    loads = [pltpu.make_async_copy(a, b, lsem.at[4 + i])
             for i, (a, b) in enumerate(((tok_h, tok), (gains_h, gains), (scale_h, scale)))]
    for load in loads:
        load.start()
    for index, w in enumerate(("mi", "mo", "up", "dn")):
        local(w, index).start()

    barrier = pltpu.get_barrier_semaphore()

    @pl.when(f + 1 < F)
    def _():
        pl.semaphore_signal(barrier, inc=1, device_id=(g, f + 1, t), device_id_type=MESH)

    @pl.when(f > 0)
    def _():
        pl.semaphore_signal(barrier, inc=1, device_id=(g, f - 1, t), device_id_type=MESH)

    for k in range(1, G):
        pl.semaphore_signal(barrier, inc=1, device_id=(lax.rem(g + k, G), f, t), device_id_type=MESH)
    for k in range(1, T):
        pl.semaphore_signal(barrier, inc=1, device_id=(g, f, peer(k)), device_id_type=MESH)
    greeted = jnp.where(f + 1 < F, 1, 0) + jnp.where(f > 0, 1, 0) + (G - 1 + T - 1)
    if off:
        @pl.when(helper)
        def _():
            for k in range(1, T):
                pl.semaphore_signal(barrier, inc=1, device_id=(g, helped, peer(k)), device_id_type=MESH)

        @pl.when(end)
        def _():
            for k in range(1, T):
                pl.semaphore_signal(barrier, inc=1, device_id=(g, inner, peer(k)), device_id_type=MESH)
        greeted = greeted + jnp.where(helper | end, T - 1, 0)
    pl.semaphore_wait(barrier, greeted)

    send_own("mi", 0)
    send_own("mo", 0)
    send_own("up", 0)
    for load in loads:
        load.wait()
    g1[t] = normalize(tok[...], gains[0:1, :]).astype(jnp.bfloat16)
    gather_start(g1, sems1)

    for d in range(1, F):
        pump("mi", d, 0)
        pump("mo", d, 0)
        if d < NU:
            send_own("up", d)
    for c in range(F, NU):
        send_own("up", c)
    send_whole("up")

    for c in range(NU // 2):
        pump("up", 1, c)

    y_wait_all("mi")
    local("mi", 0).wait()
    gather_finish(g1, sems1)
    mixed_in = jnp.dot(g1[...].reshape(T * R, D), mi[...],
                       preferred_element_type=jnp.float32).astype(jnp.bfloat16)
    scaled = (pooling(mixed_in, t * PWt, PWt * T // GROUPS) * scale[...]).astype(jnp.bfloat16)
    y_wait_all("mo")
    local("mo", 1).wait()
    for j in range(4):
        cols = pl.ds(j * step, step)
        value = jnp.dot(scaled, mo[:, cols], preferred_element_type=jnp.float32
                        ).astype(jnp.bfloat16).reshape(half_t, 2, R, step)
        for q in range(2):
            sp1[q, :, :, cols] = value[:, q]
        swap1(j).start()
    for j in range(4):
        cols = pl.ds(j * step, step)
        swap1(j).wait_recv()
        sp1[place, :, :, cols] = merge(sp1[place, :, :, cols], rq1[:, :, cols])
    for k in range(2, T, 2):
        part1(k).start()

    def pump_all(w, d, start=0):
        def body(c, _):
            pump(w, d, c)
            return 0
        lax.fori_loop(start, pieces[w][1], body, 0)

    pump_all("up", 1, NU // 2)
    early = far <= 2

    @pl.when(mid_plane & early)
    def _():
        for c in range(ND):
            send_own("dn", c)

    total = sp1[place, t // 2].astype(jnp.float32)
    for k in range(2, T, 2):
        part1(k).wait_recv()
        total = total + rp1[k // 2 - 1].astype(jnp.float32)
    mixer_out = total.astype(jnp.bfloat16)
    middle = (tok[...].astype(jnp.float32) + normalize(mixer_out, gains[1:2, :])).astype(jnp.bfloat16)
    mid[...] = middle
    g2[0, t] = normalize(middle, gains[2:3, :]).astype(jnp.bfloat16)

    @pl.when(mid_plane)
    def _():
        gather_start(own_rows, sems2)
    if off:
        @pl.when(end)
        def _():
            end_copy().start()

    def pump_mid(d, _):
        pump_all("up", d)
        return 0
    lax.fori_loop(2, far, pump_mid, 0)

    @pl.when(~(mid_plane & early))
    def _():
        for c in range(ND):
            send_own("dn", c)
    send_whole("dn")
    if far > 1:
        pump_all("up", far)

    def up_project(i, c):
        cols = pl.ds(mult(c * cu, cu), cu)
        pre = jnp.dot(g2[i].reshape(T * R, D), up[:, cols], preferred_element_type=jnp.float32)
        pre = jnp.maximum(pre, 0.0)
        hid[i, :, cols] = (pre * pre).astype(jnp.bfloat16)

    half_u, half_d = NU // 2, (ND + 1) // 2
    turn = max(half_u - 1, 0)
    soon = [c for c in range(half_d) if half_u + c < NU]
    if off and half_d < ND:
        soon.append(half_d)
    later = [c for c in range(ND) if c not in soon]

    def act(todo):
        for what, d, c in todo:
            if what == "pass":
                y_wait("dn", helped, ND - 1)
                for k in range(1, G):
                    pass_on(k).start()
            else:
                pump("dn", d, c, what)

    up_acts = {2: [("near", 1, 0)], 3: [("near", 1, 1), ("relay", 1, 0), ("near", 1, 2)], 5: [("relay", 1, 1)],
               6: [("near", 1, 3)], 7: [("relay", 1, 2)]}
    dn_acts = {3: [("relay", 1, 3), ("near", 2, 0)], 5: [("near", 2, 1)], 7: [("near", 2, 2), ("pass", 0, 0)],
               8: [("near", 2, 3)]}

    def scheduled(acts, n):
        for index, todo in acts.items():
            @pl.when(n == index)
            def _():
                act(todo)

    def up_step(j, _):
        i, c = j // NU, lax.rem(j, NU)

        @pl.when(i == 0)
        def _():
            def landed_rows(s, _):
                @pl.when(s != f)
                def _():
                    y_wait("up", s, c)
                return 0
            lax.fori_loop(0, F, landed_rows, 0)
        if off:
            @pl.when(helper & (i == 1) & (c == 0))
            def _():
                gather_finish(end_rows, sems3)

        @pl.when((i == 0) | helper)
        def _():
            up_project(i, c)
        if off:
            @pl.when(helper & (i == 0) & (c == turn))
            def _():
                end_copy().wait_recv()
                gather_start(end_rows, sems3)
        if tuned:
            scheduled(up_acts, j)
            return 0
        first_pass = (i == 0) & (c >= half_u) & (c - half_u < half_d)
        second_pass = (i == 1) & (c == turn) & (half_d < ND)

        @pl.when(first_pass | second_pass)
        def _():
            pump("dn", 1, jnp.where(i == 0, c - half_u, half_d))
        return 0

    local("up", 2).wait()
    local("dn", 3).wait()

    def dn_compute(s, u):
        @pl.when(s != f)
        def _():
            for c in range(UD):
                if tuned and c == UD - 1:
                    @pl.when(~(helper & (s == helped) & (u == NB - 1)))
                    def _():
                        y_wait("dn", s, u * UD + c)
                else:
                    y_wait("dn", s, u * UD + c)
        cols = columns(s, u)

        def project(i):
            value = jnp.dot(hid[i], dn[:, cols], preferred_element_type=jnp.float32
                            ).astype(jnp.bfloat16).reshape(half_t, 2, R, cw)
            for q in range(2):
                sp2[i, q, :, :, cols] = value[:, q]
            swap2(i, s, u).start()
        if off:
            @pl.when(helper)
            def _():
                project(1)
        project(0)

    def dn_merge(s, u):
        cols = columns(s, u)

        def finish(i):
            swap2(i, s, u).wait_recv()
            sp2[i, place, :, :, cols] = merge(sp2[i, place, :, :, cols], rq2[i, :, :, cols])
        if off:
            @pl.when(helper)
            def _():
                finish(1)
                for k in range(0, T, 2):
                    part3(s, u, k).start()
        finish(0)
        for k in range(2, T, 2):
            part2(s, u, k).start()

    slots = (far + 1) * NB

    def dn_step(n, _):
        def one(now, _):
            m = n - 1 + now
            slot, q = m // 2, lax.rem(m, 2)
            d, u = slot // NB, lax.rem(slot, NB)
            last = helper & (d == far)
            s = jnp.where(q == 0, f - d, f + d)
            s = jnp.where(last, jnp.where(q == 0, F - 1 - helped, helped), s)
            wanted = ((m >= 0) & (slot < slots) & (s >= 0) & (s < F) & ((q == 0) | (d > 0))
                      & (last | ~(helper & (s == helped))))

            @pl.when(wanted & (now == 0))
            def _():
                dn_merge(s, u)

            @pl.when(wanted & (now == 1))
            def _():
                dn_compute(s, u)
            return 0
        lax.fori_loop(0, 2, one, 0)
        if tuned:
            scheduled(dn_acts, n)
            return 0
        slot = n // 2

        @pl.when(n == 2 * NB - 1)
        def _():
            for c in later:
                pump("dn", 1, c)

        @pl.when((lax.rem(n, 2) == 1) & (slot >= NB) & (slot < far * NB))
        def _():
            for c in range(UD):
                pump("dn", slot // NB + 1, lax.rem(slot, NB) * UD + c)
        return 0

    @pl.when(mid_plane)
    def _():
        gather_finish(own_rows, sems2)
        lax.fori_loop(0, (2 if off else 1) * NU, up_step, 0)
        lax.fori_loop(0, 2 * slots + 1, dn_step, 0)

    def landed(k):
        return tp_copy(rp2.at[k // 2], rp2.at[k // 2], p2s.at[0], p2r.at[k // 2], 2)

    for k in range(2, T, 2):
        landed(k).wait_recv()
    if off:
        @pl.when(end)
        def _():
            landed(0).wait_recv()

    @pl.when(mid_plane)
    def _():
        rp2[0] = sp2[0, place, t // 2]
    total = jnp.zeros((R, D), jnp.float32)
    for k in range(half_t):
        total = total + rp2[k].astype(jnp.float32)
    channel_out = total.astype(jnp.bfloat16)
    out[...] = (mid[...].astype(jnp.float32) + normalize(channel_out, gains[3:4, :])).astype(jnp.bfloat16)

    def sent(kind, sem):
        rows = (mi if kind == 0 else up).at[pl.ds(0, 2 * (K // G)), :]
        pltpu.make_async_remote_copy(
            src_ref=rows, dst_ref=rows, send_sem=sem, recv_sem=zr.at[0, 0],
            device_id=(g, f, sibling), device_id_type=MESH).wait_send()

    def swapped(buf, sem):
        pltpu.make_async_remote_copy(
            src_ref=buf, dst_ref=buf, send_sem=sem, recv_sem=w1r.at[0],
            device_id=(g, f, sibling), device_id_type=MESH).wait_send()

    for kind, w in ((0, "mi"), (1, "up")):
        def drain(s, _):
            moved = True if kind == 0 else (mid_plane | (s == f))

            @pl.when((s <= f) & to_right_ok(w) & moved)
            def _():
                sent(kind, zs.at[0, kind, s])

            @pl.when((s >= f) & to_left_ok(w) & moved)
            def _():
                sent(kind, zs.at[1, kind, s])

            gone = (s != f) & moved & shared(w, s)
            ends = (s == 0) | (s == F - 1) if tuned and kind == 1 else s < 0

            @pl.when(gone & ~ends)
            def _():
                for k in range(1, G):
                    sent(kind, ys.at[k - 1, kind, s])
            if tuned and kind == 1:
                @pl.when(gone & ends)
                def _():
                    for k in range(1, G):
                        swapped(up.at[pl.ds(0, 2 * (K // G) - cd // G), :], ys.at[k - 1, kind, s])

                @pl.when(helper & (s == helped))
                def _():
                    for k in range(1, G):
                        swapped(view("dn", 0, 0, 0), ys.at[k - 1, kind, s])
            if off and kind == 1:
                @pl.when((s == f) & end)
                def _():
                    for k in range(1, G):
                        sent(kind, ys.at[k - 1, kind, s])
            return 0
        lax.fori_loop(0, F, drain, 0)

    @pl.when(mid_plane)
    def _():
        swapped(rq2.at[0], w2s.at[0])
        for k in range(2, T, 2):
            swapped(rp2.at[0], p2s.at[k // 2 - 1])
        gather_drain(own_rows, sems2)
        if off:
            @pl.when(helper)
            def _():
                gather_drain(end_rows, sems3)
                swapped(rq2.at[1], w2s.at[1])
                for k in range(0, T, 2):
                    swapped(rp2.at[0], p3s.at[k // 2])
    if off:
        @pl.when(end)
        def _():
            end_copy().wait_send()
    gather_drain(g1, sems1)
    swapped(rq1, w1s.at[0])
    for k in range(2, T, 2):
        part1(k).wait_send()


def local_layer(sizes, tokens, mix_in, scale, mix_out, up_w, down_w, gains):
    G, F, T = sizes
    R, D = tokens.shape
    K, PWt = mix_in.shape
    Ht = up_w.shape[1]
    NU = max(1, min(4, Ht // 256))
    ND = max(1, min(4, K // 128))
    dims = (G, F, T, R, D, K, PWt, Ht, NU, ND)
    NP = 2 + NU + ND
    H = T // 2
    vmem, hbm = pl.BlockSpec(memory_space=pltpu.VMEM), pl.BlockSpec(memory_space=pl.ANY)
    bf, dma = jnp.bfloat16, pltpu.SemaphoreType.DMA
    return pl.pallas_call(
        functools.partial(kernel, dims),
        out_shape=pltpu.VMEM((R, D), bf),
        in_specs=[hbm] * 7,
        out_specs=vmem,
        scratch_shapes=[
            pltpu.VMEM((R, D), bf), pltpu.VMEM(gains.shape, jnp.float32), pltpu.VMEM((1, PWt), jnp.float32),
            pltpu.VMEM((D, PWt), bf), pltpu.VMEM((PWt, D), bf),
            pltpu.VMEM((D, Ht), bf), pltpu.VMEM((Ht, D), bf),
            pltpu.VMEM((T, R, D), bf), pltpu.VMEM((2, T, R, D), bf),
            pltpu.VMEM((2, T * R, Ht), bf),
            pltpu.VMEM((2, H, R, D), bf), pltpu.VMEM((H, R, D), bf), pltpu.VMEM((H - 1, R, D), bf),
            pltpu.VMEM((2, 2, H, R, D), bf), pltpu.VMEM((2, H, R, D), bf), pltpu.VMEM((H, R, D), bf),
            pltpu.VMEM((R, D), bf),
            dma((7,)), dma((2, 2, F)), dma((F, NP)),
            dma((G - 1, 2, F)), dma((G - 1, F, NP)),
            dma((3,)), dma((T,)), dma((T,)), dma((T,)),
            dma((1,)), dma((1,)),
            dma((1,)), dma((4,)), dma((2,)), dma((2, F, ND if ND % 2 else ND // 2)),
            dma((H - 1,)), dma((H - 1,)),
            dma((H - 1,)), dma((H,)), dma((H,)),
        ],
        compiler_params=pltpu.CompilerParams(
            collective_id=0, has_side_effects=True, vmem_limit_bytes=63 * 1024 * 1024),
    )(tokens, gains, scale.reshape(1, PWt), mix_in, mix_out, up_w, down_w)


def solution(mesh):
    sizes = tuple(mesh.shape[name] for name in ("grp", "fs", "tp"))
    return jax.shard_map(
        functools.partial(local_layer, sizes),
        mesh=mesh,
        in_specs=(
            P(("grp", "fs", "tp"), None),
            P("fs", "tp"),
            P("tp"),
            P("tp", "fs"),
            P("fs", "tp"),
            P("tp", "fs"),
            P(),
        ),
        out_specs=P(("grp", "fs", "tp"), None),
        check_vma=False,
    )
```

```python
import functools

import jax
import jax.numpy as jnp
from jax import lax
from jax.experimental import pallas as pl
from jax.experimental.pallas import tpu as pltpu
from jax.sharding import PartitionSpec as P

GROUPS = 4
EPS = 1e-06
MESH = pl.DeviceIdType.MESH


def normalize(values, gain):
    upcast = values.astype(jnp.float32)
    return upcast * lax.rsqrt(jnp.mean(upcast * upcast, axis=-1, keepdims=True) + EPS) * gain


def pooling(mixed_in, first_channel, group_width):
    length, width = mixed_in.shape
    upcast = mixed_in.astype(jnp.float32)
    row = lax.broadcasted_iota(jnp.int32, (length, width), 0)
    group = (first_channel + lax.broadcasted_iota(jnp.int32, (length, width), 1)) // group_width
    position = (row + 1).astype(jnp.float32)
    total, average = upcast, jnp.zeros_like(upcast)
    for index in range(GROUPS):
        step = 1 << index
        total = total + jnp.where(row >= step, pltpu.roll(total, step, axis=0), 0.0)
        mean = total / jnp.minimum(position, float(2 * step))
        average = jnp.where(group == index, mean, average)
    return average - upcast


def kernel(dims, tok_h, gains_h, scale_h, mi_h, mo_h, up_h, dn_h, out,
           tok, gains, scale, mi, mo, up, dn, g1, g2, hid, sp1, rq1, rp1, sp2, rq2, rp2, mid,
           lsem, zs, zr, ys, yr, gs, g1r, g2r, g3r, es, er,
           w1s, w1r, w2s, w2r, p1s, p1r, p2s, p2r, p3s):
    G, F, T, R, D, K, PWt, Ht, NU, ND = dims
    g, f, t = lax.axis_index("grp"), lax.axis_index("fs"), lax.axis_index("tp")
    cu, cd = Ht // NU, K // ND
    UD = 1 if ND % 2 else 2
    NB = ND // UD
    off = F >= 4
    tuned = F == 4 and NU == 4 and ND == 4
    far = F - 2 if off else F - 1
    first, last = (1, F - 2) if off else (0, F - 1)
    mid_plane = (f >= first) & (f <= last)
    end = (f < first) | (f > last)
    helper = (f == 1) | (f == F - 2) if off else f < 0
    helped = jnp.where(f == 1, 0, F - 1)
    inner = jnp.where(f == 0, 1, F - 2)
    sibling = t + 1 - 2 * lax.rem(t, 2)
    place, half_t = lax.rem(t, 2), T // 2
    step = D // 4

    def to_right_ok(w):
        return f + 1 < F if w in ("mi", "mo") else (f + 1 <= last)

    def to_left_ok(w):
        return f > 0 if w in ("mi", "mo") else (f - 1 >= first)

    def shared(w, s):
        return True if w in ("mi", "mo") or not off else ~(helper & (s == helped))
    pieces = {"mi": (0, 1), "mo": (1, 1), "up": (2, NU), "dn": (2 + NU, ND)}
    kinds = {"mi": 0, "mo": 0, "up": 1, "dn": 1}
    bufs = {"mi": (mi_h, mi), "mo": (mo_h, mo), "up": (up_h, up), "dn": (dn_h, dn)}

    def mult(value, by):
        return pl.multiple_of(value, by)

    def span(w, s, c, half):
        base = s * K
        if w == "mi":
            return pl.ds(mult(base + half * (K // G), K // G), K // G), pl.ds(0, PWt)
        if w == "mo":
            return pl.ds(mult(half * (PWt // G), PWt // G), PWt // G), pl.ds(mult(base, 128), K)
        if w == "up":
            return pl.ds(mult(base + half * (K // G), K // G), K // G), pl.ds(mult(c * cu, cu), cu)
        return pl.ds(mult(half * (Ht // G), Ht // G), Ht // G), pl.ds(mult(base + c * cd, cd), cd)

    def view(w, s, c, half):
        return bufs[w][1].at[span(w, s, c, half)]

    def z_copy(w, s, c, to_right):
        p = pieces[w][0] + c
        target = f + 1 if to_right else f - 1
        side = 0 if to_right else 1
        return pltpu.make_async_remote_copy(
            src_ref=view(w, s, c, g), dst_ref=view(w, s, c, g), send_sem=zs.at[side, kinds[w], s], recv_sem=zr.at[s, p],
            device_id=(g, target, t), device_id_type=MESH)

    def y_copy(w, s, c, k, half=None):
        p = pieces[w][0] + c
        half = g if half is None else half
        return pltpu.make_async_remote_copy(
            src_ref=view(w, s, c, half), dst_ref=view(w, s, c, half),
            send_sem=ys.at[k - 1, kinds[w], s], recv_sem=yr.at[k - 1, s, p],
            device_id=(lax.rem(g + k, G), f, t), device_id_type=MESH)

    def send_own(w, c):
        @pl.when(to_right_ok(w))
        def _():
            z_copy(w, f, c, True).start()

        @pl.when(to_left_ok(w))
        def _():
            z_copy(w, f, c, False).start()

    def whole_copy(w, c, k):
        p = pieces[w][0] + c
        half = lax.rem(g - k + G, G)
        return pltpu.make_async_remote_copy(
            src_ref=view(w, f, c, half), dst_ref=view(w, f, c, half),
            send_sem=ys.at[k - 1, kinds[w], f], recv_sem=yr.at[k - 1, f, p],
            device_id=(g, inner, t), device_id_type=MESH)

    def send_whole(w):
        if off:
            order = list(range(pieces[w][1]))
            if tuned and w == "dn":
                order = order[:1:-1] + order[:2]

            @pl.when(end)
            def _():
                for c in order:
                    for k in range(1, G):
                        whole_copy(w, c, k).start()

    def pass_on(k):
        half = lax.rem(g - k + G, G)
        p = pieces["dn"][0] + ND - 1
        block = view("dn", helped, ND - 1, half)
        return pltpu.make_async_remote_copy(
            src_ref=block, dst_ref=block, send_sem=ys.at[k - 1, 1, helped], recv_sem=yr.at[k - 1, helped, p],
            device_id=(g, F - 1 - f, t), device_id_type=MESH)

    def pump(w, d, c, kind=None):
        for to_right in (True, False):
            s = f - d if to_right else f + d
            more = to_right_ok(w) if to_right else to_left_ok(w)
            here = (s >= 0) & (s < F)
            if w in ("up", "dn"):
                here = here & mid_plane
            theirs = helper & (s == helped)
            if kind is not None:
                here = here & (theirs if kind == "relay" else ~theirs)
            spread = shared(w, s)
            if tuned and w == "dn" and c == ND - 1:
                spread = spread & (s > 0) & (s < F - 1)

            @pl.when(here)
            def _():
                z_copy(w, s, c, to_right).wait_recv()

                @pl.when(more)
                def _():
                    z_copy(w, s, c, to_right).start()

                @pl.when(spread)
                def _():
                    for k in range(1, G):
                        y_copy(w, s, c, k).start()

    def y_wait(w, s, c):
        for k in range(1, G):
            y_copy(w, s, c, k, lax.rem(g - k + G, G)).wait_recv()

    def y_wait_all(w):
        def body(i, _):
            s, c = i // pieces[w][1], lax.rem(i, pieces[w][1])

            @pl.when(s != f)
            def _():
                y_wait(w, s, c)
            return 0
        lax.fori_loop(0, F * pieces[w][1], body, 0)

    def local(w, index):
        cols, rows = pl.ds(mult(f * K, K), K), pl.ds(mult(f * K, K), K)
        dst = bufs[w][1].at[rows, :] if w in ("mi", "up") else bufs[w][1].at[:, cols]
        return pltpu.make_async_copy(bufs[w][0], dst, lsem.at[index])

    def peer(k):
        return lax.rem(t + k, T)

    def tp_copy(src, dst, send, recv, k):
        return pltpu.make_async_remote_copy(
            src_ref=src, dst_ref=dst, send_sem=send, recv_sem=recv,
            device_id=(g, f, peer(k)), device_id_type=MESH)

    def gather_copy(buf, sems, block, target):
        return pltpu.make_async_remote_copy(
            src_ref=buf.at[block], dst_ref=buf.at[block], send_sem=gs.at[sems[0]],
            recv_sem=sems[1].at[block], device_id=(g, f, target), device_id_type=MESH)

    def gather_start(buf, sems):
        for k in range(2, T, 2):
            gather_copy(buf, sems, t, peer(k)).start()
        gather_copy(buf, sems, t, sibling).start()

    def gather_finish(buf, sems):
        for k in range(2, T, 2):
            block = lax.rem(t - k + T, T)
            gather_copy(buf, sems, block, sibling).wait_recv()
            gather_copy(buf, sems, block, sibling).start()
        for k in range(0, T, 2):
            block = lax.rem(sibling - k + T, T)
            gather_copy(buf, sems, block, sibling).wait_recv()

    def gather_drain(buf, sems):
        sent = buf.at[pl.ds(0, T - 1)]
        pltpu.make_async_remote_copy(
            src_ref=sent, dst_ref=sent, send_sem=gs.at[sems[0]], recv_sem=sems[1].at[0],
            device_id=(g, f, sibling), device_id_type=MESH).wait_send()

    own_rows, end_rows = g2.at[0], g2.at[1]
    sems1, sems2, sems3 = (0, g1r), (1, g2r), (2, g3r)

    def end_copy():
        return pltpu.make_async_remote_copy(
            src_ref=g2.at[0, t], dst_ref=g2.at[1, t], send_sem=es.at[0], recv_sem=er.at[0],
            device_id=(g, inner, t), device_id_type=MESH)

    def swap1(j):
        cols = pl.ds(j * step, step)
        return pltpu.make_async_remote_copy(
            src_ref=sp1.at[1 - place, :, :, cols], dst_ref=rq1.at[:, :, cols],
            send_sem=w1s.at[0], recv_sem=w1r.at[j], device_id=(g, f, sibling), device_id_type=MESH)

    def part1(k):
        return tp_copy(sp1.at[place, peer(k) // 2], rp1.at[k // 2 - 1],
                       p1s.at[k // 2 - 1], p1r.at[k // 2 - 1], k)

    def columns(s, c, n):
        return pl.ds(mult(s * K + c * cd, cd), n * cd)

    def swap2(i, s, c, n):
        return pltpu.make_async_remote_copy(
            src_ref=sp2.at[i, 1 - place, :, :, columns(s, c, n)], dst_ref=rq2.at[i, :, :, columns(s, c, n)],
            send_sem=w2s.at[i], recv_sem=w2r.at[i, s, c],
            device_id=(g, f, sibling), device_id_type=MESH)

    def part2(s, c, n, k):
        return tp_copy(sp2.at[0, place, peer(k) // 2, :, columns(s, c, n)], rp2.at[k // 2, :, columns(s, c, n)],
                       p2s.at[k // 2 - 1], p2r.at[k // 2], k)

    def part3(s, c, n, k):
        return pltpu.make_async_remote_copy(
            src_ref=sp2.at[1, place, peer(k) // 2, :, columns(s, c, n)], dst_ref=rp2.at[k // 2, :, columns(s, c, n)],
            send_sem=p3s.at[k // 2], recv_sem=p2r.at[k // 2],
            device_id=(g, helped, peer(k)), device_id_type=MESH)

    def merge(a, b):
        return (a.astype(jnp.float32) + b.astype(jnp.float32)).astype(jnp.bfloat16)

    loads = [pltpu.make_async_copy(a, b, lsem.at[4 + i])
             for i, (a, b) in enumerate(((tok_h, tok), (gains_h, gains), (scale_h, scale)))]
    local("mi", 0).start()
    local("mo", 1).start()
    for load in loads:
        load.start()
    local("up", 2).start()
    local("dn", 3).start()

    barrier = pltpu.get_barrier_semaphore()

    @pl.when(f + 1 < F)
    def _():
        pl.semaphore_signal(barrier, inc=1, device_id=(g, f + 1, t), device_id_type=MESH)

    @pl.when(f > 0)
    def _():
        pl.semaphore_signal(barrier, inc=1, device_id=(g, f - 1, t), device_id_type=MESH)

    for k in range(1, G):
        pl.semaphore_signal(barrier, inc=1, device_id=(lax.rem(g + k, G), f, t), device_id_type=MESH)
    for k in range(1, T):
        pl.semaphore_signal(barrier, inc=1, device_id=(g, f, peer(k)), device_id_type=MESH)
    greeted = jnp.where(f + 1 < F, 1, 0) + jnp.where(f > 0, 1, 0) + (G - 1 + T - 1)
    if off:
        @pl.when(helper)
        def _():
            for k in range(1, T):
                pl.semaphore_signal(barrier, inc=1, device_id=(g, helped, peer(k)), device_id_type=MESH)

        @pl.when(end)
        def _():
            for k in range(1, T):
                pl.semaphore_signal(barrier, inc=1, device_id=(g, inner, peer(k)), device_id_type=MESH)
        greeted = greeted + jnp.where(helper | end, T - 1, 0)
    pl.semaphore_wait(barrier, greeted)

    local("mi", 0).wait()
    send_own("mi", 0)
    local("mo", 1).wait()
    send_own("mo", 0)
    local("up", 2).wait()
    send_own("up", 0)

    @pl.when(~mid_plane)
    def _():
        for c in range(1, NU):
            send_own("up", c)
    send_whole("up")
    for load in loads:
        load.wait()
    g1[t] = normalize(tok[...], gains[0:1, :]).astype(jnp.bfloat16)
    gather_start(g1, sems1)
    local("dn", 3).wait()

    for d in range(1, F):
        for kind in ("near", "relay"):
            if kind == "near" or (off and d == 1):
                pump("mi", d, 0, kind)
                pump("mo", d, 0, kind)
        if d < NU:
            @pl.when(mid_plane)
            def _():
                send_own("up", d)

    @pl.when(mid_plane)
    def _():
        for c in range(F, NU):
            send_own("up", c)

    for c in range(NU // 2):
        pump("up", 1, c)

    y_wait_all("mi")
    gather_finish(g1, sems1)
    mixed_in = jnp.dot(g1[...].reshape(T * R, D), mi[...],
                       preferred_element_type=jnp.float32).astype(jnp.bfloat16)
    scaled = (pooling(mixed_in, t * PWt, PWt * T // GROUPS) * scale[...]).astype(jnp.bfloat16)
    y_wait_all("mo")
    for j in range(4):
        cols = pl.ds(j * step, step)
        value = jnp.dot(scaled, mo[:, cols], preferred_element_type=jnp.float32
                        ).astype(jnp.bfloat16).reshape(half_t, 2, R, step)
        for q in range(2):
            sp1[q, :, :, cols] = value[:, q]
        swap1(j).start()
    for j in range(4):
        cols = pl.ds(j * step, step)
        swap1(j).wait_recv()
        sp1[place, :, :, cols] = merge(sp1[place, :, :, cols], rq1[:, :, cols])
    for k in range(2, T, 2):
        part1(k).start()

    def pump_all(w, d, start=0):
        def body(c, _):
            pump(w, d, c)
            return 0
        lax.fori_loop(start, pieces[w][1], body, 0)

    pump_all("up", 1, NU // 2)
    early = far <= 2

    @pl.when(mid_plane & early)
    def _():
        for c in range(ND):
            send_own("dn", c)

    total = sp1[place, t // 2].astype(jnp.float32)
    for k in range(2, T, 2):
        part1(k).wait_recv()
        total = total + rp1[k // 2 - 1].astype(jnp.float32)
    mixer_out = total.astype(jnp.bfloat16)
    middle = (tok[...].astype(jnp.float32) + normalize(mixer_out, gains[1:2, :])).astype(jnp.bfloat16)
    mid[...] = middle
    g2[0, t] = normalize(middle, gains[2:3, :]).astype(jnp.bfloat16)

    @pl.when(mid_plane)
    def _():
        gather_start(own_rows, sems2)
    if off:
        @pl.when(end)
        def _():
            end_copy().start()

    def pump_mid(d, _):
        pump_all("up", d)
        return 0
    lax.fori_loop(2, far, pump_mid, 0)

    @pl.when(~(mid_plane & early))
    def _():
        for c in range(ND):
            send_own("dn", c)
    send_whole("dn")
    if far > 1:
        pump_all("up", far)

    def up_project(i, c):
        cols = pl.ds(mult(c * cu, cu), cu)
        pre = jnp.dot(g2[i].reshape(T * R, D), up[:, cols], preferred_element_type=jnp.float32)
        pre = jnp.maximum(pre, 0.0)
        hid[i, :, cols] = (pre * pre).astype(jnp.bfloat16)

    half_u, half_d = NU // 2, (ND + 1) // 2
    turn = max(half_u - 1, 0)
    soon = [c for c in range(half_d) if half_u + c < NU]
    if off and half_d < ND:
        soon.append(half_d)
    later = [c for c in range(ND) if c not in soon]

    def act(todo):
        for what, d, c in todo:
            if what == "pass":
                y_wait("dn", helped, ND - 1)
                for k in range(1, G):
                    pass_on(k).start()
            else:
                pump("dn", d, c, what)

    up_acts = {2: [("near", 1, 0)], 3: [("near", 1, 1), ("relay", 1, 0), ("near", 1, 2)], 5: [("relay", 1, 1)],
               6: [("near", 1, 3)], 7: [("relay", 1, 2)]}

    def scheduled(acts, n):
        for index, todo in acts.items():
            @pl.when(n == index)
            def _():
                act(todo)

    def up_step(j, _):
        i, c = j // NU, lax.rem(j, NU)

        @pl.when(i == 0)
        def _():
            def landed_rows(s, _):
                @pl.when(s != f)
                def _():
                    y_wait("up", s, c)
                return 0
            lax.fori_loop(0, F, landed_rows, 0)
        if off:
            @pl.when(helper & (i == 1) & (c == 0))
            def _():
                gather_finish(end_rows, sems3)

        @pl.when((i == 0) | helper)
        def _():
            up_project(i, c)
        if off:
            @pl.when(helper & (i == 0) & (c == turn))
            def _():
                end_copy().wait_recv()
                gather_start(end_rows, sems3)
        if tuned:
            scheduled(up_acts, j)
            return 0
        first_pass = (i == 0) & (c >= half_u) & (c - half_u < half_d)
        second_pass = (i == 1) & (c == turn) & (half_d < ND)

        @pl.when(first_pass | second_pass)
        def _():
            pump("dn", 1, jnp.where(i == 0, c - half_u, half_d))
        return 0

    def project(i, s, first, n):
        cols = columns(s, first, n)
        value = jnp.dot(hid[i], dn[:, cols], preferred_element_type=jnp.float32
                        ).astype(jnp.bfloat16).reshape(half_t, 2, R, n * cd)
        for q in range(2):
            sp2[i, q, :, :, cols] = value[:, q]
        swap2(i, s, first, n).start()

    def finish(i, s, first, n):
        cols = columns(s, first, n)
        swap2(i, s, first, n).wait_recv()
        sp2[i, place, :, :, cols] = merge(sp2[i, place, :, :, cols], rq2[i, :, :, cols])

        @pl.when(i == 0)
        def _():
            for k in range(2, T, 2):
                part2(s, first, n, k).start()
        if off:
            @pl.when(i == 1)
            def _():
                for k in range(0, T, 2):
                    part3(s, first, n, k).start()

    OWN, NEAR, HELPED, FAR = range(4)
    codes, before = [], {}

    def queue(kind, who, c, n, rows=(1, 0), wait=True):
        for i in rows:
            fresh = kind == 0 and wait and who != OWN and i == rows[0]
            codes.append(kind + 2 * (n - 1) + 4 * i + 8 * fresh + 16 * who + 64 * c)

    def also(*todo):
        before.setdefault(len(codes), []).extend(todo)

    if tuned:
        queue(0, OWN, 0, 2)
        queue(0, OWN, 2, 2)
        queue(1, OWN, 0, 2)
        also(("relay", 1, 3), ("near", 2, 0))
        queue(1, OWN, 2, 2)
        queue(0, NEAR, 0, 2)
        also(("near", 2, 1))
        queue(1, NEAR, 0, 2)
        queue(0, NEAR, 2, 2)
        also(("pass", 0, 0))
        queue(1, NEAR, 2, 2)
        also(("near", 2, 2))
        queue(0, HELPED, 2, 2)
        queue(0, FAR, 0, 1)
        queue(1, HELPED, 2, 2)
        queue(1, FAR, 0, 1)
        queue(0, FAR, 1, 1, (1,))
        also(("near", 2, 3))
        queue(0, HELPED, 0, 1, (1,))
        queue(0, FAR, 1, 1, (0,), False)
        queue(1, FAR, 1, 1, (1,))
        queue(0, HELPED, 0, 1, (0,), False)
        queue(1, HELPED, 0, 1, (1,))
        queue(1, FAR, 1, 1, (0,))
        queue(0, FAR, 2, 1, (1,))
        queue(1, HELPED, 0, 1, (0,))
        queue(0, FAR, 3, 1, (1,))
        queue(0, HELPED, 1, 1, (1,))
        queue(1, FAR, 2, 1, (1,))
        queue(0, FAR, 2, 1, (0,), False)
        queue(1, FAR, 3, 1, (1,))
        queue(1, HELPED, 1, 1, (1,))
        queue(0, FAR, 3, 1, (0,), False)
        queue(0, HELPED, 1, 1, (0,), False)
        queue(1, FAR, 2, 1, (0,))
        queue(1, FAR, 3, 1, (0,))
        queue(1, HELPED, 1, 1, (0,))

    def choose(n, values):
        out = jnp.int32(values[0])
        for index, value in enumerate(values[1:]):
            out = jnp.where(n == index + 1, value, out)
        return out

    def dn_op(n, _):
        scheduled(before, n)
        code = choose(n, codes)
        kind, size, i = lax.rem(code, 2), lax.rem(code // 2, 2) + 1, lax.rem(code // 4, 2)
        fresh, who, first = lax.rem(code // 8, 2), lax.rem(code // 16, 4), code // 64
        s = jnp.where(who == OWN, f, jnp.where(who == NEAR, F - 1 - f, jnp.where(who == HELPED, helped, F - 1 - helped)))
        for c in range(2):
            passed = (who == HELPED) & (first + c == ND - 1)

            @pl.when((fresh == 1) & (c < size) & ~passed)
            def _():
                y_wait("dn", s, first + c)
        for width in (1, 2):
            @pl.when((kind == 0) & (size == width))
            def _():
                project(i, s, first, width)

            @pl.when((kind == 1) & (size == width))
            def _():
                finish(i, s, first, width)
        return 0

    slots = (far + 1) * NB

    def dn_step(n, _):
        def one(now, _):
            m = n - 1 + now
            slot, q = m // 2, lax.rem(m, 2)
            d, first = slot // NB, lax.rem(slot, NB) * UD
            last = helper & (d == far)
            s = jnp.where(q == 0, f - d, f + d)
            s = jnp.where(last, jnp.where(q == 0, F - 1 - helped, helped), s)
            wanted = ((m >= 0) & (slot < slots) & (s >= 0) & (s < F) & ((q == 0) | (d > 0))
                      & (last | ~(helper & (s == helped))))

            @pl.when(wanted & (now == 1) & (s != f))
            def _():
                for c in range(UD):
                    y_wait("dn", s, first + c)

            def rows(i, _):
                @pl.when(wanted & (now == 0))
                def _():
                    finish(i, s, first, UD)

                @pl.when(wanted & (now == 1))
                def _():
                    project(i, s, first, UD)
                return 0
            lax.fori_loop(0, jnp.where(helper, 2, 1), rows, 0)
            return 0
        lax.fori_loop(0, 2, one, 0)
        slot = n // 2

        @pl.when(n == 2 * NB - 1)
        def _():
            for c in later:
                pump("dn", 1, c)

        @pl.when((lax.rem(n, 2) == 1) & (slot >= NB) & (slot < far * NB))
        def _():
            for c in range(UD):
                pump("dn", slot // NB + 1, lax.rem(slot, NB) * UD + c)
        return 0

    @pl.when(mid_plane)
    def _():
        gather_finish(own_rows, sems2)
        lax.fori_loop(0, (2 if off else 1) * NU, up_step, 0)
        if tuned:
            lax.fori_loop(0, len(codes), dn_op, 0)
        else:
            lax.fori_loop(0, 2 * slots + 1, dn_step, 0)

    def landed(k):
        return tp_copy(rp2.at[k // 2], rp2.at[k // 2], p2s.at[0], p2r.at[k // 2], 2)

    for k in range(2, T, 2):
        landed(k).wait_recv()
    if off:
        @pl.when(end)
        def _():
            landed(0).wait_recv()

    @pl.when(mid_plane)
    def _():
        rp2[0] = sp2[0, place, t // 2]
    total = jnp.zeros((R, D), jnp.float32)
    for k in range(half_t):
        total = total + rp2[k].astype(jnp.float32)
    channel_out = total.astype(jnp.bfloat16)
    out[...] = (mid[...].astype(jnp.float32) + normalize(channel_out, gains[3:4, :])).astype(jnp.bfloat16)

    def sent(kind, sem):
        rows = (mi if kind == 0 else up).at[pl.ds(0, 2 * (K // G)), :]
        pltpu.make_async_remote_copy(
            src_ref=rows, dst_ref=rows, send_sem=sem, recv_sem=zr.at[0, 0],
            device_id=(g, f, sibling), device_id_type=MESH).wait_send()

    def swapped(buf, sem):
        pltpu.make_async_remote_copy(
            src_ref=buf, dst_ref=buf, send_sem=sem, recv_sem=w1r.at[0],
            device_id=(g, f, sibling), device_id_type=MESH).wait_send()

    for kind, w in ((0, "mi"), (1, "up")):
        def drain(s, _):
            moved = True if kind == 0 else (mid_plane | (s == f))

            @pl.when((s <= f) & to_right_ok(w) & moved)
            def _():
                sent(kind, zs.at[0, kind, s])

            @pl.when((s >= f) & to_left_ok(w) & moved)
            def _():
                sent(kind, zs.at[1, kind, s])

            gone = (s != f) & moved & shared(w, s)
            ends = (s == 0) | (s == F - 1) if tuned and kind == 1 else s < 0

            @pl.when(gone & ~ends)
            def _():
                for k in range(1, G):
                    sent(kind, ys.at[k - 1, kind, s])
            if tuned and kind == 1:
                @pl.when(gone & ends)
                def _():
                    for k in range(1, G):
                        swapped(up.at[pl.ds(0, 2 * (K // G) - cd // G), :], ys.at[k - 1, kind, s])

                @pl.when(helper & (s == helped))
                def _():
                    for k in range(1, G):
                        swapped(view("dn", 0, 0, 0), ys.at[k - 1, kind, s])
            if off and kind == 1:
                @pl.when((s == f) & end)
                def _():
                    for k in range(1, G):
                        sent(kind, ys.at[k - 1, kind, s])
            return 0
        lax.fori_loop(0, F, drain, 0)

    @pl.when(mid_plane)
    def _():
        swapped(rq2.at[0], w2s.at[0])
        for k in range(2, T, 2):
            swapped(rp2.at[0], p2s.at[k // 2 - 1])
        gather_drain(own_rows, sems2)
        if off:
            @pl.when(helper)
            def _():
                gather_drain(end_rows, sems3)
                swapped(rq2.at[1], w2s.at[1])
                for k in range(0, T, 2):
                    swapped(rp2.at[0], p3s.at[k // 2])
    if off:
        @pl.when(end)
        def _():
            end_copy().wait_send()
    gather_drain(g1, sems1)
    swapped(rq1, w1s.at[0])
    for k in range(2, T, 2):
        part1(k).wait_send()


def local_layer(sizes, tokens, mix_in, scale, mix_out, up_w, down_w, gains):
    G, F, T = sizes
    R, D = tokens.shape
    K, PWt = mix_in.shape
    Ht = up_w.shape[1]
    NU = max(1, min(4, Ht // 256))
    ND = max(1, min(4, K // 128))
    dims = (G, F, T, R, D, K, PWt, Ht, NU, ND)
    NP = 2 + NU + ND
    H = T // 2
    vmem, hbm = pl.BlockSpec(memory_space=pltpu.VMEM), pl.BlockSpec(memory_space=pl.ANY)
    bf, dma = jnp.bfloat16, pltpu.SemaphoreType.DMA
    return pl.pallas_call(
        functools.partial(kernel, dims),
        out_shape=pltpu.VMEM((R, D), bf),
        in_specs=[hbm] * 7,
        out_specs=vmem,
        scratch_shapes=[
            pltpu.VMEM((R, D), bf), pltpu.VMEM(gains.shape, jnp.float32), pltpu.VMEM((1, PWt), jnp.float32),
            pltpu.VMEM((D, PWt), bf), pltpu.VMEM((PWt, D), bf),
            pltpu.VMEM((D, Ht), bf), pltpu.VMEM((Ht, D), bf),
            pltpu.VMEM((T, R, D), bf), pltpu.VMEM((2, T, R, D), bf),
            pltpu.VMEM((2, T * R, Ht), bf),
            pltpu.VMEM((2, H, R, D), bf), pltpu.VMEM((H, R, D), bf), pltpu.VMEM((H - 1, R, D), bf),
            pltpu.VMEM((2, 2, H, R, D), bf), pltpu.VMEM((2, H, R, D), bf), pltpu.VMEM((H, R, D), bf),
            pltpu.VMEM((R, D), bf),
            dma((7,)), dma((2, 2, F)), dma((F, NP)),
            dma((G - 1, 2, F)), dma((G - 1, F, NP)),
            dma((3,)), dma((T,)), dma((T,)), dma((T,)),
            dma((1,)), dma((1,)),
            dma((1,)), dma((4,)), dma((2,)), dma((2, F, ND)),
            dma((H - 1,)), dma((H - 1,)),
            dma((H - 1,)), dma((H,)), dma((H,)),
        ],
        compiler_params=pltpu.CompilerParams(
            collective_id=0, has_side_effects=True, vmem_limit_bytes=63 * 1024 * 1024),
    )(tokens, gains, scale.reshape(1, PWt), mix_in, mix_out, up_w, down_w)


def solution(mesh):
    sizes = tuple(mesh.shape[name] for name in ("grp", "fs", "tp"))
    return jax.shard_map(
        functools.partial(local_layer, sizes),
        mesh=mesh,
        in_specs=(
            P(("grp", "fs", "tp"), None),
            P("fs", "tp"),
            P("tp"),
            P("tp", "fs"),
            P("fs", "tp"),
            P("tp", "fs"),
            P(),
        ),
        out_specs=P(("grp", "fs", "tp"), None),
        check_vma=False,
    )
```

```python
import functools

import jax
import jax.numpy as jnp
from jax import lax
from jax.experimental import pallas as pl
from jax.experimental.pallas import tpu as pltpu
from jax.sharding import PartitionSpec as P

GROUPS = 4
EPS = 1e-06
MESH = pl.DeviceIdType.MESH


def normalize(values, gain):
    upcast = values.astype(jnp.float32)
    return upcast * lax.rsqrt(jnp.mean(upcast * upcast, axis=-1, keepdims=True) + EPS) * gain


def pooling(mixed_in, first_channel, group_width):
    length, width = mixed_in.shape
    upcast = mixed_in.astype(jnp.float32)
    row = lax.broadcasted_iota(jnp.int32, (length, width), 0)
    group = (first_channel + lax.broadcasted_iota(jnp.int32, (length, width), 1)) // group_width
    position = (row + 1).astype(jnp.float32)
    total, average = upcast, jnp.zeros_like(upcast)
    for index in range(GROUPS):
        step = 1 << index
        total = total + jnp.where(row >= step, pltpu.roll(total, step, axis=0), 0.0)
        mean = total / jnp.minimum(position, float(2 * step))
        average = jnp.where(group == index, mean, average)
    return average - upcast


def kernel(dims, tok_h, gains_h, scale_h, mi_h, mo_h, up_h, dn_h, out,
           tok, gains, scale, mi, mo, up, dn, g1, g2, hid, sp1, rq1, rp1, sp2, rq2, rp2, mid,
           lsem, zs, zr, ys, yr, gs, g1r, g2r, g3r, es, er,
           w1s, w1r, w2s, w2r, p1s, p1r, p2s, p2r, p3s):
    G, F, T, R, D, K, PWt, Ht, NU, ND = dims
    g, f, t = lax.axis_index("grp"), lax.axis_index("fs"), lax.axis_index("tp")
    cu, cd = Ht // NU, K // ND
    UD = 1 if ND % 2 else 2
    NB = ND // UD
    off = F >= 4
    tuned = F == 4 and NU == 4 and ND == 4
    far = F - 2 if off else F - 1
    first, last = (1, F - 2) if off else (0, F - 1)
    mid_plane = (f >= first) & (f <= last)
    end = (f < first) | (f > last)
    helper = (f == 1) | (f == F - 2) if off else f < 0
    helped = jnp.where(f == 1, 0, F - 1)
    inner = jnp.where(f == 0, 1, F - 2)
    sibling = t + 1 - 2 * lax.rem(t, 2)
    place, half_t = lax.rem(t, 2), T // 2
    step = D // 4

    def to_right_ok(w):
        return f + 1 < F if w in ("mi", "mo") else (f + 1 <= last)

    def to_left_ok(w):
        return f > 0 if w in ("mi", "mo") else (f - 1 >= first)

    def shared(w, s):
        return True if w in ("mi", "mo") or not off else ~(helper & (s == helped))
    pieces = {"mi": (0, 1), "mo": (1, 1), "up": (2, NU), "dn": (2 + NU, ND)}
    kinds = {"mi": 0, "mo": 0, "up": 1, "dn": 1}
    bufs = {"mi": (mi_h, mi), "mo": (mo_h, mo), "up": (up_h, up), "dn": (dn_h, dn)}

    def slot_of(s, where):
        return s - jnp.where(s > where, 1, 0)

    def mult(value, by):
        return pl.multiple_of(value, by)

    def span(w, s, c, half):
        base = s * K
        if w == "mi":
            return pl.ds(mult(base + half * (K // G), K // G), K // G), pl.ds(0, PWt)
        if w == "mo":
            return pl.ds(mult(half * (PWt // G), PWt // G), PWt // G), pl.ds(mult(base, 128), K)
        if w == "up":
            return pl.ds(mult(base + half * (K // G), K // G), K // G), pl.ds(mult(c * cu, cu), cu)
        return pl.ds(mult(half * (Ht // G), Ht // G), Ht // G), pl.ds(mult(base + c * cd, cd), cd)

    def view(w, s, c, half):
        return bufs[w][1].at[span(w, s, c, half)]

    def z_copy(w, s, c, to_right):
        p = pieces[w][0] + c
        target = f + 1 if to_right else f - 1
        side = 0 if to_right else 1
        return pltpu.make_async_remote_copy(
            src_ref=view(w, s, c, g), dst_ref=view(w, s, c, g), send_sem=zs.at[side, kinds[w], s], recv_sem=zr.at[s - side, p],
            device_id=(g, target, t), device_id_type=MESH)

    def y_copy(w, s, c, k, half=None):
        p = pieces[w][0] + c
        half = g if half is None else half
        return pltpu.make_async_remote_copy(
            src_ref=view(w, s, c, half), dst_ref=view(w, s, c, half),
            send_sem=ys.at[k - 1, kinds[w], s], recv_sem=yr.at[k - 1, slot_of(s, f), p],
            device_id=(lax.rem(g + k, G), f, t), device_id_type=MESH)

    def send_own(w, c):
        @pl.when(to_right_ok(w))
        def _():
            z_copy(w, f, c, True).start()

        @pl.when(to_left_ok(w))
        def _():
            z_copy(w, f, c, False).start()

    def whole_copy(w, c, k):
        p = pieces[w][0] + c
        half = lax.rem(g - k + G, G)
        return pltpu.make_async_remote_copy(
            src_ref=view(w, f, c, half), dst_ref=view(w, f, c, half),
            send_sem=ys.at[k - 1, kinds[w], f], recv_sem=yr.at[k - 1, slot_of(f, inner), p],
            device_id=(g, inner, t), device_id_type=MESH)

    def send_whole(w):
        if off:
            order = list(range(pieces[w][1]))
            if tuned and w == "dn":
                order = order[:1:-1] + order[:2]

            @pl.when(end)
            def _():
                for c in order:
                    for k in range(1, G):
                        whole_copy(w, c, k).start()

    def pass_on(k):
        half = lax.rem(g - k + G, G)
        p = pieces["dn"][0] + ND - 1
        block = view("dn", helped, ND - 1, half)
        return pltpu.make_async_remote_copy(
            src_ref=block, dst_ref=block, send_sem=ys.at[k - 1, 1, helped], recv_sem=yr.at[k - 1, slot_of(helped, F - 1 - f), p],
            device_id=(g, F - 1 - f, t), device_id_type=MESH)

    def pump(w, d, c, kind=None):
        for to_right in (True, False):
            s = f - d if to_right else f + d
            more = to_right_ok(w) if to_right else to_left_ok(w)
            here = (s >= 0) & (s < F)
            if w in ("up", "dn"):
                here = here & mid_plane
            theirs = helper & (s == helped)
            if kind is not None:
                here = here & (theirs if kind == "relay" else ~theirs)
            spread = shared(w, s)
            if tuned and w == "dn" and c == ND - 1:
                spread = spread & (s > 0) & (s < F - 1)

            @pl.when(here)
            def _():
                z_copy(w, s, c, to_right).wait_recv()

                @pl.when(more)
                def _():
                    z_copy(w, s, c, to_right).start()

                @pl.when(spread)
                def _():
                    for k in range(1, G):
                        y_copy(w, s, c, k).start()

    def y_wait(w, s, c):
        for k in range(1, G):
            y_copy(w, s, c, k, lax.rem(g - k + G, G)).wait_recv()

    def y_wait_all(w):
        def body(i, _):
            s, c = i // pieces[w][1], lax.rem(i, pieces[w][1])

            @pl.when(s != f)
            def _():
                y_wait(w, s, c)
            return 0
        lax.fori_loop(0, F * pieces[w][1], body, 0)

    def local(w, index):
        cols, rows = pl.ds(mult(f * K, K), K), pl.ds(mult(f * K, K), K)
        dst = bufs[w][1].at[rows, :] if w in ("mi", "up") else bufs[w][1].at[:, cols]
        return pltpu.make_async_copy(bufs[w][0], dst, lsem.at[index])

    def peer(k):
        return lax.rem(t + k, T)

    def tp_copy(src, dst, send, recv, k):
        return pltpu.make_async_remote_copy(
            src_ref=src, dst_ref=dst, send_sem=send, recv_sem=recv,
            device_id=(g, f, peer(k)), device_id_type=MESH)

    def gather_copy(buf, sems, block, target):
        return pltpu.make_async_remote_copy(
            src_ref=buf.at[block], dst_ref=buf.at[block], send_sem=gs.at[sems[0]],
            recv_sem=sems[1].at[block], device_id=(g, f, target), device_id_type=MESH)

    def gather_start(buf, sems):
        for k in range(2, T, 2):
            gather_copy(buf, sems, t, peer(k)).start()
        gather_copy(buf, sems, t, sibling).start()

    def gather_finish(buf, sems):
        for k in range(2, T, 2):
            block = lax.rem(t - k + T, T)
            gather_copy(buf, sems, block, sibling).wait_recv()
            gather_copy(buf, sems, block, sibling).start()
        for k in range(0, T, 2):
            block = lax.rem(sibling - k + T, T)
            gather_copy(buf, sems, block, sibling).wait_recv()

    def gather_drain(buf, sems):
        sent = buf.at[pl.ds(0, T - 1)]
        pltpu.make_async_remote_copy(
            src_ref=sent, dst_ref=sent, send_sem=gs.at[sems[0]], recv_sem=sems[1].at[0],
            device_id=(g, f, sibling), device_id_type=MESH).wait_send()

    own_rows, end_rows = g2.at[0], g2.at[1]
    sems1, sems2, sems3 = (0, g1r), (1, g2r), (2, g3r)

    def end_copy():
        return pltpu.make_async_remote_copy(
            src_ref=g2.at[0, t], dst_ref=g2.at[1, t], send_sem=es.at[0], recv_sem=er.at[0],
            device_id=(g, inner, t), device_id_type=MESH)

    def swap1(j):
        cols = pl.ds(j * step, step)
        return pltpu.make_async_remote_copy(
            src_ref=sp1.at[1 - place, :, :, cols], dst_ref=rq1.at[:, :, cols],
            send_sem=w1s.at[0], recv_sem=w1r.at[j], device_id=(g, f, sibling), device_id_type=MESH)

    def part1(k):
        return tp_copy(sp1.at[place, peer(k) // 2], rp1.at[k // 2 - 1],
                       p1s.at[k // 2 - 1], p1r.at[k // 2 - 1], k)

    def columns(s, c, n):
        return pl.ds(mult(s * K + c * cd, cd), n * cd)

    def swap2(i, s, c, n):
        return pltpu.make_async_remote_copy(
            src_ref=sp2.at[i, 1 - place, :, :, columns(s, c, n)], dst_ref=rq2.at[i, :, :, columns(s, c, n)],
            send_sem=w2s.at[i], recv_sem=w2r.at[i, s, c],
            device_id=(g, f, sibling), device_id_type=MESH)

    def part2(s, c, n, k):
        return tp_copy(sp2.at[0, place, peer(k) // 2, :, columns(s, c, n)], rp2.at[k // 2, :, columns(s, c, n)],
                       p2s.at[k // 2 - 1], p2r.at[k // 2], k)

    def part3(s, c, n, k):
        return pltpu.make_async_remote_copy(
            src_ref=sp2.at[1, place, peer(k) // 2, :, columns(s, c, n)], dst_ref=rp2.at[k // 2, :, columns(s, c, n)],
            send_sem=p3s.at[k // 2], recv_sem=p2r.at[k // 2],
            device_id=(g, helped, peer(k)), device_id_type=MESH)

    def merge(a, b):
        return (a.astype(jnp.float32) + b.astype(jnp.float32)).astype(jnp.bfloat16)

    loads = [pltpu.make_async_copy(a, b, lsem.at[4 + i])
             for i, (a, b) in enumerate(((tok_h, tok), (gains_h, gains), (scale_h, scale)))]
    local("mi", 0).start()
    local("mo", 1).start()
    for load in loads:
        load.start()
    local("up", 2).start()
    local("dn", 3).start()

    barrier = pltpu.get_barrier_semaphore()

    @pl.when(f + 1 < F)
    def _():
        pl.semaphore_signal(barrier, inc=1, device_id=(g, f + 1, t), device_id_type=MESH)

    @pl.when(f > 0)
    def _():
        pl.semaphore_signal(barrier, inc=1, device_id=(g, f - 1, t), device_id_type=MESH)

    for k in range(1, G):
        pl.semaphore_signal(barrier, inc=1, device_id=(lax.rem(g + k, G), f, t), device_id_type=MESH)
    for k in range(1, T):
        pl.semaphore_signal(barrier, inc=1, device_id=(g, f, peer(k)), device_id_type=MESH)
    greeted = jnp.where(f + 1 < F, 1, 0) + jnp.where(f > 0, 1, 0) + (G - 1 + T - 1)
    pl.semaphore_wait(barrier, greeted)

    local("mi", 0).wait()
    send_own("mi", 0)
    local("mo", 1).wait()
    send_own("mo", 0)
    local("up", 2).wait()
    send_own("up", 0)

    @pl.when(~mid_plane)
    def _():
        for c in range(1, NU):
            send_own("up", c)
    send_whole("up")
    for load in loads:
        load.wait()
    g1[t] = normalize(tok[...], gains[0:1, :]).astype(jnp.bfloat16)
    gather_start(g1, sems1)
    local("dn", 3).wait()

    for d in range(1, F):
        for kind in ("near", "relay"):
            if kind == "near" or (off and d == 1):
                pump("mi", d, 0, kind)
                pump("mo", d, 0, kind)
        if d < NU:
            @pl.when(mid_plane)
            def _():
                send_own("up", d)

    @pl.when(mid_plane)
    def _():
        for c in range(F, NU):
            send_own("up", c)

    for c in range(NU // 2):
        pump("up", 1, c)

    y_wait_all("mi")
    gather_finish(g1, sems1)
    mixed_in = jnp.dot(g1[...].reshape(T * R, D), mi[...],
                       preferred_element_type=jnp.float32).astype(jnp.bfloat16)
    scaled = (pooling(mixed_in, t * PWt, PWt * T // GROUPS) * scale[...]).astype(jnp.bfloat16)
    y_wait_all("mo")
    for j in range(4):
        cols = pl.ds(j * step, step)
        value = jnp.dot(scaled, mo[:, cols], preferred_element_type=jnp.float32
                        ).astype(jnp.bfloat16).reshape(half_t, 2, R, step)
        for q in range(2):
            sp1[q, :, :, cols] = value[:, q]
        swap1(j).start()
    for j in range(4):
        cols = pl.ds(j * step, step)
        swap1(j).wait_recv()
        sp1[place, :, :, cols] = merge(sp1[place, :, :, cols], rq1[:, :, cols])
    for k in range(2, T, 2):
        part1(k).start()

    def pump_all(w, d, start=0):
        def body(c, _):
            pump(w, d, c)
            return 0
        lax.fori_loop(start, pieces[w][1], body, 0)

    pump_all("up", 1, NU // 2)
    early = far <= 2

    @pl.when(mid_plane & early)
    def _():
        for c in range(ND):
            send_own("dn", c)

    total = sp1[place, t // 2].astype(jnp.float32)
    for k in range(2, T, 2):
        part1(k).wait_recv()
        total = total + rp1[k // 2 - 1].astype(jnp.float32)
    mixer_out = total.astype(jnp.bfloat16)
    middle = (tok[...].astype(jnp.float32) + normalize(mixer_out, gains[1:2, :])).astype(jnp.bfloat16)
    mid[...] = middle
    g2[0, t] = normalize(middle, gains[2:3, :]).astype(jnp.bfloat16)

    @pl.when(mid_plane)
    def _():
        gather_start(own_rows, sems2)
    if off:
        @pl.when(end)
        def _():
            end_copy().start()

    def pump_mid(d, _):
        pump_all("up", d)
        return 0
    lax.fori_loop(2, far, pump_mid, 0)

    @pl.when(~(mid_plane & early))
    def _():
        for c in range(ND):
            send_own("dn", c)
    send_whole("dn")
    if far > 1:
        pump_all("up", far)

    def up_project(i, c):
        cols = pl.ds(mult(c * cu, cu), cu)
        pre = jnp.dot(g2[i].reshape(T * R, D), up[:, cols], preferred_element_type=jnp.float32)
        pre = jnp.maximum(pre, 0.0)
        hid[i, :, cols] = (pre * pre).astype(jnp.bfloat16)

    half_u, half_d = NU // 2, (ND + 1) // 2
    turn = max(half_u - 1, 0)
    soon = [c for c in range(half_d) if half_u + c < NU]
    if off and half_d < ND:
        soon.append(half_d)
    later = [c for c in range(ND) if c not in soon]

    def act(todo):
        for what, d, c in todo:
            if what == "pass":
                y_wait("dn", helped, ND - 1)
                for k in range(1, G):
                    pass_on(k).start()
            else:
                pump("dn", d, c, what)

    up_acts = {2: [("near", 1, 0)], 3: [("near", 1, 1), ("relay", 1, 0), ("near", 1, 2)], 5: [("relay", 1, 1)],
               6: [("near", 1, 3)], 7: [("relay", 1, 2)]}

    def scheduled(acts, n):
        for index, todo in acts.items():
            @pl.when(n == index)
            def _():
                act(todo)

    def up_step(j, _):
        i, c = j // NU, lax.rem(j, NU)

        @pl.when(i == 0)
        def _():
            def landed_rows(s, _):
                @pl.when(s != f)
                def _():
                    y_wait("up", s, c)
                return 0
            lax.fori_loop(0, F, landed_rows, 0)
        if off:
            @pl.when(helper & (i == 1) & (c == 0))
            def _():
                gather_finish(end_rows, sems3)

        @pl.when((i == 0) | helper)
        def _():
            up_project(i, c)
        if off:
            @pl.when(helper & (i == 0) & (c == turn))
            def _():
                end_copy().wait_recv()
                gather_start(end_rows, sems3)
        if tuned:
            scheduled(up_acts, j)
            return 0
        first_pass = (i == 0) & (c >= half_u) & (c - half_u < half_d)
        second_pass = (i == 1) & (c == turn) & (half_d < ND)

        @pl.when(first_pass | second_pass)
        def _():
            pump("dn", 1, jnp.where(i == 0, c - half_u, half_d))
        return 0

    def project(i, s, first, n):
        cols = columns(s, first, n)
        value = jnp.dot(hid[i], dn[:, cols], preferred_element_type=jnp.float32
                        ).astype(jnp.bfloat16).reshape(half_t, 2, R, n * cd)
        for q in range(2):
            sp2[i, q, :, :, cols] = value[:, q]
        swap2(i, s, first, n).start()

    def finish(i, s, first, n):
        cols = columns(s, first, n)
        swap2(i, s, first, n).wait_recv()
        sp2[i, place, :, :, cols] = merge(sp2[i, place, :, :, cols], rq2[i, :, :, cols])

        @pl.when(i == 0)
        def _():
            for k in range(2, T, 2):
                part2(s, first, n, k).start()
        if off:
            @pl.when(i == 1)
            def _():
                for k in range(0, T, 2):
                    part3(s, first, n, k).start()

    def project_pair(i, left, right):
        cols = [columns(s, c, 1) for s, c in (left, right)]
        both = jnp.concatenate([dn[:, col] for col in cols], axis=1)
        value = jnp.dot(hid[i], both, preferred_element_type=jnp.float32).astype(jnp.bfloat16)
        for j, (s, c) in enumerate((left, right)):
            part = value[:, j * cd:(j + 1) * cd].reshape(half_t, 2, R, cd)
            for q in range(2):
                sp2[i, q, :, :, cols[j]] = part[:, q]
            swap2(i, s, c, 1).start()

    OWN, NEAR, HELPED, FAR = range(4)
    codes, before, PAIR = [], {}, 64 * ND

    def queue(kind, who, c, n, rows=(1, 0), wait=True):
        for i in rows:
            fresh = kind == 0 and wait and who != OWN and i == rows[0]
            codes.append(kind + 2 * (n - 1) + 4 * i + 8 * fresh + 16 * who + 64 * c)

    def queue_pair(i, fresh):
        codes.append(4 * i + 8 * fresh + 16 * FAR + 64 * (ND - 1) + PAIR)

    def also(*todo):
        before.setdefault(len(codes), []).extend(todo)

    if tuned:
        queue(0, OWN, 0, 2)
        queue(0, OWN, 2, 2)
        queue(1, OWN, 0, 2)
        also(("relay", 1, 3), ("near", 2, 0))
        queue(1, OWN, 2, 2)
        queue(0, NEAR, 0, 2)
        also(("near", 2, 1))
        queue(1, NEAR, 0, 2)
        queue(0, NEAR, 2, 2)
        also(("pass", 0, 0))
        queue(1, NEAR, 2, 2)
        also(("near", 2, 2))
        queue(0, HELPED, 2, 2)
        queue(0, FAR, 0, 1)
        queue(1, HELPED, 2, 2)
        queue(1, FAR, 0, 1)
        queue(0, FAR, 1, 1, (1,))
        also(("near", 2, 3))
        queue(0, HELPED, 0, 1, (1,))
        queue(0, FAR, 1, 1, (0,), False)
        queue(1, FAR, 1, 1, (1,))
        queue(0, HELPED, 0, 1, (0,), False)
        queue(1, HELPED, 0, 1, (1,))
        queue(1, FAR, 1, 1, (0,))
        queue(0, FAR, 2, 1, (1,))
        queue(1, HELPED, 0, 1, (0,))
        queue_pair(1, True)
        queue(1, FAR, 2, 1, (1,))
        queue(0, FAR, 2, 1, (0,), False)
        queue(1, FAR, 3, 1, (1,))
        queue(1, HELPED, 1, 1, (1,))
        queue_pair(0, False)
        queue(1, FAR, 2, 1, (0,))
        queue(1, FAR, 3, 1, (0,))
        queue(1, HELPED, 1, 1, (0,))

    def choose(n, values):
        out = jnp.int32(values[0])
        for index, value in enumerate(values[1:]):
            out = jnp.where(n == index + 1, value, out)
        return out

    def dn_op(n, _):
        scheduled(before, n)
        code = choose(n, codes)
        pair = code >= PAIR
        code = lax.rem(code, PAIR)
        kind, size, i = lax.rem(code, 2), lax.rem(code // 2, 2) + 1, lax.rem(code // 4, 2)
        fresh, who, first = lax.rem(code // 8, 2), lax.rem(code // 16, 4), code // 64
        s = jnp.where(who == OWN, f, jnp.where(who == NEAR, F - 1 - f, jnp.where(who == HELPED, helped, F - 1 - helped)))
        for c in range(2):
            passed = (who == HELPED) & (first + c == ND - 1)

            @pl.when((fresh == 1) & (c < size) & ~passed)
            def _():
                y_wait("dn", s, first + c)

        @pl.when((fresh == 1) & pair)
        def _():
            y_wait("dn", helped, 1)

        @pl.when(pair)
        def _():
            project_pair(i, (s, first), (helped, 1))
        for width in (1, 2):
            @pl.when((kind == 0) & (size == width) & ~pair)
            def _():
                project(i, s, first, width)

            @pl.when((kind == 1) & (size == width))
            def _():
                finish(i, s, first, width)
        return 0

    slots = (far + 1) * NB

    def dn_step(n, _):
        def one(now, _):
            m = n - 1 + now
            slot, q = m // 2, lax.rem(m, 2)
            d, first = slot // NB, lax.rem(slot, NB) * UD
            last = helper & (d == far)
            s = jnp.where(q == 0, f - d, f + d)
            s = jnp.where(last, jnp.where(q == 0, F - 1 - helped, helped), s)
            wanted = ((m >= 0) & (slot < slots) & (s >= 0) & (s < F) & ((q == 0) | (d > 0))
                      & (last | ~(helper & (s == helped))))

            @pl.when(wanted & (now == 1) & (s != f))
            def _():
                for c in range(UD):
                    y_wait("dn", s, first + c)

            def rows(i, _):
                @pl.when(wanted & (now == 0))
                def _():
                    finish(i, s, first, UD)

                @pl.when(wanted & (now == 1))
                def _():
                    project(i, s, first, UD)
                return 0
            lax.fori_loop(0, jnp.where(helper, 2, 1), rows, 0)
            return 0
        lax.fori_loop(0, 2, one, 0)
        slot = n // 2

        @pl.when(n == 2 * NB - 1)
        def _():
            for c in later:
                pump("dn", 1, c)

        @pl.when((lax.rem(n, 2) == 1) & (slot >= NB) & (slot < far * NB))
        def _():
            for c in range(UD):
                pump("dn", slot // NB + 1, lax.rem(slot, NB) * UD + c)
        return 0

    @pl.when(mid_plane)
    def _():
        gather_finish(own_rows, sems2)
        lax.fori_loop(0, (2 if off else 1) * NU, up_step, 0)
        if tuned:
            lax.fori_loop(0, len(codes), dn_op, 0)
        else:
            lax.fori_loop(0, 2 * slots + 1, dn_step, 0)

    def landed(k):
        return tp_copy(rp2.at[k // 2], rp2.at[k // 2], p2s.at[0], p2r.at[k // 2], 2)

    for k in range(2, T, 2):
        landed(k).wait_recv()
    if off:
        @pl.when(end)
        def _():
            landed(0).wait_recv()

    @pl.when(mid_plane)
    def _():
        rp2[0] = sp2[0, place, t // 2]
    total = jnp.zeros((R, D), jnp.float32)
    for k in range(half_t):
        total = total + rp2[k].astype(jnp.float32)
    channel_out = total.astype(jnp.bfloat16)
    out[...] = (mid[...].astype(jnp.float32) + normalize(channel_out, gains[3:4, :])).astype(jnp.bfloat16)

    def sent(kind, sem):
        rows = (mi if kind == 0 else up).at[pl.ds(0, 2 * (K // G)), :]
        pltpu.make_async_remote_copy(
            src_ref=rows, dst_ref=rows, send_sem=sem, recv_sem=zr.at[0, 0],
            device_id=(g, f, sibling), device_id_type=MESH).wait_send()

    def swapped(buf, sem):
        pltpu.make_async_remote_copy(
            src_ref=buf, dst_ref=buf, send_sem=sem, recv_sem=w1r.at[0],
            device_id=(g, f, sibling), device_id_type=MESH).wait_send()

    for kind, w in ((0, "mi"), (1, "up")):
        def drain(s, _):
            moved = True if kind == 0 else (mid_plane | (s == f))

            @pl.when((s <= f) & to_right_ok(w) & moved)
            def _():
                sent(kind, zs.at[0, kind, s])

            @pl.when((s >= f) & to_left_ok(w) & moved)
            def _():
                sent(kind, zs.at[1, kind, s])

            gone = (s != f) & moved & shared(w, s)
            ends = (s == 0) | (s == F - 1) if tuned and kind == 1 else s < 0

            @pl.when(gone & ~ends)
            def _():
                for k in range(1, G):
                    sent(kind, ys.at[k - 1, kind, s])
            if tuned and kind == 1:
                @pl.when(gone & ends)
                def _():
                    for k in range(1, G):
                        swapped(up.at[pl.ds(0, 2 * (K // G) - cd // G), :], ys.at[k - 1, kind, s])

                @pl.when(helper & (s == helped))
                def _():
                    for k in range(1, G):
                        swapped(view("dn", 0, 0, 0), ys.at[k - 1, kind, s])
            if off and kind == 1:
                @pl.when((s == f) & end)
                def _():
                    for k in range(1, G):
                        sent(kind, ys.at[k - 1, kind, s])
            return 0
        lax.fori_loop(0, F, drain, 0)

    @pl.when(mid_plane)
    def _():
        swapped(rq2.at[0], w2s.at[0])
        for k in range(2, T, 2):
            swapped(rp2.at[0], p2s.at[k // 2 - 1])
        gather_drain(own_rows, sems2)
        if off:
            @pl.when(helper)
            def _():
                gather_drain(end_rows, sems3)
                swapped(rq2.at[1], w2s.at[1])
                for k in range(0, T, 2):
                    swapped(rp2.at[0], p3s.at[k // 2])
    if off:
        @pl.when(end)
        def _():
            end_copy().wait_send()
    gather_drain(g1, sems1)
    swapped(rq1, w1s.at[0])
    for k in range(2, T, 2):
        part1(k).wait_send()


def local_layer(sizes, tokens, mix_in, scale, mix_out, up_w, down_w, gains):
    G, F, T = sizes
    R, D = tokens.shape
    K, PWt = mix_in.shape
    Ht = up_w.shape[1]
    NU = max(1, min(4, Ht // 256))
    ND = max(1, min(4, K // 128))
    dims = (G, F, T, R, D, K, PWt, Ht, NU, ND)
    NP = 2 + NU + ND
    H = T // 2
    vmem, hbm = pl.BlockSpec(memory_space=pltpu.VMEM), pl.BlockSpec(memory_space=pl.ANY)
    bf, dma = jnp.bfloat16, pltpu.SemaphoreType.DMA
    return pl.pallas_call(
        functools.partial(kernel, dims),
        out_shape=pltpu.VMEM((R, D), bf),
        in_specs=[hbm] * 7,
        out_specs=vmem,
        scratch_shapes=[
            pltpu.VMEM((R, D), bf), pltpu.VMEM(gains.shape, jnp.float32), pltpu.VMEM((1, PWt), jnp.float32),
            pltpu.VMEM((D, PWt), bf), pltpu.VMEM((PWt, D), bf),
            pltpu.VMEM((D, Ht), bf), pltpu.VMEM((Ht, D), bf),
            pltpu.VMEM((T, R, D), bf), pltpu.VMEM((2, T, R, D), bf),
            pltpu.VMEM((2, T * R, Ht), bf),
            pltpu.VMEM((2, H, R, D), bf), pltpu.VMEM((H, R, D), bf), pltpu.VMEM((H - 1, R, D), bf),
            pltpu.VMEM((2, 2, H, R, D), bf), pltpu.VMEM((2, H, R, D), bf), pltpu.VMEM((H, R, D), bf),
            pltpu.VMEM((R, D), bf),
            dma((7,)), dma((2, 2, F)), dma((F - 1, NP)),
            dma((G - 1, 2, F)), dma((G - 1, F - 1, NP)),
            dma((3,)), dma((T,)), dma((T,)), dma((T,)),
            dma((1,)), dma((1,)),
            dma((1,)), dma((4,)), dma((2,)), dma((2, F, ND)),
            dma((H - 1,)), dma((H - 1,)),
            dma((H - 1,)), dma((H,)), dma((H,)),
        ],
        compiler_params=pltpu.CompilerParams(
            collective_id=0, has_side_effects=True, vmem_limit_bytes=63 * 1024 * 1024),
    )(tokens, gains, scale.reshape(1, PWt), mix_in, mix_out, up_w, down_w)


def solution(mesh):
    sizes = tuple(mesh.shape[name] for name in ("grp", "fs", "tp"))
    return jax.shard_map(
        functools.partial(local_layer, sizes),
        mesh=mesh,
        in_specs=(
            P(("grp", "fs", "tp"), None),
            P("fs", "tp"),
            P("tp"),
            P("tp", "fs"),
            P("fs", "tp"),
            P("tp", "fs"),
            P(),
        ),
        out_specs=P(("grp", "fs", "tp"), None),
        check_vma=False,
    )
```

```python
import functools

import jax
import jax.numpy as jnp
from jax import lax
from jax.experimental import pallas as pl
from jax.experimental.pallas import tpu as pltpu
from jax.sharding import PartitionSpec as P

GROUPS = 4
EPS = 1e-06
MESH = pl.DeviceIdType.MESH


def normalize(values, gain):
    upcast = values.astype(jnp.float32)
    return upcast * lax.rsqrt(jnp.mean(upcast * upcast, axis=-1, keepdims=True) + EPS) * gain


def pooling(mixed_in, first_channel, group_width):
    length, width = mixed_in.shape
    upcast = mixed_in.astype(jnp.float32)
    row = lax.broadcasted_iota(jnp.int32, (length, width), 0)
    group = (first_channel + lax.broadcasted_iota(jnp.int32, (length, width), 1)) // group_width
    position = (row + 1).astype(jnp.float32)
    total, average = upcast, jnp.zeros_like(upcast)
    for index in range(GROUPS):
        step = 1 << index
        total = total + jnp.where(row >= step, pltpu.roll(total, step, axis=0), 0.0)
        mean = total / jnp.minimum(position, float(2 * step))
        average = jnp.where(group == index, mean, average)
    return average - upcast


def kernel(dims, tok_h, gains_h, scale_h, mi_h, mo_h, up_h, dn_h, out,
           tok, gains, scale, mi, mo, up, dn, g1, g2, hid, sp1, rq1, rp1, sp2, rq2, rp2, mid,
           lsem, zs, zr, ys, yr, gs, g1r, g2r, g3r, es, er,
           w1s, w1r, w2s, w2r, p1s, p1r, p2s, p2r, p3s):
    G, F, T, R, D, K, PWt, Ht, NU, ND, NP = dims
    g, f, t = lax.axis_index("grp"), lax.axis_index("fs"), lax.axis_index("tp")
    cu, cd = Ht // NU, K // ND
    UD = 1 if ND % 2 else 2
    NB = ND // UD
    off = F >= 4
    tuned = F == 4 and NU == 4 and ND == 4
    far = F - 2 if off else F - 1
    first, last = (1, F - 2) if off else (0, F - 1)
    mid_plane = (f >= first) & (f <= last)
    end = (f < first) | (f > last)
    helper = (f == 1) | (f == F - 2) if off else f < 0
    helped = jnp.where(f == 1, 0, F - 1)
    inner = jnp.where(f == 0, 1, F - 2)
    sibling = t + 1 - 2 * lax.rem(t, 2)
    place, half_t = lax.rem(t, 2), T // 2
    step = D // 4

    def to_right_ok(w):
        return f + 1 < F if w in ("mi", "mo") else (f + 1 <= last)

    def to_left_ok(w):
        return f > 0 if w in ("mi", "mo") else (f - 1 >= first)

    def shared(w, s):
        return True if w in ("mi", "mo") or not off else ~(helper & (s == helped))
    NM = 1
    pieces = {"mi": (0, NM), "mo": (NM, 1), "up": (NM + 1, NU), "dn": (NM + 1 + NU, ND)}
    kinds = {"mi": 0, "mo": 0, "up": 1, "dn": 1}
    bufs = {"mi": (mi_h, mi), "mo": (mo_h, mo), "up": (up_h, up), "dn": (dn_h, dn)}

    def slot_of(s, where):
        return s - jnp.where(s > where, 1, 0)

    def zsem(side, kind, s):
        return zs.at[side, 0, 0] if tuned else zs.at[side, kind, s]

    def ysem(k, kind, s):
        return ys.at[k - 1, 0, 0] if tuned else ys.at[k - 1, kind, s]

    def yrsem(k, w, s, c, where):
        slot = slot_of(s, where)
        if not tuned:
            return yr.at[k - 1, slot * NP + pieces[w][0] + c]
        base = {"mi": 0, "mo": 1, "up": 2, "dn": 2 + NU + slot * ND}[w]
        return yr.at[k - 1, base + c]

    def mult(value, by):
        return pl.multiple_of(value, by)

    def span(w, s, c, half):
        base = s * K
        if w == "mi":
            size = K // G // NM
            return pl.ds(mult(base + (half * NM + c) * size, size), size), pl.ds(0, PWt)
        if w == "mo":
            return pl.ds(mult(half * (PWt // G), PWt // G), PWt // G), pl.ds(mult(base, 128), K)
        if w == "up":
            return pl.ds(mult(base + half * (K // G), K // G), K // G), pl.ds(mult(c * cu, cu), cu)
        return pl.ds(mult(half * (Ht // G), Ht // G), Ht // G), pl.ds(mult(base + c * cd, cd), cd)

    def view(w, s, c, half):
        return bufs[w][1].at[span(w, s, c, half)]

    def z_copy(w, s, c, to_right):
        p = pieces[w][0] + c
        target = f + 1 if to_right else f - 1
        side = 0 if to_right else 1
        return pltpu.make_async_remote_copy(
            src_ref=view(w, s, c, g), dst_ref=view(w, s, c, g), send_sem=zsem(side, kinds[w], s), recv_sem=zr.at[s - side, p],
            device_id=(g, target, t), device_id_type=MESH)

    def y_copy(w, s, c, k, half=None):
        half = g if half is None else half
        return pltpu.make_async_remote_copy(
            src_ref=view(w, s, c, half), dst_ref=view(w, s, c, half),
            send_sem=ysem(k, kinds[w], s), recv_sem=yrsem(k, w, s, c, f),
            device_id=(lax.rem(g + k, G), f, t), device_id_type=MESH)

    def send_own(w, c):
        @pl.when(to_right_ok(w))
        def _():
            z_copy(w, f, c, True).start()

        @pl.when(to_left_ok(w))
        def _():
            z_copy(w, f, c, False).start()

    def whole_copy(w, c, k):
        half = lax.rem(g - k + G, G)
        return pltpu.make_async_remote_copy(
            src_ref=view(w, f, c, half), dst_ref=view(w, f, c, half),
            send_sem=ysem(k, kinds[w], f), recv_sem=yrsem(k, w, f, c, inner),
            device_id=(g, inner, t), device_id_type=MESH)

    def send_whole(w):
        if off:
            order = list(range(pieces[w][1]))
            if tuned and w == "dn":
                order = order[:1:-1] + order[:2]

            @pl.when(end)
            def _():
                for c in order:
                    for k in range(1, G):
                        whole_copy(w, c, k).start()

    def pass_on(k):
        half = lax.rem(g - k + G, G)
        block = view("dn", helped, ND - 1, half)
        return pltpu.make_async_remote_copy(
            src_ref=block, dst_ref=block, send_sem=ysem(k, 1, helped), recv_sem=yrsem(k, "dn", helped, ND - 1, F - 1 - f),
            device_id=(g, F - 1 - f, t), device_id_type=MESH)

    def pump(w, d, c, kind=None):
        for to_right in (True, False):
            s = f - d if to_right else f + d
            more = to_right_ok(w) if to_right else to_left_ok(w)
            here = (s >= 0) & (s < F)
            if w in ("up", "dn"):
                here = here & mid_plane
            theirs = helper & (s == helped)
            if kind is not None:
                here = here & (theirs if kind == "relay" else ~theirs)
            spread = shared(w, s)
            if tuned and w == "dn" and c == ND - 1:
                spread = spread & (s > 0) & (s < F - 1)

            @pl.when(here)
            def _():
                z_copy(w, s, c, to_right).wait_recv()

                @pl.when(more)
                def _():
                    z_copy(w, s, c, to_right).start()

                @pl.when(spread)
                def _():
                    for k in range(1, G):
                        y_copy(w, s, c, k).start()

    def y_wait(w, s, c):
        for k in range(1, G):
            y_copy(w, s, c, k, lax.rem(g - k + G, G)).wait_recv()

    def y_wait_rows(w, c):
        size, cols = (F - 1) * (K // G), pl.ds(0, PWt)
        if w == "mo":
            size, cols = PWt // G, pl.ds(0, (F - 1) * K)
        if w == "up":
            cols = pl.ds(mult(c * cu, cu), cu)
        rows = bufs[w][1].at[pl.ds(0, size), cols]
        for k in range(1, G):
            pltpu.make_async_remote_copy(
                src_ref=rows, dst_ref=rows, send_sem=ysem(k, 0, 0), recv_sem=yrsem(k, w, 0, c, f),
                device_id=(lax.rem(g + k, G), f, t), device_id_type=MESH).wait_recv()

    def y_wait_all(w):
        if tuned:
            y_wait_rows(w, 0)
            return

        def body(i, _):
            s, c = i // pieces[w][1], lax.rem(i, pieces[w][1])

            @pl.when(s != f)
            def _():
                y_wait(w, s, c)
            return 0
        lax.fori_loop(0, F * pieces[w][1], body, 0)

    def local(w, index):
        cols, rows = pl.ds(mult(f * K, K), K), pl.ds(mult(f * K, K), K)
        dst = bufs[w][1].at[rows, :] if w in ("mi", "up") else bufs[w][1].at[:, cols]
        return pltpu.make_async_copy(bufs[w][0], dst, lsem.at[index])

    def peer(k):
        return lax.rem(t + k, T)

    def tp_copy(src, dst, send, recv, k):
        return pltpu.make_async_remote_copy(
            src_ref=src, dst_ref=dst, send_sem=send, recv_sem=recv,
            device_id=(g, f, peer(k)), device_id_type=MESH)

    def gather_copy(buf, sems, block, target):
        return pltpu.make_async_remote_copy(
            src_ref=buf.at[block], dst_ref=buf.at[block], send_sem=gs.at[sems[0]],
            recv_sem=sems[1].at[block], device_id=(g, f, target), device_id_type=MESH)

    def gather_start(buf, sems):
        for k in range(2, T, 2):
            gather_copy(buf, sems, t, peer(k)).start()
        gather_copy(buf, sems, t, sibling).start()

    def gather_finish(buf, sems):
        for k in range(2, T, 2):
            block = lax.rem(t - k + T, T)
            gather_copy(buf, sems, block, sibling).wait_recv()
            gather_copy(buf, sems, block, sibling).start()
        for k in range(0, T, 2):
            block = lax.rem(sibling - k + T, T)
            gather_copy(buf, sems, block, sibling).wait_recv()

    def gather_drain(buf, sems):
        sent = buf.at[pl.ds(0, T - 1)]
        pltpu.make_async_remote_copy(
            src_ref=sent, dst_ref=sent, send_sem=gs.at[sems[0]], recv_sem=sems[1].at[0],
            device_id=(g, f, sibling), device_id_type=MESH).wait_send()

    own_rows, end_rows = g2.at[0], g2.at[1]
    sems1, sems2, sems3 = (0, g1r), (1, g2r), (2, g3r)

    def end_copy():
        return pltpu.make_async_remote_copy(
            src_ref=g2.at[0, t], dst_ref=g2.at[1, t], send_sem=es.at[0], recv_sem=er.at[0],
            device_id=(g, inner, t), device_id_type=MESH)

    def swap1(j):
        cols = pl.ds(j * step, step)
        return pltpu.make_async_remote_copy(
            src_ref=sp1.at[1 - place, :, :, cols], dst_ref=rq1.at[:, :, cols],
            send_sem=w1s.at[0], recv_sem=w1r.at[j], device_id=(g, f, sibling), device_id_type=MESH)

    def part1(k):
        return tp_copy(sp1.at[place, peer(k) // 2], rp1.at[k // 2 - 1],
                       p1s.at[k // 2 - 1], p1r.at[k // 2 - 1], k)

    def columns(s, c, n):
        return pl.ds(mult(s * K + c * cd, cd), n * cd)

    def swap_index(s, c):
        if not tuned:
            return s * ND + c
        base = jnp.where(s == f, 2 * ND - 1, 2 * ND + 1) + c // 2
        return jnp.where(s == helped, c, jnp.where(s == F - 1 - helped, ND - 1 + c, base))

    def swap2(i, s, c, n):
        return pltpu.make_async_remote_copy(
            src_ref=sp2.at[i, 1 - place, :, :, columns(s, c, n)], dst_ref=rq2.at[i, :, :, columns(s, c, n)],
            send_sem=w2s.at[i], recv_sem=w2r.at[i, swap_index(s, c)],
            device_id=(g, f, sibling), device_id_type=MESH)

    def part2(s, c, n, k):
        return tp_copy(sp2.at[0, place, peer(k) // 2, :, columns(s, c, n)], rp2.at[k // 2, :, columns(s, c, n)],
                       p2s.at[k // 2 - 1], p2r.at[k // 2], k)

    def part3(s, c, n, k):
        return pltpu.make_async_remote_copy(
            src_ref=sp2.at[1, place, peer(k) // 2, :, columns(s, c, n)], dst_ref=rp2.at[k // 2, :, columns(s, c, n)],
            send_sem=p3s.at[k // 2], recv_sem=p2r.at[k // 2],
            device_id=(g, helped, peer(k)), device_id_type=MESH)

    def merge(a, b):
        return (a.astype(jnp.float32) + b.astype(jnp.float32)).astype(jnp.bfloat16)

    loads = [pltpu.make_async_copy(a, b, lsem.at[4 + i])
             for i, (a, b) in enumerate(((tok_h, tok), (gains_h, gains), (scale_h, scale)))]
    local("mi", 0).start()
    local("mo", 1).start()
    for load in loads:
        load.start()
    local("up", 2).start()
    local("dn", 3).start()

    barrier = pltpu.get_barrier_semaphore()

    @pl.when(f + 1 < F)
    def _():
        pl.semaphore_signal(barrier, inc=1, device_id=(g, f + 1, t), device_id_type=MESH)

    @pl.when(f > 0)
    def _():
        pl.semaphore_signal(barrier, inc=1, device_id=(g, f - 1, t), device_id_type=MESH)

    for k in range(1, G):
        pl.semaphore_signal(barrier, inc=1, device_id=(lax.rem(g + k, G), f, t), device_id_type=MESH)
    for k in range(1, T):
        pl.semaphore_signal(barrier, inc=1, device_id=(g, f, peer(k)), device_id_type=MESH)
    greeted = jnp.where(f + 1 < F, 1, 0) + jnp.where(f > 0, 1, 0) + (G - 1 + T - 1)
    pl.semaphore_wait(barrier, greeted)

    local("mi", 0).wait()
    for c in range(NM):
        send_own("mi", c)
    local("mo", 1).wait()
    send_own("mo", 0)
    local("up", 2).wait()
    send_own("up", 0)

    @pl.when(~mid_plane)
    def _():
        for c in range(1, NU):
            send_own("up", c)
    send_whole("up")
    for load in loads:
        load.wait()
    g1[t] = normalize(tok[...], gains[0:1, :]).astype(jnp.bfloat16)
    gather_start(g1, sems1)
    local("dn", 3).wait()

    for d in range(1, F):
        for kind in ("near", "relay"):
            if kind == "near" or (off and d == 1):
                for c in range(NM):
                    pump("mi", d, c, kind)
                pump("mo", d, 0, kind)
        if d < NU:
            @pl.when(mid_plane)
            def _():
                send_own("up", d)
        if tuned and d == 1:
            pump("up", 1, 0, "near")

    @pl.when(mid_plane)
    def _():
        for c in range(F, NU):
            send_own("up", c)

    for c in range(NU // 2):
        pump("up", 1, c, "relay" if tuned and c == 0 else None)

    y_wait_all("mi")
    gather_finish(g1, sems1)
    mixed_in = jnp.dot(g1[...].reshape(T * R, D), mi[...],
                       preferred_element_type=jnp.float32).astype(jnp.bfloat16)
    scaled = (pooling(mixed_in, t * PWt, PWt * T // GROUPS) * scale[...]).astype(jnp.bfloat16)
    y_wait_all("mo")
    if tuned:
        pump("up", 1, NU // 2)
    for j in range(4):
        cols = pl.ds(j * step, step)
        value = jnp.dot(scaled, mo[:, cols], preferred_element_type=jnp.float32
                        ).astype(jnp.bfloat16).reshape(half_t, 2, R, step)
        for q in range(2):
            sp1[q, :, :, cols] = value[:, q]
        swap1(j).start()
    for j in range(4):
        cols = pl.ds(j * step, step)
        swap1(j).wait_recv()
        sp1[place, :, :, cols] = merge(sp1[place, :, :, cols], rq1[:, :, cols])
    for k in range(2, T, 2):
        part1(k).start()

    def pump_all(w, d, start=0):
        def body(c, _):
            pump(w, d, c)
            return 0
        lax.fori_loop(start, pieces[w][1], body, 0)

    pump_all("up", 1, NU // 2 + 1 if tuned else NU // 2)
    if tuned:
        pump("up", far, 0)
    early = far <= 2

    @pl.when(mid_plane & early)
    def _():
        for c in range(ND):
            send_own("dn", c)

    total = sp1[place, t // 2].astype(jnp.float32)
    for k in range(2, T, 2):
        part1(k).wait_recv()
        total = total + rp1[k // 2 - 1].astype(jnp.float32)
    mixer_out = total.astype(jnp.bfloat16)
    middle = (tok[...].astype(jnp.float32) + normalize(mixer_out, gains[1:2, :])).astype(jnp.bfloat16)
    mid[...] = middle
    g2[0, t] = normalize(middle, gains[2:3, :]).astype(jnp.bfloat16)

    @pl.when(mid_plane)
    def _():
        gather_start(own_rows, sems2)
    if off:
        @pl.when(end)
        def _():
            end_copy().start()

    def pump_mid(d, _):
        pump_all("up", d)
        return 0
    lax.fori_loop(2, far, pump_mid, 0)

    @pl.when(~(mid_plane & early))
    def _():
        for c in range(ND):
            send_own("dn", c)
    send_whole("dn")
    if far > 1:
        pump_all("up", far, 1 if tuned else 0)

    def up_project(i, c):
        cols = pl.ds(mult(c * cu, cu), cu)
        pre = jnp.dot(g2[i].reshape(T * R, D), up[:, cols], preferred_element_type=jnp.float32)
        pre = jnp.maximum(pre, 0.0)
        hid[i, :, cols] = (pre * pre).astype(jnp.bfloat16)

    half_u, half_d = NU // 2, (ND + 1) // 2
    turn = max(half_u - 1, 0)
    soon = [c for c in range(half_d) if half_u + c < NU]
    if off and half_d < ND:
        soon.append(half_d)
    later = [c for c in range(ND) if c not in soon]

    def act(todo):
        for what, d, c in todo:
            if what == "pass":
                y_wait("dn", helped, ND - 1)
                for k in range(1, G):
                    pass_on(k).start()
            else:
                pump("dn", d, c, what)

    up_acts = {2: [("near", 1, 0)], 3: [("near", 1, 1), ("relay", 1, 0), ("near", 1, 2)], 5: [("relay", 1, 1)],
               6: [("near", 1, 3)], 7: [("relay", 1, 2)]}

    def scheduled(acts, n):
        for index, todo in acts.items():
            @pl.when(n == index)
            def _():
                act(todo)

    def up_step(j, _):
        i, c = j // NU, lax.rem(j, NU)

        @pl.when(i == 0)
        def _():
            if tuned:
                y_wait_rows("up", c)
                return

            def landed_rows(s, _):
                @pl.when(s != f)
                def _():
                    y_wait("up", s, c)
                return 0
            lax.fori_loop(0, F, landed_rows, 0)
        if off:
            @pl.when(helper & (i == 1) & (c == 0))
            def _():
                gather_finish(end_rows, sems3)

        @pl.when((i == 0) | helper)
        def _():
            up_project(i, c)
        if off:
            @pl.when(helper & (i == 0) & (c == turn))
            def _():
                end_copy().wait_recv()
                gather_start(end_rows, sems3)
        if tuned:
            scheduled(up_acts, j)
            return 0
        first_pass = (i == 0) & (c >= half_u) & (c - half_u < half_d)
        second_pass = (i == 1) & (c == turn) & (half_d < ND)

        @pl.when(first_pass | second_pass)
        def _():
            pump("dn", 1, jnp.where(i == 0, c - half_u, half_d))
        return 0

    def project(i, s, first, n):
        cols = columns(s, first, n)
        value = jnp.dot(hid[i], dn[:, cols], preferred_element_type=jnp.float32
                        ).astype(jnp.bfloat16).reshape(half_t, 2, R, n * cd)
        for q in range(2):
            sp2[i, q, :, :, cols] = value[:, q]
        swap2(i, s, first, n).start()

    def finish(i, s, first, n):
        cols = columns(s, first, n)
        swap2(i, s, first, n).wait_recv()
        sp2[i, place, :, :, cols] = merge(sp2[i, place, :, :, cols], rq2[i, :, :, cols])

        @pl.when(i == 0)
        def _():
            for k in range(2, T, 2):
                part2(s, first, n, k).start()
        if off:
            @pl.when(i == 1)
            def _():
                for chip in range(half_t):
                    part3(s, first, n, lax.rem(2 * chip + place - t + T, T)).start()

    def project_pair(i, left, right):
        cols = [columns(s, c, 1) for s, c in (left, right)]
        both = jnp.concatenate([dn[:, col] for col in cols], axis=1)
        value = jnp.dot(hid[i], both, preferred_element_type=jnp.float32).astype(jnp.bfloat16)
        for j, (s, c) in enumerate((left, right)):
            part = value[:, j * cd:(j + 1) * cd].reshape(half_t, 2, R, cd)
            for q in range(2):
                sp2[i, q, :, :, cols[j]] = part[:, q]
            swap2(i, s, c, 1).start()

    OWN, NEAR, HELPED, FAR = range(4)
    codes, before, PAIR = [], {}, 64 * ND

    def queue(kind, who, c, n, rows=(1, 0), wait=True):
        for i in rows:
            fresh = kind == 0 and wait and who != OWN and i == rows[0]
            codes.append(kind + 2 * (n - 1) + 4 * i + 8 * fresh + 16 * who + 64 * c)

    def queue_pair(i, fresh):
        codes.append(4 * i + 8 * fresh + 16 * FAR + 64 * (ND - 1) + PAIR)

    def also(*todo):
        before.setdefault(len(codes), []).extend(todo)

    if tuned:
        queue(0, OWN, 0, 2)
        queue(0, OWN, 2, 2)
        queue(1, OWN, 0, 2)
        also(("near", 2, 0), ("relay", 1, 3))
        queue(1, OWN, 2, 2)
        queue(0, NEAR, 0, 2)
        also(("near", 2, 1))
        queue(1, NEAR, 0, 2)
        queue(0, NEAR, 2, 2)
        also(("pass", 0, 0))
        queue(1, NEAR, 2, 2)
        also(("near", 2, 2))
        queue(0, HELPED, 2, 2)
        queue(0, FAR, 0, 1)
        queue(1, HELPED, 2, 2)
        queue(1, FAR, 0, 1)
        queue(0, FAR, 1, 1, (1,))
        also(("near", 2, 3))
        queue(0, HELPED, 0, 1, (1,))
        queue(0, FAR, 1, 1, (0,), False)
        queue(1, FAR, 1, 1, (1,))
        queue(0, HELPED, 0, 1, (0,), False)
        queue(1, HELPED, 0, 1, (1,))
        queue(1, FAR, 1, 1, (0,))
        queue(1, HELPED, 0, 1, (0,))
        tails = []
        split = len(codes)
        for second in (False, True):
            if second:
                queue_pair(1, True)
                queue(0, FAR, 2, 1, (1,))
                queue_pair(0, False)
                queue(0, FAR, 2, 1, (0,), False)
                queue(1, FAR, 3, 1, (1,))
                queue(1, HELPED, 1, 1, (1,))
                queue(1, FAR, 2, 1, (1,))
            else:
                queue_pair(1, True)
                queue(0, FAR, 2, 1, (1,))
                queue(1, FAR, 3, 1, (1,))
                queue(1, HELPED, 1, 1, (1,))
                queue_pair(0, False)
                queue(1, FAR, 2, 1, (1,))
                queue(0, FAR, 2, 1, (0,), False)
            queue(1, FAR, 3, 1, (0,))
            queue(1, HELPED, 1, 1, (0,))
            queue(1, FAR, 2, 1, (0,))
            tails.append(codes[split:])
            del codes[split:]

    def choose(n, values):
        out = jnp.int32(values[0])
        for index, value in enumerate(values[1:]):
            out = jnp.where(n == index + 1, value, out)
        return out

    def dn_op(n, _):
        scheduled(before, n)
        code = jnp.where(place == 0, choose(n, codes + tails[0]), choose(n, codes + tails[1]))
        pair = code >= PAIR
        code = lax.rem(code, PAIR)
        kind, size, i = lax.rem(code, 2), lax.rem(code // 2, 2) + 1, lax.rem(code // 4, 2)
        fresh, who, first = lax.rem(code // 8, 2), lax.rem(code // 16, 4), code // 64
        s = jnp.where(who == OWN, f, jnp.where(who == NEAR, F - 1 - f, jnp.where(who == HELPED, helped, F - 1 - helped)))
        for c in range(2):
            passed = ((who == HELPED) & (first + c == ND - 1)) | pair

            @pl.when((fresh == 1) & (c < size) & ~passed)
            def _():
                y_wait("dn", s, first + c)

        @pl.when((fresh == 1) & pair)
        def _():
            y_wait("dn", helped, 1)
            y_wait("dn", s, ND - 1)

        @pl.when(pair)
        def _():
            project_pair(i, (s, first), (helped, 1))
        for width in (1, 2):
            @pl.when((kind == 0) & (size == width) & ~pair)
            def _():
                project(i, s, first, width)

            @pl.when((kind == 1) & (size == width))
            def _():
                finish(i, s, first, width)
        return 0

    slots = (far + 1) * NB

    def dn_step(n, _):
        def one(now, _):
            m = n - 1 + now
            slot, q = m // 2, lax.rem(m, 2)
            d, first = slot // NB, lax.rem(slot, NB) * UD
            last = helper & (d == far)
            s = jnp.where(q == 0, f - d, f + d)
            s = jnp.where(last, jnp.where(q == 0, F - 1 - helped, helped), s)
            wanted = ((m >= 0) & (slot < slots) & (s >= 0) & (s < F) & ((q == 0) | (d > 0))
                      & (last | ~(helper & (s == helped))))

            @pl.when(wanted & (now == 1) & (s != f))
            def _():
                for c in range(UD):
                    y_wait("dn", s, first + c)

            def rows(i, _):
                @pl.when(wanted & (now == 0))
                def _():
                    finish(i, s, first, UD)

                @pl.when(wanted & (now == 1))
                def _():
                    project(i, s, first, UD)
                return 0
            lax.fori_loop(0, jnp.where(helper, 2, 1), rows, 0)
            return 0
        lax.fori_loop(0, 2, one, 0)
        slot = n // 2

        @pl.when(n == 2 * NB - 1)
        def _():
            for c in later:
                pump("dn", 1, c)

        @pl.when((lax.rem(n, 2) == 1) & (slot >= NB) & (slot < far * NB))
        def _():
            for c in range(UD):
                pump("dn", slot // NB + 1, lax.rem(slot, NB) * UD + c)
        return 0

    @pl.when(mid_plane)
    def _():
        gather_finish(own_rows, sems2)
        lax.fori_loop(0, (2 if off else 1) * NU, up_step, 0)
        if tuned:
            lax.fori_loop(0, len(codes + tails[0]), dn_op, 0)
        else:
            lax.fori_loop(0, 2 * slots + 1, dn_step, 0)

    def landed(k):
        return tp_copy(rp2.at[k // 2], rp2.at[k // 2], p2s.at[0], p2r.at[k // 2], 2)

    for k in range(2, T, 2):
        landed(k).wait_recv()
    if off:
        @pl.when(end)
        def _():
            landed(0).wait_recv()

    @pl.when(mid_plane)
    def _():
        rp2[0] = sp2[0, place, t // 2]
    total = jnp.zeros((R, D), jnp.float32)
    for k in range(half_t):
        total = total + rp2[k].astype(jnp.float32)
    channel_out = total.astype(jnp.bfloat16)
    out[...] = (mid[...].astype(jnp.float32) + normalize(channel_out, gains[3:4, :])).astype(jnp.bfloat16)

    def sent(kind, sem):
        rows = (mi if kind == 0 else up).at[pl.ds(0, 2 * (K // G)), :]
        pltpu.make_async_remote_copy(
            src_ref=rows, dst_ref=rows, send_sem=sem, recv_sem=zr.at[0, 0],
            device_id=(g, f, sibling), device_id_type=MESH).wait_send()

    def swapped(buf, sem):
        pltpu.make_async_remote_copy(
            src_ref=buf, dst_ref=buf, send_sem=sem, recv_sem=w1r.at[0],
            device_id=(g, f, sibling), device_id_type=MESH).wait_send()

    if tuned:
        large = 2 * (K // G)
        small = large * PWt // Ht

        def gone(amount, sem):
            swapped(up.at[pl.ds(0, amount[0] * small + amount[1] * large), :], sem)

        for side, plans in enumerate((((0, (1, 1)), (1, (2, 2)), (2, (3, 0))), ((3, (1, 1)), (2, (2, 2)), (1, (3, 0))))):
            for place_f, amount in plans:
                @pl.when(f == place_f)
                def _():
                    gone(amount, zsem(side, 0, 0))
        for k in range(1, G):
            @pl.when(mid_plane)
            def _():
                gone((3, 2), ysem(k, 0, 0))

            @pl.when(end)
            def _():
                gone((3, 1), ysem(k, 0, 0))

    for kind, w in () if tuned else ((0, "mi"), (1, "up")):
        def drain(s, _):
            moved = True if kind == 0 else (mid_plane | (s == f))

            @pl.when((s <= f) & to_right_ok(w) & moved)
            def _():
                sent(kind, zs.at[0, kind, s])

            @pl.when((s >= f) & to_left_ok(w) & moved)
            def _():
                sent(kind, zs.at[1, kind, s])

            @pl.when((s != f) & moved & shared(w, s))
            def _():
                for k in range(1, G):
                    sent(kind, ys.at[k - 1, kind, s])
            if off and kind == 1:
                @pl.when((s == f) & end)
                def _():
                    for k in range(1, G):
                        sent(kind, ys.at[k - 1, kind, s])
            return 0
        lax.fori_loop(0, F, drain, 0)

    @pl.when(mid_plane)
    def _():
        swapped(rq2.at[0], w2s.at[0])
        for k in range(2, T, 2):
            swapped(rp2.at[0], p2s.at[k // 2 - 1])
        gather_drain(own_rows, sems2)
        if off:
            @pl.when(helper)
            def _():
                gather_drain(end_rows, sems3)
                swapped(rq2.at[1], w2s.at[1])
                for k in range(0, T, 2):
                    swapped(rp2.at[0], p3s.at[k // 2])
    if off:
        @pl.when(end)
        def _():
            end_copy().wait_send()
    gather_drain(g1, sems1)
    swapped(rq1, w1s.at[0])
    for k in range(2, T, 2):
        part1(k).wait_send()


def local_layer(sizes, tokens, mix_in, scale, mix_out, up_w, down_w, gains):
    G, F, T = sizes
    R, D = tokens.shape
    K, PWt = mix_in.shape
    Ht = up_w.shape[1]
    NU = max(1, min(4, Ht // 256))
    ND = max(1, min(4, K // 128))
    NP = 2 + NU + ND
    dims = (G, F, T, R, D, K, PWt, Ht, NU, ND, NP)
    tuned = F == 4 and NU == 4 and ND == 4
    kinds, arrivals = (1, 1) if tuned else (2, F), 2 + NU + (F - 1) * ND if tuned else (F - 1) * NP
    H = T // 2
    vmem, hbm = pl.BlockSpec(memory_space=pltpu.VMEM), pl.BlockSpec(memory_space=pl.ANY)
    bf, dma = jnp.bfloat16, pltpu.SemaphoreType.DMA
    return pl.pallas_call(
        functools.partial(kernel, dims),
        out_shape=pltpu.VMEM((R, D), bf),
        in_specs=[hbm] * 7,
        out_specs=vmem,
        scratch_shapes=[
            pltpu.VMEM((R, D), bf), pltpu.VMEM(gains.shape, jnp.float32), pltpu.VMEM((1, PWt), jnp.float32),
            pltpu.VMEM((D, PWt), bf), pltpu.VMEM((PWt, D), bf),
            pltpu.VMEM((D, Ht), bf), pltpu.VMEM((Ht, D), bf),
            pltpu.VMEM((T, R, D), bf), pltpu.VMEM((2, T, R, D), bf),
            pltpu.VMEM((2, T * R, Ht), bf),
            pltpu.VMEM((2, H, R, D), bf), pltpu.VMEM((H, R, D), bf), pltpu.VMEM((H - 1, R, D), bf),
            pltpu.VMEM((2, 2, H, R, D), bf), pltpu.VMEM((2, H, R, D), bf), pltpu.VMEM((H, R, D), bf),
            pltpu.VMEM((R, D), bf),
            dma((7,)), dma((2,) + kinds), dma((F - 1, NP)),
            dma((G - 1,) + kinds), dma((G - 1, arrivals)),
            dma((3,)), dma((T,)), dma((T,)), dma((T,)),
            dma((1,)), dma((1,)),
            dma((1,)), dma((4,)), dma((2,)), dma((2, 2 * ND + 3 if tuned else F * ND)),
            dma((H - 1,)), dma((H - 1,)),
            dma((H - 1,)), dma((H,)), dma((H,)),
        ],
        compiler_params=pltpu.CompilerParams(
            collective_id=0, has_side_effects=True, vmem_limit_bytes=63 * 1024 * 1024),
    )(tokens, gains, scale.reshape(1, PWt), mix_in, mix_out, up_w, down_w)


def solution(mesh):
    sizes = tuple(mesh.shape[name] for name in ("grp", "fs", "tp"))
    return jax.shard_map(
        functools.partial(local_layer, sizes),
        mesh=mesh,
        in_specs=(
            P(("grp", "fs", "tp"), None),
            P("fs", "tp"),
            P("tp"),
            P("tp", "fs"),
            P("fs", "tp"),
            P("tp", "fs"),
            P(),
        ),
        out_specs=P(("grp", "fs", "tp"), None),
        check_vma=False,
    )
```

```python
import functools

import jax
import jax.numpy as jnp
from jax import lax
from jax.experimental import pallas as pl
from jax.experimental.pallas import tpu as pltpu
from jax.sharding import PartitionSpec as P

GROUPS = 4
EPS = 1e-06
MESH = pl.DeviceIdType.MESH


def normalize(values, gain):
    upcast = values.astype(jnp.float32)
    return upcast * lax.rsqrt(jnp.mean(upcast * upcast, axis=-1, keepdims=True) + EPS) * gain


def pooling(mixed_in, first_channel, group_width):
    length, width = mixed_in.shape
    upcast = mixed_in.astype(jnp.float32)
    row = lax.broadcasted_iota(jnp.int32, (length, width), 0)
    group = (first_channel + lax.broadcasted_iota(jnp.int32, (length, width), 1)) // group_width
    position = (row + 1).astype(jnp.float32)
    total, average = upcast, jnp.zeros_like(upcast)
    for index in range(GROUPS):
        step = 1 << index
        total = total + jnp.where(row >= step, pltpu.roll(total, step, axis=0), 0.0)
        mean = total / jnp.minimum(position, float(2 * step))
        average = jnp.where(group == index, mean, average)
    return average - upcast


def kernel(dims, tok_h, gains_h, scale_h, mi_h, mo_h, up_h, dn_h, out,
           tok, gains, scale, mi, mo, up, dn, g1, g2, hid, sp1, rq1, rp1, sp2, rq2, rp2, mid,
           lsem, zs, zr, ys, yr, gs, g1r, g2r, g3r, es, er,
           w1s, w1r, w2s, w2r, p1s, p1r, p2s, p2r, p3s):
    G, F, T, R, D, K, PWt, Ht, NU, ND, NP = dims
    g, f, t = lax.axis_index("grp"), lax.axis_index("fs"), lax.axis_index("tp")
    cu, cd = Ht // NU, K // ND
    UD = 1 if ND % 2 else 2
    NB = ND // UD
    off = F >= 4
    tuned = F == 4 and NU == 4 and ND == 4
    far = F - 2 if off else F - 1
    first, last = (1, F - 2) if off else (0, F - 1)
    mid_plane = (f >= first) & (f <= last)
    end = (f < first) | (f > last)
    helper = (f == 1) | (f == F - 2) if off else f < 0
    helped = jnp.where(f == 1, 0, F - 1)
    inner = jnp.where(f == 0, 1, F - 2)
    sibling = t + 1 - 2 * lax.rem(t, 2)
    place, half_t = lax.rem(t, 2), T // 2
    step = D // 4

    def to_right_ok(w):
        return f + 1 < F if w in ("mi", "mo") else (f + 1 <= last)

    def to_left_ok(w):
        return f > 0 if w in ("mi", "mo") else (f - 1 >= first)

    def shared(w, s):
        return True if w in ("mi", "mo") or not off else ~(helper & (s == helped))
    NM = 1
    pieces = {"mi": (0, NM), "mo": (NM, 1), "up": (NM + 1, NU), "dn": (NM + 1 + NU, ND)}
    kinds = {"mi": 0, "mo": 0, "up": 1, "dn": 1}
    bufs = {"mi": (mi_h, mi), "mo": (mo_h, mo), "up": (up_h, up), "dn": (dn_h, dn)}

    def slot_of(s, where):
        return s - jnp.where(s > where, 1, 0)

    def zsem(side, kind, s):
        return zs.at[side, 0, 0] if tuned else zs.at[side, kind, s]

    def ysem(k, kind, s):
        return ys.at[k - 1, 0, 0] if tuned else ys.at[k - 1, kind, s]

    def yrsem(k, w, s, c, where):
        slot = slot_of(s, where)
        if not tuned:
            return yr.at[k - 1, slot * NP + pieces[w][0] + c]
        base = {"mi": 0, "mo": 1, "up": 2, "dn": 2 + NU + slot * ND}[w]
        return yr.at[k - 1, base + c]

    def mult(value, by):
        return pl.multiple_of(value, by)

    def span(w, s, c, half):
        base = s * K
        if w == "mi":
            size = K // G // NM
            return pl.ds(mult(base + (half * NM + c) * size, size), size), pl.ds(0, PWt)
        if w == "mo":
            return pl.ds(mult(half * (PWt // G), PWt // G), PWt // G), pl.ds(mult(base, 128), K)
        if w == "up":
            return pl.ds(mult(base + half * (K // G), K // G), K // G), pl.ds(mult(c * cu, cu), cu)
        return pl.ds(mult(half * (Ht // G), Ht // G), Ht // G), pl.ds(mult(base + c * cd, cd), cd)

    def view(w, s, c, half):
        return bufs[w][1].at[span(w, s, c, half)]

    def z_copy(w, s, c, to_right):
        p = pieces[w][0] + c
        target = f + 1 if to_right else f - 1
        side = 0 if to_right else 1
        return pltpu.make_async_remote_copy(
            src_ref=view(w, s, c, g), dst_ref=view(w, s, c, g), send_sem=zsem(side, kinds[w], s), recv_sem=zr.at[s - side, p],
            device_id=(g, target, t), device_id_type=MESH)

    def y_copy(w, s, c, k, half=None):
        half = g if half is None else half
        return pltpu.make_async_remote_copy(
            src_ref=view(w, s, c, half), dst_ref=view(w, s, c, half),
            send_sem=ysem(k, kinds[w], s), recv_sem=yrsem(k, w, s, c, f),
            device_id=(lax.rem(g + k, G), f, t), device_id_type=MESH)

    def send_own(w, c):
        @pl.when(to_right_ok(w))
        def _():
            z_copy(w, f, c, True).start()

        @pl.when(to_left_ok(w))
        def _():
            z_copy(w, f, c, False).start()

    def whole_copy(w, c, k):
        half = lax.rem(g - k + G, G)
        return pltpu.make_async_remote_copy(
            src_ref=view(w, f, c, half), dst_ref=view(w, f, c, half),
            send_sem=ysem(k, kinds[w], f), recv_sem=yrsem(k, w, f, c, inner),
            device_id=(g, inner, t), device_id_type=MESH)

    def send_whole(w):
        if off:
            order = list(range(pieces[w][1]))
            if tuned and w == "dn":
                order = order[:1:-1] + order[:2]

            @pl.when(end)
            def _():
                for c in order:
                    for k in range(1, G):
                        whole_copy(w, c, k).start()

    def pass_on(k):
        half = lax.rem(g - k + G, G)
        block = view("dn", helped, ND - 1, half)
        return pltpu.make_async_remote_copy(
            src_ref=block, dst_ref=block, send_sem=ysem(k, 1, helped), recv_sem=yrsem(k, "dn", helped, ND - 1, F - 1 - f),
            device_id=(g, F - 1 - f, t), device_id_type=MESH)

    def pump(w, d, c, kind=None):
        for to_right in (True, False):
            s = f - d if to_right else f + d
            more = to_right_ok(w) if to_right else to_left_ok(w)
            here = (s >= 0) & (s < F)
            if w in ("up", "dn"):
                here = here & mid_plane
            theirs = helper & (s == helped)
            if kind is not None:
                here = here & (theirs if kind == "relay" else ~theirs)
            spread = shared(w, s)
            if tuned and w == "dn" and c == ND - 1:
                spread = spread & (s > 0) & (s < F - 1)

            @pl.when(here)
            def _():
                z_copy(w, s, c, to_right).wait_recv()

                @pl.when(more)
                def _():
                    z_copy(w, s, c, to_right).start()

                @pl.when(spread)
                def _():
                    for k in range(1, G):
                        y_copy(w, s, c, k).start()

    def y_wait(w, s, c):
        for k in range(1, G):
            y_copy(w, s, c, k, lax.rem(g - k + G, G)).wait_recv()

    def y_wait_rows(w, c):
        size, cols = (F - 1) * (K // G), pl.ds(0, PWt)
        if w == "mo":
            size, cols = PWt // G, pl.ds(0, (F - 1) * K)
        if w == "up":
            cols = pl.ds(mult(c * cu, cu), cu)
        rows = bufs[w][1].at[pl.ds(0, size), cols]
        for k in range(1, G):
            pltpu.make_async_remote_copy(
                src_ref=rows, dst_ref=rows, send_sem=ysem(k, 0, 0), recv_sem=yrsem(k, w, 0, c, f),
                device_id=(lax.rem(g + k, G), f, t), device_id_type=MESH).wait_recv()

    def y_wait_all(w):
        if tuned:
            y_wait_rows(w, 0)
            return

        def body(i, _):
            s, c = i // pieces[w][1], lax.rem(i, pieces[w][1])

            @pl.when(s != f)
            def _():
                y_wait(w, s, c)
            return 0
        lax.fori_loop(0, F * pieces[w][1], body, 0)

    def local(w, index):
        cols, rows = pl.ds(mult(f * K, K), K), pl.ds(mult(f * K, K), K)
        dst = bufs[w][1].at[rows, :] if w in ("mi", "up") else bufs[w][1].at[:, cols]
        return pltpu.make_async_copy(bufs[w][0], dst, lsem.at[index])

    def peer(k):
        return lax.rem(t + k, T)

    def tp_copy(src, dst, send, recv, k):
        return pltpu.make_async_remote_copy(
            src_ref=src, dst_ref=dst, send_sem=send, recv_sem=recv,
            device_id=(g, f, peer(k)), device_id_type=MESH)

    def gather_copy(buf, sems, block, target):
        return pltpu.make_async_remote_copy(
            src_ref=buf.at[block], dst_ref=buf.at[block], send_sem=gs.at[sems[0]],
            recv_sem=sems[1].at[block], device_id=(g, f, target), device_id_type=MESH)

    def gather_start(buf, sems):
        for k in range(2, T, 2):
            gather_copy(buf, sems, t, peer(k)).start()
        gather_copy(buf, sems, t, sibling).start()

    def gather_finish(buf, sems):
        for k in range(2, T, 2):
            block = lax.rem(t - k + T, T)
            gather_copy(buf, sems, block, sibling).wait_recv()
            gather_copy(buf, sems, block, sibling).start()
        for k in range(0, T, 2):
            block = lax.rem(sibling - k + T, T)
            gather_copy(buf, sems, block, sibling).wait_recv()

    def gather_drain(buf, sems):
        sent = buf.at[pl.ds(0, T - 1)]
        pltpu.make_async_remote_copy(
            src_ref=sent, dst_ref=sent, send_sem=gs.at[sems[0]], recv_sem=sems[1].at[0],
            device_id=(g, f, sibling), device_id_type=MESH).wait_send()

    own_rows, end_rows = g2.at[0], g2.at[1]
    sems1, sems2, sems3 = (0, g1r), (1, g2r), (2, g3r)

    def end_copy():
        return pltpu.make_async_remote_copy(
            src_ref=g2.at[0, t], dst_ref=g2.at[1, t], send_sem=es.at[0], recv_sem=er.at[0],
            device_id=(g, inner, t), device_id_type=MESH)

    def swap1(j):
        cols = pl.ds(j * step, step)
        return pltpu.make_async_remote_copy(
            src_ref=sp1.at[1 - place, :, :, cols], dst_ref=rq1.at[:, :, cols],
            send_sem=w1s.at[0], recv_sem=w1r.at[j], device_id=(g, f, sibling), device_id_type=MESH)

    def part1(k):
        return tp_copy(sp1.at[place, peer(k) // 2], rp1.at[k // 2 - 1],
                       p1s.at[k // 2 - 1], p1r.at[k // 2 - 1], k)

    def columns(s, c, n):
        return pl.ds(mult(s * K + c * cd, cd), n * cd)

    def swap_index(s, c):
        if not tuned:
            return s * ND + c
        base = jnp.where(s == f, 2 * ND - 1, 2 * ND + 1) + c // 2
        return jnp.where(s == helped, c, jnp.where(s == F - 1 - helped, ND - 1 + c, base))

    def swap2(i, s, c, n):
        return pltpu.make_async_remote_copy(
            src_ref=sp2.at[i, 1 - place, :, :, columns(s, c, n)], dst_ref=rq2.at[i, :, :, columns(s, c, n)],
            send_sem=w2s.at[i], recv_sem=w2r.at[i, swap_index(s, c)],
            device_id=(g, f, sibling), device_id_type=MESH)

    def part2(s, c, n, k):
        return tp_copy(sp2.at[0, place, peer(k) // 2, :, columns(s, c, n)], rp2.at[k // 2, :, columns(s, c, n)],
                       p2s.at[k // 2 - 1], p2r.at[k // 2], k)

    def part3(s, c, n, k):
        return pltpu.make_async_remote_copy(
            src_ref=sp2.at[1, place, peer(k) // 2, :, columns(s, c, n)], dst_ref=rp2.at[k // 2, :, columns(s, c, n)],
            send_sem=p3s.at[k // 2], recv_sem=p2r.at[k // 2],
            device_id=(g, helped, peer(k)), device_id_type=MESH)

    def merge(a, b):
        return (a.astype(jnp.float32) + b.astype(jnp.float32)).astype(jnp.bfloat16)

    loads = [pltpu.make_async_copy(a, b, lsem.at[4 + i])
             for i, (a, b) in enumerate(((tok_h, tok), (gains_h, gains), (scale_h, scale)))]
    local("mi", 0).start()
    local("mo", 1).start()
    for load in loads:
        load.start()
    local("up", 2).start()
    local("dn", 3).start()

    barrier = pltpu.get_barrier_semaphore()

    @pl.when(f + 1 < F)
    def _():
        pl.semaphore_signal(barrier, inc=1, device_id=(g, f + 1, t), device_id_type=MESH)

    @pl.when(f > 0)
    def _():
        pl.semaphore_signal(barrier, inc=1, device_id=(g, f - 1, t), device_id_type=MESH)

    for k in range(1, G):
        pl.semaphore_signal(barrier, inc=1, device_id=(lax.rem(g + k, G), f, t), device_id_type=MESH)
    for k in range(1, T):
        pl.semaphore_signal(barrier, inc=1, device_id=(g, f, peer(k)), device_id_type=MESH)
    greeted = jnp.where(f + 1 < F, 1, 0) + jnp.where(f > 0, 1, 0) + (G - 1 + T - 1)
    pl.semaphore_wait(barrier, greeted)

    local("mi", 0).wait()
    for c in range(NM):
        send_own("mi", c)
    local("mo", 1).wait()
    send_own("mo", 0)
    local("up", 2).wait()
    send_own("up", 0)

    @pl.when(~mid_plane)
    def _():
        for c in range(1, NU):
            send_own("up", c)
    send_whole("up")
    for load in loads:
        load.wait()
    g1[t] = normalize(tok[...], gains[0:1, :]).astype(jnp.bfloat16)
    gather_start(g1, sems1)
    local("dn", 3).wait()

    for d in range(1, F):
        for kind in ("near", "relay"):
            if kind == "near" or (off and d == 1):
                for c in range(NM):
                    pump("mi", d, c, kind)
                pump("mo", d, 0, kind)
        if d < NU:
            @pl.when(mid_plane)
            def _():
                send_own("up", d)
        if tuned and d == 1:
            pump("up", 1, 0, "near")

    @pl.when(mid_plane)
    def _():
        for c in range(F, NU):
            send_own("up", c)

    for c in range(NU // 2):
        pump("up", 1, c, "relay" if tuned and c == 0 else None)

    y_wait_all("mi")
    gather_finish(g1, sems1)
    mixed_in = jnp.dot(g1[...].reshape(T * R, D), mi[...],
                       preferred_element_type=jnp.float32).astype(jnp.bfloat16)
    scaled = (pooling(mixed_in, t * PWt, PWt * T // GROUPS) * scale[...]).astype(jnp.bfloat16)
    y_wait_all("mo")
    if tuned:
        pump("up", 1, NU // 2)
    for j in range(4):
        cols = pl.ds(j * step, step)
        value = jnp.dot(scaled, mo[:, cols], preferred_element_type=jnp.float32
                        ).astype(jnp.bfloat16).reshape(half_t, 2, R, step)
        for q in range(2):
            sp1[q, :, :, cols] = value[:, q]
        swap1(j).start()
    for j in range(4):
        cols = pl.ds(j * step, step)
        swap1(j).wait_recv()
        sp1[place, :, :, cols] = merge(sp1[place, :, :, cols], rq1[:, :, cols])
    for k in range(2, T, 2):
        part1(k).start()

    def pump_all(w, d, start=0):
        def body(c, _):
            pump(w, d, c)
            return 0
        lax.fori_loop(start, pieces[w][1], body, 0)

    pump_all("up", 1, NU // 2 + 1 if tuned else NU // 2)
    if tuned:
        pump("up", far, 0)
    early = far <= 2

    @pl.when(mid_plane & early)
    def _():
        for c in range(ND):
            send_own("dn", c)

    total = sp1[place, t // 2].astype(jnp.float32)
    for k in range(2, T, 2):
        part1(k).wait_recv()
        total = total + rp1[k // 2 - 1].astype(jnp.float32)
    mixer_out = total.astype(jnp.bfloat16)
    middle = (tok[...].astype(jnp.float32) + normalize(mixer_out, gains[1:2, :])).astype(jnp.bfloat16)
    mid[...] = middle
    g2[0, t] = normalize(middle, gains[2:3, :]).astype(jnp.bfloat16)

    @pl.when(mid_plane)
    def _():
        gather_start(own_rows, sems2)
    if off:
        @pl.when(end)
        def _():
            end_copy().start()

    def pump_mid(d, _):
        pump_all("up", d)
        return 0
    lax.fori_loop(2, far, pump_mid, 0)

    @pl.when(~(mid_plane & early))
    def _():
        for c in range(ND):
            send_own("dn", c)
    send_whole("dn")
    if far > 1:
        pump_all("up", far, 1 if tuned else 0)

    def up_project(i, c):
        cols = pl.ds(mult(c * cu, cu), cu)
        pre = jnp.dot(g2[i].reshape(T * R, D), up[:, cols], preferred_element_type=jnp.float32)
        pre = jnp.maximum(pre, 0.0)
        hid[i, :, cols] = (pre * pre).astype(jnp.bfloat16)

    half_u, half_d = NU // 2, (ND + 1) // 2
    turn = max(half_u - 1, 0)
    soon = [c for c in range(half_d) if half_u + c < NU]
    if off and half_d < ND:
        soon.append(half_d)
    later = [c for c in range(ND) if c not in soon]

    def act(todo):
        for what, d, c in todo:
            if what == "pass":
                y_wait("dn", helped, ND - 1)
                for k in range(1, G):
                    pass_on(k).start()
            else:
                pump("dn", d, c, what)

    up_acts = {2: [("near", 1, 0)], 3: [("near", 1, 1), ("relay", 1, 0), ("near", 1, 2)], 5: [("relay", 1, 1)],
               6: [("near", 1, 3)], 7: [("relay", 1, 2)]}

    def scheduled(acts, n):
        for index, todo in acts.items():
            @pl.when(n == index)
            def _():
                act(todo)

    def up_step(j, _):
        i, c = j // NU, lax.rem(j, NU)

        @pl.when(i == 0)
        def _():
            if tuned:
                y_wait_rows("up", c)
                return

            def landed_rows(s, _):
                @pl.when(s != f)
                def _():
                    y_wait("up", s, c)
                return 0
            lax.fori_loop(0, F, landed_rows, 0)
        if off:
            @pl.when(helper & (i == 1) & (c == 0))
            def _():
                gather_finish(end_rows, sems3)

        @pl.when((i == 0) | helper)
        def _():
            up_project(i, c)
        if off:
            @pl.when(helper & (i == 0) & (c == turn))
            def _():
                end_copy().wait_recv()
                gather_start(end_rows, sems3)
        if tuned:
            scheduled(up_acts, j)
            return 0
        first_pass = (i == 0) & (c >= half_u) & (c - half_u < half_d)
        second_pass = (i == 1) & (c == turn) & (half_d < ND)

        @pl.when(first_pass | second_pass)
        def _():
            pump("dn", 1, jnp.where(i == 0, c - half_u, half_d))
        return 0

    def project(i, s, first, n):
        cols = columns(s, first, n)
        value = jnp.dot(hid[i], dn[:, cols], preferred_element_type=jnp.float32
                        ).astype(jnp.bfloat16).reshape(half_t, 2, R, n * cd)
        for q in range(2):
            sp2[i, q, :, :, cols] = value[:, q]
        swap2(i, s, first, n).start()

    def finish(i, s, first, n):
        cols = columns(s, first, n)
        swap2(i, s, first, n).wait_recv()
        sp2[i, place, :, :, cols] = merge(sp2[i, place, :, :, cols], rq2[i, :, :, cols])

        @pl.when(i == 0)
        def _():
            for k in range(2, T, 2):
                part2(s, first, n, k).start()
        if off:
            @pl.when(i == 1)
            def _():
                for chip in range(half_t):
                    part3(s, first, n, lax.rem(2 * chip + place - t + T, T)).start()

    def project_pair(i, left, right):
        cols = [columns(s, c, 1) for s, c in (left, right)]
        both = jnp.concatenate([dn[:, col] for col in cols], axis=1)
        value = jnp.dot(hid[i], both, preferred_element_type=jnp.float32).astype(jnp.bfloat16)
        for j, (s, c) in enumerate((left, right)):
            part = value[:, j * cd:(j + 1) * cd].reshape(half_t, 2, R, cd)
            for q in range(2):
                sp2[i, q, :, :, cols[j]] = part[:, q]
            swap2(i, s, c, 1).start()

    OWN, NEAR, HELPED, FAR = range(4)
    codes, before, PAIR = [], {}, 64 * ND

    def queue(kind, who, c, n, rows=(1, 0), wait=True):
        for i in rows:
            fresh = kind == 0 and wait and who != OWN and i == rows[0]
            codes.append(kind + 2 * (n - 1) + 4 * i + 8 * fresh + 16 * who + 64 * c)

    def queue_pair(i, fresh):
        codes.append(4 * i + 8 * fresh + 16 * FAR + 64 * (ND - 1) + PAIR)

    def also(*todo):
        before.setdefault(len(codes), []).extend(todo)

    if tuned:
        queue(0, OWN, 0, 2)
        queue(0, OWN, 2, 2)
        queue(1, OWN, 0, 2)
        also(("near", 2, 0), ("relay", 1, 3))
        queue(1, OWN, 2, 2)
        queue(0, NEAR, 0, 2)
        also(("near", 2, 1))
        queue(1, NEAR, 0, 2)
        queue(0, NEAR, 2, 2)
        also(("pass", 0, 0))
        queue(1, NEAR, 2, 2)
        also(("near", 2, 2))
        queue(0, HELPED, 2, 2)
        queue(0, FAR, 0, 1)
        queue(1, HELPED, 2, 2)
        queue(1, FAR, 0, 1)
        queue(0, FAR, 1, 1, (1,))
        also(("near", 2, 3))
        queue(0, HELPED, 0, 1, (1,))
        queue(0, FAR, 1, 1, (0,), False)
        queue(1, FAR, 1, 1, (1,))
        queue(0, HELPED, 0, 1, (0,), False)
        queue(1, HELPED, 0, 1, (1,))
        queue(1, FAR, 1, 1, (0,))
        tails = []
        split = len(codes)
        for second in (False, True):
            if second:
                queue_pair(1, True)
                queue(0, FAR, 2, 1, (1,))
                queue(1, HELPED, 0, 1, (0,))
                queue_pair(0, False)
                queue(1, FAR, 3, 1, (1,))
                queue(1, HELPED, 1, 1, (1,))
                queue(0, FAR, 2, 1, (0,), False)
                queue(1, FAR, 2, 1, (1,))
            else:
                queue_pair(1, True)
                queue(0, FAR, 2, 1, (1,))
                queue(1, FAR, 3, 1, (1,))
                queue(1, HELPED, 1, 1, (1,))
                queue_pair(0, False)
                queue(1, FAR, 2, 1, (1,))
                queue(0, FAR, 2, 1, (0,), False)
                queue(1, HELPED, 0, 1, (0,))
            queue(1, FAR, 2, 1, (0,))
            queue(1, FAR, 3, 1, (0,))
            queue(1, HELPED, 1, 1, (0,))
            tails.append(codes[split:])
            del codes[split:]

    def choose(n, values):
        out = jnp.int32(values[0])
        for index, value in enumerate(values[1:]):
            out = jnp.where(n == index + 1, value, out)
        return out

    def dn_op(n, _):
        scheduled(before, n)
        code = jnp.where(place == 0, choose(n, codes + tails[0]), choose(n, codes + tails[1]))
        pair = code >= PAIR
        code = lax.rem(code, PAIR)
        kind, size, i = lax.rem(code, 2), lax.rem(code // 2, 2) + 1, lax.rem(code // 4, 2)
        fresh, who, first = lax.rem(code // 8, 2), lax.rem(code // 16, 4), code // 64
        s = jnp.where(who == OWN, f, jnp.where(who == NEAR, F - 1 - f, jnp.where(who == HELPED, helped, F - 1 - helped)))
        for c in range(2):
            passed = ((who == HELPED) & (first + c == ND - 1)) | pair

            @pl.when((fresh == 1) & (c < size) & ~passed)
            def _():
                y_wait("dn", s, first + c)

        @pl.when((fresh == 1) & pair)
        def _():
            y_wait("dn", helped, 1)
            y_wait("dn", s, ND - 1)

        @pl.when(pair)
        def _():
            project_pair(i, (s, first), (helped, 1))
        for width in (1, 2):
            @pl.when((kind == 0) & (size == width) & ~pair)
            def _():
                project(i, s, first, width)

            @pl.when((kind == 1) & (size == width))
            def _():
                finish(i, s, first, width)
        return 0

    slots = (far + 1) * NB

    def dn_step(n, _):
        def one(now, _):
            m = n - 1 + now
            slot, q = m // 2, lax.rem(m, 2)
            d, first = slot // NB, lax.rem(slot, NB) * UD
            last = helper & (d == far)
            s = jnp.where(q == 0, f - d, f + d)
            s = jnp.where(last, jnp.where(q == 0, F - 1 - helped, helped), s)
            wanted = ((m >= 0) & (slot < slots) & (s >= 0) & (s < F) & ((q == 0) | (d > 0))
                      & (last | ~(helper & (s == helped))))

            @pl.when(wanted & (now == 1) & (s != f))
            def _():
                for c in range(UD):
                    y_wait("dn", s, first + c)

            def rows(i, _):
                @pl.when(wanted & (now == 0))
                def _():
                    finish(i, s, first, UD)

                @pl.when(wanted & (now == 1))
                def _():
                    project(i, s, first, UD)
                return 0
            lax.fori_loop(0, jnp.where(helper, 2, 1), rows, 0)
            return 0
        lax.fori_loop(0, 2, one, 0)
        slot = n // 2

        @pl.when(n == 2 * NB - 1)
        def _():
            for c in later:
                pump("dn", 1, c)

        @pl.when((lax.rem(n, 2) == 1) & (slot >= NB) & (slot < far * NB))
        def _():
            for c in range(UD):
                pump("dn", slot // NB + 1, lax.rem(slot, NB) * UD + c)
        return 0

    @pl.when(mid_plane)
    def _():
        gather_finish(own_rows, sems2)
        lax.fori_loop(0, (2 if off else 1) * NU, up_step, 0)
        if tuned:
            lax.fori_loop(0, len(codes + tails[0]), dn_op, 0)
        else:
            lax.fori_loop(0, 2 * slots + 1, dn_step, 0)

    def landed(k):
        return tp_copy(rp2.at[k // 2], rp2.at[k // 2], p2s.at[0], p2r.at[k // 2], 2)

    for k in range(2, T, 2):
        landed(k).wait_recv()
    if off:
        @pl.when(end)
        def _():
            landed(0).wait_recv()

    @pl.when(mid_plane)
    def _():
        rp2[0] = sp2[0, place, t // 2]
    total = jnp.zeros((R, D), jnp.float32)
    for k in range(half_t):
        total = total + rp2[k].astype(jnp.float32)
    channel_out = total.astype(jnp.bfloat16)
    out[...] = (mid[...].astype(jnp.float32) + normalize(channel_out, gains[3:4, :])).astype(jnp.bfloat16)

    def sent(kind, sem):
        rows = (mi if kind == 0 else up).at[pl.ds(0, 2 * (K // G)), :]
        pltpu.make_async_remote_copy(
            src_ref=rows, dst_ref=rows, send_sem=sem, recv_sem=zr.at[0, 0],
            device_id=(g, f, sibling), device_id_type=MESH).wait_send()

    def swapped(buf, sem):
        pltpu.make_async_remote_copy(
            src_ref=buf, dst_ref=buf, send_sem=sem, recv_sem=w1r.at[0],
            device_id=(g, f, sibling), device_id_type=MESH).wait_send()

    if tuned:
        large = 2 * (K // G)
        small = large * PWt // Ht

        def gone(amount, sem):
            swapped(up.at[pl.ds(0, amount[0] * small + amount[1] * large), :], sem)

        for side, plans in enumerate((((0, (1, 1)), (1, (2, 2)), (2, (3, 0))), ((3, (1, 1)), (2, (2, 2)), (1, (3, 0))))):
            for place_f, amount in plans:
                @pl.when(f == place_f)
                def _():
                    gone(amount, zsem(side, 0, 0))
        for k in range(1, G):
            @pl.when(mid_plane)
            def _():
                gone((3, 2), ysem(k, 0, 0))

            @pl.when(end)
            def _():
                gone((3, 1), ysem(k, 0, 0))

    for kind, w in () if tuned else ((0, "mi"), (1, "up")):
        def drain(s, _):
            moved = True if kind == 0 else (mid_plane | (s == f))

            @pl.when((s <= f) & to_right_ok(w) & moved)
            def _():
                sent(kind, zs.at[0, kind, s])

            @pl.when((s >= f) & to_left_ok(w) & moved)
            def _():
                sent(kind, zs.at[1, kind, s])

            @pl.when((s != f) & moved & shared(w, s))
            def _():
                for k in range(1, G):
                    sent(kind, ys.at[k - 1, kind, s])
            if off and kind == 1:
                @pl.when((s == f) & end)
                def _():
                    for k in range(1, G):
                        sent(kind, ys.at[k - 1, kind, s])
            return 0
        lax.fori_loop(0, F, drain, 0)

    @pl.when(mid_plane)
    def _():
        swapped(rq2.at[0], w2s.at[0])
        for k in range(2, T, 2):
            swapped(rp2.at[0], p2s.at[k // 2 - 1])
        gather_drain(own_rows, sems2)
        if off:
            @pl.when(helper)
            def _():
                gather_drain(end_rows, sems3)
                swapped(rq2.at[1], w2s.at[1])
                for k in range(0, T, 2):
                    swapped(rp2.at[0], p3s.at[k // 2])
    if off:
        @pl.when(end)
        def _():
            end_copy().wait_send()
    gather_drain(g1, sems1)
    swapped(rq1, w1s.at[0])
    for k in range(2, T, 2):
        part1(k).wait_send()


def local_layer(sizes, tokens, mix_in, scale, mix_out, up_w, down_w, gains):
    G, F, T = sizes
    R, D = tokens.shape
    K, PWt = mix_in.shape
    Ht = up_w.shape[1]
    NU = max(1, min(4, Ht // 256))
    ND = max(1, min(4, K // 128))
    NP = 2 + NU + ND
    dims = (G, F, T, R, D, K, PWt, Ht, NU, ND, NP)
    tuned = F == 4 and NU == 4 and ND == 4
    kinds, arrivals = (1, 1) if tuned else (2, F), 2 + NU + (F - 1) * ND if tuned else (F - 1) * NP
    H = T // 2
    vmem, hbm = pl.BlockSpec(memory_space=pltpu.VMEM), pl.BlockSpec(memory_space=pl.ANY)
    bf, dma = jnp.bfloat16, pltpu.SemaphoreType.DMA
    return pl.pallas_call(
        functools.partial(kernel, dims),
        out_shape=pltpu.VMEM((R, D), bf),
        in_specs=[hbm] * 7,
        out_specs=vmem,
        scratch_shapes=[
            pltpu.VMEM((R, D), bf), pltpu.VMEM(gains.shape, jnp.float32), pltpu.VMEM((1, PWt), jnp.float32),
            pltpu.VMEM((D, PWt), bf), pltpu.VMEM((PWt, D), bf),
            pltpu.VMEM((D, Ht), bf), pltpu.VMEM((Ht, D), bf),
            pltpu.VMEM((T, R, D), bf), pltpu.VMEM((2, T, R, D), bf),
            pltpu.VMEM((2, T * R, Ht), bf),
            pltpu.VMEM((2, H, R, D), bf), pltpu.VMEM((H, R, D), bf), pltpu.VMEM((H - 1, R, D), bf),
            pltpu.VMEM((2, 2, H, R, D), bf), pltpu.VMEM((2, H, R, D), bf), pltpu.VMEM((H, R, D), bf),
            pltpu.VMEM((R, D), bf),
            dma((7,)), dma((2,) + kinds), dma((F - 1, NP)),
            dma((G - 1,) + kinds), dma((G - 1, arrivals)),
            dma((3,)), dma((T,)), dma((T,)), dma((T,)),
            dma((1,)), dma((1,)),
            dma((1,)), dma((4,)), dma((2,)), dma((2, 2 * ND + 3 if tuned else F * ND)),
            dma((H - 1,)), dma((H - 1,)),
            dma((H - 1,)), dma((H,)), dma((H,)),
        ],
        compiler_params=pltpu.CompilerParams(
            collective_id=0, has_side_effects=True, vmem_limit_bytes=63 * 1024 * 1024),
    )(tokens, gains, scale.reshape(1, PWt), mix_in, mix_out, up_w, down_w)


def solution(mesh):
    sizes = tuple(mesh.shape[name] for name in ("grp", "fs", "tp"))
    return jax.shard_map(
        functools.partial(local_layer, sizes),
        mesh=mesh,
        in_specs=(
            P(("grp", "fs", "tp"), None),
            P("fs", "tp"),
            P("tp"),
            P("tp", "fs"),
            P("fs", "tp"),
            P("tp", "fs"),
            P(),
        ),
        out_specs=P(("grp", "fs", "tp"), None),
        check_vma=False,
    )
```

```python
import functools

import jax
import jax.numpy as jnp
from jax import lax
from jax.experimental import pallas as pl
from jax.experimental.pallas import tpu as pltpu
from jax.sharding import PartitionSpec as P

GROUPS = 4
EPS = 1e-06
MESH = pl.DeviceIdType.MESH


def normalize(values, gain):
    upcast = values.astype(jnp.float32)
    return upcast * lax.rsqrt(jnp.mean(upcast * upcast, axis=-1, keepdims=True) + EPS) * gain


def pooling(mixed_in, first_channel, group_width):
    length, width = mixed_in.shape
    upcast = mixed_in.astype(jnp.float32)
    row = lax.broadcasted_iota(jnp.int32, (length, width), 0)
    group = (first_channel + lax.broadcasted_iota(jnp.int32, (length, width), 1)) // group_width
    position = (row + 1).astype(jnp.float32)
    total, average = upcast, jnp.zeros_like(upcast)
    for index in range(GROUPS):
        step = 1 << index
        total = total + jnp.where(row >= step, pltpu.roll(total, step, axis=0), 0.0)
        mean = total / jnp.minimum(position, float(2 * step))
        average = jnp.where(group == index, mean, average)
    return average - upcast


def kernel(dims, tok_h, gains_h, scale_h, mi_h, mo_h, up_h, dn_h, out,
           tok, gains, scale, mi, mo, up, dn, g1, g2, hid, sp1, rq1, rp1, sp2, rq2, rp2, mid,
           lsem, zs, zr, ys, yr, gs, g1r, g2r, g3r, es, er,
           w1s, w1r, w2s, w2r, p1s, p1r, p2s, p2r, p3s):
    G, F, T, R, D, K, PWt, Ht, NU, ND, NP = dims
    g, f, t = lax.axis_index("grp"), lax.axis_index("fs"), lax.axis_index("tp")
    cu, cd = Ht // NU, K // ND
    UD = 1 if ND % 2 else 2
    NB = ND // UD
    off = F >= 4
    tuned = F == 4 and NU == 4 and ND == 4
    far = F - 2 if off else F - 1
    first, last = (1, F - 2) if off else (0, F - 1)
    mid_plane = (f >= first) & (f <= last)
    end = (f < first) | (f > last)
    helper = (f == 1) | (f == F - 2) if off else f < 0
    helped = jnp.where(f == 1, 0, F - 1)
    inner = jnp.where(f == 0, 1, F - 2)
    sibling = t + 1 - 2 * lax.rem(t, 2)
    place, half_t = lax.rem(t, 2), T // 2
    step = D // 4

    def to_right_ok(w):
        return f + 1 < F if w in ("mi", "mo") else (f + 1 <= last)

    def to_left_ok(w):
        return f > 0 if w in ("mi", "mo") else (f - 1 >= first)

    def shared(w, s):
        return True if w in ("mi", "mo") or not off else ~(helper & (s == helped))
    NM = 1
    pieces = {"mi": (0, NM), "mo": (NM, 1), "up": (NM + 1, NU), "dn": (NM + 1 + NU, ND)}
    kinds = {"mi": 0, "mo": 0, "up": 1, "dn": 1}
    bufs = {"mi": (mi_h, mi), "mo": (mo_h, mo), "up": (up_h, up), "dn": (dn_h, dn)}

    def slot_of(s, where):
        return s - jnp.where(s > where, 1, 0)

    def zsem(side, kind, s):
        return zs.at[side, 0, 0] if tuned else zs.at[side, kind, s]

    def ysem(k, kind, s):
        return ys.at[k - 1, 0, 0] if tuned else ys.at[k - 1, kind, s]

    def yrsem(k, w, s, c, where):
        slot = slot_of(s, where)
        if not tuned:
            return yr.at[k - 1, slot * NP + pieces[w][0] + c]
        base = {"mi": 0, "mo": 1, "up": 2, "dn": 2 + NU + slot * ND}[w]
        return yr.at[k - 1, base + c]

    def mult(value, by):
        return pl.multiple_of(value, by)

    def span(w, s, c, half):
        base = s * K
        if w == "mi":
            size = K // G // NM
            return pl.ds(mult(base + (half * NM + c) * size, size), size), pl.ds(0, PWt)
        if w == "mo":
            return pl.ds(mult(half * (PWt // G), PWt // G), PWt // G), pl.ds(mult(base, 128), K)
        if w == "up":
            return pl.ds(mult(base + half * (K // G), K // G), K // G), pl.ds(mult(c * cu, cu), cu)
        return pl.ds(mult(half * (Ht // G), Ht // G), Ht // G), pl.ds(mult(base + c * cd, cd), cd)

    def view(w, s, c, half):
        return bufs[w][1].at[span(w, s, c, half)]

    def z_copy(w, s, c, to_right):
        p = pieces[w][0] + c
        target = f + 1 if to_right else f - 1
        side = 0 if to_right else 1
        return pltpu.make_async_remote_copy(
            src_ref=view(w, s, c, g), dst_ref=view(w, s, c, g), send_sem=zsem(side, kinds[w], s), recv_sem=zr.at[s - side, p],
            device_id=(g, target, t), device_id_type=MESH)

    def y_copy(w, s, c, k, half=None):
        half = g if half is None else half
        return pltpu.make_async_remote_copy(
            src_ref=view(w, s, c, half), dst_ref=view(w, s, c, half),
            send_sem=ysem(k, kinds[w], s), recv_sem=yrsem(k, w, s, c, f),
            device_id=(lax.rem(g + k, G), f, t), device_id_type=MESH)

    def send_own(w, c):
        @pl.when(to_right_ok(w))
        def _():
            z_copy(w, f, c, True).start()

        @pl.when(to_left_ok(w))
        def _():
            z_copy(w, f, c, False).start()

    def whole_copy(w, c, k):
        half = lax.rem(g - k + G, G)
        return pltpu.make_async_remote_copy(
            src_ref=view(w, f, c, half), dst_ref=view(w, f, c, half),
            send_sem=ysem(k, kinds[w], f), recv_sem=yrsem(k, w, f, c, inner),
            device_id=(g, inner, t), device_id_type=MESH)

    def send_whole(w):
        if off:
            order = list(range(pieces[w][1]))
            if tuned and w == "dn":
                order = order[:1:-1] + order[:2]

            @pl.when(end)
            def _():
                for c in order:
                    for k in range(1, G):
                        whole_copy(w, c, k).start()

    def pass_on(k):
        half = lax.rem(g - k + G, G)
        block = view("dn", helped, ND - 1, half)
        return pltpu.make_async_remote_copy(
            src_ref=block, dst_ref=block, send_sem=ysem(k, 1, helped), recv_sem=yrsem(k, "dn", helped, ND - 1, F - 1 - f),
            device_id=(g, F - 1 - f, t), device_id_type=MESH)

    def pump(w, d, c, kind=None):
        for to_right in (True, False):
            s = f - d if to_right else f + d
            more = to_right_ok(w) if to_right else to_left_ok(w)
            here = (s >= 0) & (s < F)
            if w in ("up", "dn"):
                here = here & mid_plane
            theirs = helper & (s == helped)
            if kind is not None:
                here = here & (theirs if kind == "relay" else ~theirs)
            spread = shared(w, s)
            if tuned and w == "dn" and c == ND - 1:
                spread = spread & (s > 0) & (s < F - 1)

            @pl.when(here)
            def _():
                z_copy(w, s, c, to_right).wait_recv()

                @pl.when(more)
                def _():
                    z_copy(w, s, c, to_right).start()

                @pl.when(spread)
                def _():
                    for k in range(1, G):
                        y_copy(w, s, c, k).start()

    def y_wait(w, s, c):
        for k in range(1, G):
            y_copy(w, s, c, k, lax.rem(g - k + G, G)).wait_recv()

    def y_wait_rows(w, c):
        size, cols = (F - 1) * (K // G), pl.ds(0, PWt)
        if w == "mo":
            size, cols = PWt // G, pl.ds(0, (F - 1) * K)
        if w == "up":
            cols = pl.ds(mult(c * cu, cu), cu)
        rows = bufs[w][1].at[pl.ds(0, size), cols]
        for k in range(1, G):
            pltpu.make_async_remote_copy(
                src_ref=rows, dst_ref=rows, send_sem=ysem(k, 0, 0), recv_sem=yrsem(k, w, 0, c, f),
                device_id=(lax.rem(g + k, G), f, t), device_id_type=MESH).wait_recv()

    def y_wait_all(w):
        if tuned:
            y_wait_rows(w, 0)
            return

        def body(i, _):
            s, c = i // pieces[w][1], lax.rem(i, pieces[w][1])

            @pl.when(s != f)
            def _():
                y_wait(w, s, c)
            return 0
        lax.fori_loop(0, F * pieces[w][1], body, 0)

    def local(w, index):
        cols, rows = pl.ds(mult(f * K, K), K), pl.ds(mult(f * K, K), K)
        dst = bufs[w][1].at[rows, :] if w in ("mi", "up") else bufs[w][1].at[:, cols]
        return pltpu.make_async_copy(bufs[w][0], dst, lsem.at[index])

    def peer(k):
        return lax.rem(t + k, T)

    def tp_copy(src, dst, send, recv, k):
        return pltpu.make_async_remote_copy(
            src_ref=src, dst_ref=dst, send_sem=send, recv_sem=recv,
            device_id=(g, f, peer(k)), device_id_type=MESH)

    def gather_copy(buf, sems, block, target):
        return pltpu.make_async_remote_copy(
            src_ref=buf.at[block], dst_ref=buf.at[block], send_sem=gs.at[sems[0]],
            recv_sem=sems[1].at[block], device_id=(g, f, target), device_id_type=MESH)

    def gather_start(buf, sems):
        for k in range(2, T, 2):
            gather_copy(buf, sems, t, peer(k)).start()
        gather_copy(buf, sems, t, sibling).start()

    def gather_finish(buf, sems):
        for k in range(2, T, 2):
            block = lax.rem(t - k + T, T)
            gather_copy(buf, sems, block, sibling).wait_recv()
            gather_copy(buf, sems, block, sibling).start()
        for k in range(0, T, 2):
            block = lax.rem(sibling - k + T, T)
            gather_copy(buf, sems, block, sibling).wait_recv()

    def gather_drain(buf, sems):
        sent = buf.at[pl.ds(0, T - 1)]
        pltpu.make_async_remote_copy(
            src_ref=sent, dst_ref=sent, send_sem=gs.at[sems[0]], recv_sem=sems[1].at[0],
            device_id=(g, f, sibling), device_id_type=MESH).wait_send()

    own_rows, end_rows = g2.at[0], g2.at[1]
    sems1, sems2, sems3 = (0, g1r), (1, g2r), (2, g3r)

    def end_copy():
        return pltpu.make_async_remote_copy(
            src_ref=g2.at[0, t], dst_ref=g2.at[1, t], send_sem=es.at[0], recv_sem=er.at[0],
            device_id=(g, inner, t), device_id_type=MESH)

    def swap1(j):
        cols = pl.ds(j * step, step)
        return pltpu.make_async_remote_copy(
            src_ref=sp1.at[1 - place, :, :, cols], dst_ref=rq1.at[:, :, cols],
            send_sem=w1s.at[0], recv_sem=w1r.at[j], device_id=(g, f, sibling), device_id_type=MESH)

    def part1(k):
        return tp_copy(sp1.at[place, peer(k) // 2], rp1.at[k // 2 - 1],
                       p1s.at[k // 2 - 1], p1r.at[k // 2 - 1], k)

    def columns(s, c, n):
        return pl.ds(mult(s * K + c * cd, cd), n * cd)

    def swap_index(s, c):
        if not tuned:
            return s * ND + c
        base = jnp.where(s == f, 2 * ND - 1, 2 * ND + 1) + c // 2
        return jnp.where(s == helped, c, jnp.where(s == F - 1 - helped, ND - 1 + c, base))

    def swap2(i, s, c, n):
        return pltpu.make_async_remote_copy(
            src_ref=sp2.at[i, 1 - place, :, :, columns(s, c, n)], dst_ref=rq2.at[i, :, :, columns(s, c, n)],
            send_sem=w2s.at[i], recv_sem=w2r.at[i, swap_index(s, c)],
            device_id=(g, f, sibling), device_id_type=MESH)

    def part2(s, c, n, k):
        return tp_copy(sp2.at[0, place, peer(k) // 2, :, columns(s, c, n)], rp2.at[k // 2, :, columns(s, c, n)],
                       p2s.at[k // 2 - 1], p2r.at[k // 2], k)

    def part3(s, c, n, k):
        return pltpu.make_async_remote_copy(
            src_ref=sp2.at[1, place, peer(k) // 2, :, columns(s, c, n)], dst_ref=rp2.at[k // 2, :, columns(s, c, n)],
            send_sem=p3s.at[k // 2], recv_sem=p2r.at[k // 2],
            device_id=(g, helped, peer(k)), device_id_type=MESH)

    def merge(a, b):
        return (a.astype(jnp.float32) + b.astype(jnp.float32)).astype(jnp.bfloat16)

    loads = [pltpu.make_async_copy(a, b, lsem.at[4 + i])
             for i, (a, b) in enumerate(((tok_h, tok), (gains_h, gains), (scale_h, scale)))]
    local("mi", 0).start()
    local("mo", 1).start()
    for load in loads:
        load.start()
    local("up", 2).start()
    local("dn", 3).start()

    barrier = pltpu.get_barrier_semaphore()

    @pl.when(f + 1 < F)
    def _():
        pl.semaphore_signal(barrier, inc=1, device_id=(g, f + 1, t), device_id_type=MESH)

    @pl.when(f > 0)
    def _():
        pl.semaphore_signal(barrier, inc=1, device_id=(g, f - 1, t), device_id_type=MESH)

    for k in range(1, G):
        pl.semaphore_signal(barrier, inc=1, device_id=(lax.rem(g + k, G), f, t), device_id_type=MESH)
    for k in range(1, T):
        pl.semaphore_signal(barrier, inc=1, device_id=(g, f, peer(k)), device_id_type=MESH)
    greeted = jnp.where(f + 1 < F, 1, 0) + jnp.where(f > 0, 1, 0) + (G - 1 + T - 1)
    pl.semaphore_wait(barrier, greeted)

    local("mi", 0).wait()
    for c in range(NM):
        send_own("mi", c)
    local("mo", 1).wait()
    send_own("mo", 0)
    local("up", 2).wait()
    send_own("up", 0)

    @pl.when(~mid_plane)
    def _():
        for c in range(1, NU):
            send_own("up", c)
    send_whole("up")
    for load in loads:
        load.wait()
    g1[t] = normalize(tok[...], gains[0:1, :]).astype(jnp.bfloat16)
    gather_start(g1, sems1)
    local("dn", 3).wait()

    for d in range(1, F):
        for kind in ("near", "relay"):
            if kind == "near" or (off and d == 1):
                for c in range(NM):
                    pump("mi", d, c, kind)
                pump("mo", d, 0, kind)
        if d < NU:
            @pl.when(mid_plane)
            def _():
                send_own("up", d)
        if tuned and d == 1:
            pump("up", 1, 0, "near")

    @pl.when(mid_plane)
    def _():
        for c in range(F, NU):
            send_own("up", c)

    for c in range(NU // 2):
        pump("up", 1, c, "relay" if tuned and c == 0 else None)

    y_wait_all("mi")
    gather_finish(g1, sems1)
    mixed_in = jnp.dot(g1[...].reshape(T * R, D), mi[...],
                       preferred_element_type=jnp.float32).astype(jnp.bfloat16)
    scaled = (pooling(mixed_in, t * PWt, PWt * T // GROUPS) * scale[...]).astype(jnp.bfloat16)
    y_wait_all("mo")
    if tuned:
        pump("up", 1, NU // 2)
    for j in range(4):
        cols = pl.ds(j * step, step)
        value = jnp.dot(scaled, mo[:, cols], preferred_element_type=jnp.float32
                        ).astype(jnp.bfloat16).reshape(half_t, 2, R, step)
        for q in range(2):
            sp1[q, :, :, cols] = value[:, q]
        swap1(j).start()
    for j in range(4):
        cols = pl.ds(j * step, step)
        swap1(j).wait_recv()
        sp1[place, :, :, cols] = merge(sp1[place, :, :, cols], rq1[:, :, cols])
    for k in range(2, T, 2):
        part1(k).start()

    def pump_all(w, d, start=0):
        def body(c, _):
            pump(w, d, c)
            return 0
        lax.fori_loop(start, pieces[w][1], body, 0)

    pump_all("up", 1, NU // 2 + 1 if tuned else NU // 2)
    if tuned:
        pump("up", far, 0)
    early = far <= 2

    @pl.when(mid_plane & early)
    def _():
        for c in range(ND):
            send_own("dn", c)

    total = sp1[place, t // 2].astype(jnp.float32)
    for k in range(2, T, 2):
        part1(k).wait_recv()
        total = total + rp1[k // 2 - 1].astype(jnp.float32)
    mixer_out = total.astype(jnp.bfloat16)
    middle = (tok[...].astype(jnp.float32) + normalize(mixer_out, gains[1:2, :])).astype(jnp.bfloat16)
    mid[...] = middle
    g2[0, t] = normalize(middle, gains[2:3, :]).astype(jnp.bfloat16)

    @pl.when(mid_plane)
    def _():
        gather_start(own_rows, sems2)
    if off:
        @pl.when(end)
        def _():
            end_copy().start()

    def pump_mid(d, _):
        pump_all("up", d)
        return 0
    lax.fori_loop(2, far, pump_mid, 0)

    @pl.when(~(mid_plane & early))
    def _():
        for c in range(ND):
            send_own("dn", c)
    send_whole("dn")
    if far > 1:
        pump_all("up", far, 1 if tuned else 0)

    def up_project(i, c):
        cols = pl.ds(mult(c * cu, cu), cu)
        pre = jnp.dot(g2[i].reshape(T * R, D), up[:, cols], preferred_element_type=jnp.float32)
        pre = jnp.maximum(pre, 0.0)
        hid[i, :, cols] = (pre * pre).astype(jnp.bfloat16)

    half_u, half_d = NU // 2, (ND + 1) // 2
    turn = max(half_u - 1, 0)
    soon = [c for c in range(half_d) if half_u + c < NU]
    if off and half_d < ND:
        soon.append(half_d)
    later = [c for c in range(ND) if c not in soon]

    def act(todo):
        for what, d, c in todo:
            if what == "pass":
                y_wait("dn", helped, ND - 1)
                for k in range(1, G):
                    pass_on(k).start()
            else:
                pump("dn", d, c, what)

    up_acts = {2: [("near", 1, 0)], 3: [("near", 1, 1), ("relay", 1, 0), ("near", 1, 2)], 5: [("relay", 1, 1)],
               6: [("near", 1, 3)], 7: [("relay", 1, 2)]}

    def scheduled(acts, n):
        for index, todo in acts.items():
            @pl.when(n == index)
            def _():
                act(todo)

    def up_step(j, _):
        i, c = j // NU, lax.rem(j, NU)

        @pl.when(i == 0)
        def _():
            if tuned:
                y_wait_rows("up", c)
                return

            def landed_rows(s, _):
                @pl.when(s != f)
                def _():
                    y_wait("up", s, c)
                return 0
            lax.fori_loop(0, F, landed_rows, 0)
        if off:
            @pl.when(helper & (i == 1) & (c == 0))
            def _():
                gather_finish(end_rows, sems3)

        @pl.when((i == 0) | helper)
        def _():
            up_project(i, c)
        if off:
            @pl.when(helper & (i == 0) & (c == turn))
            def _():
                end_copy().wait_recv()
                gather_start(end_rows, sems3)
        if tuned:
            scheduled(up_acts, j)
            return 0
        first_pass = (i == 0) & (c >= half_u) & (c - half_u < half_d)
        second_pass = (i == 1) & (c == turn) & (half_d < ND)

        @pl.when(first_pass | second_pass)
        def _():
            pump("dn", 1, jnp.where(i == 0, c - half_u, half_d))
        return 0

    def project(i, s, first, n):
        cols = columns(s, first, n)
        value = jnp.dot(hid[i], dn[:, cols], preferred_element_type=jnp.float32
                        ).astype(jnp.bfloat16).reshape(half_t, 2, R, n * cd)
        for q in range(2):
            sp2[i, q, :, :, cols] = value[:, q]
        swap2(i, s, first, n).start()

    def finish(i, s, first, n):
        cols = columns(s, first, n)
        swap2(i, s, first, n).wait_recv()
        sp2[i, place, :, :, cols] = merge(sp2[i, place, :, :, cols], rq2[i, :, :, cols])

        @pl.when(i == 0)
        def _():
            for k in range(2, T, 2):
                part2(s, first, n, k).start()
        if off:
            @pl.when(i == 1)
            def _():
                for chip in range(half_t):
                    part3(s, first, n, lax.rem(2 * chip + place - t + T, T)).start()

    OWN, NEAR, HELPED, FAR = range(4)
    codes, before = [], {}

    def queue(kind, who, c, n, rows=(1, 0), wait=True):
        for i in rows:
            fresh = kind == 0 and wait and who != OWN and i == rows[0]
            codes.append(kind + 2 * (n - 1) + 4 * i + 8 * fresh + 16 * who + 64 * c)

    def also(*todo):
        before.setdefault(len(codes), []).extend(todo)

    if tuned:
        queue(0, OWN, 0, 2)
        queue(0, OWN, 2, 2)
        queue(1, OWN, 0, 2)
        also(("near", 2, 0), ("relay", 1, 3))
        queue(1, OWN, 2, 2)
        queue(0, NEAR, 0, 2)
        also(("near", 2, 1))
        queue(1, NEAR, 0, 2)
        queue(0, NEAR, 2, 2)
        also(("pass", 0, 0))
        queue(1, NEAR, 2, 2)
        also(("near", 2, 2))
        queue(0, HELPED, 2, 2)
        queue(0, FAR, 0, 1)
        queue(1, HELPED, 2, 2)
        queue(1, FAR, 0, 1)
        queue(0, FAR, 1, 1, (1,))
        also(("near", 2, 3))
        queue(0, HELPED, 0, 1, (1,))
        queue(0, FAR, 1, 1, (0,), False)
        queue(1, FAR, 1, 1, (1,))
        queue(0, HELPED, 0, 1, (0,), False)
        queue(1, HELPED, 0, 1, (1,))
        queue(1, FAR, 1, 1, (0,))
        tails = []
        split = len(codes)
        for second in (False, True):
            if second:
                queue(0, HELPED, 1, 1, (1,))
                queue(0, FAR, 2, 2, (1,))
                queue(1, HELPED, 1, 1, (1,))
                queue(0, HELPED, 1, 1, (0,), False)
                queue(1, HELPED, 0, 1, (0,))
                queue(1, FAR, 2, 2, (1,))
                queue(0, FAR, 2, 2, (0,), False)
                queue(1, HELPED, 1, 1, (0,))
                queue(1, FAR, 2, 2, (0,))
            else:
                queue(0, HELPED, 1, 1, (1,))
                queue(0, FAR, 2, 2, (1,))
                queue(1, HELPED, 1, 1, (1,))
                queue(0, HELPED, 1, 1, (0,), False)
                queue(1, FAR, 2, 2, (1,))
                queue(0, FAR, 2, 2, (0,), False)
                queue(1, HELPED, 0, 1, (0,))
                queue(1, HELPED, 1, 1, (0,))
                queue(1, FAR, 2, 2, (0,))
            tails.append(codes[split:])
            del codes[split:]

    def choose(n, values):
        out = jnp.int32(values[0])
        for index, value in enumerate(values[1:]):
            out = jnp.where(n == index + 1, value, out)
        return out

    def dn_op(n, _):
        scheduled(before, n)
        code = jnp.where(place == 0, choose(n, codes + tails[0]), choose(n, codes + tails[1]))
        kind, size, i = lax.rem(code, 2), lax.rem(code // 2, 2) + 1, lax.rem(code // 4, 2)
        fresh, who, first = lax.rem(code // 8, 2), lax.rem(code // 16, 4), code // 64
        s = jnp.where(who == OWN, f, jnp.where(who == NEAR, F - 1 - f, jnp.where(who == HELPED, helped, F - 1 - helped)))
        for c in range(2):
            passed = (who == HELPED) & (first + c == ND - 1)

            @pl.when((fresh == 1) & (c < size) & ~passed)
            def _():
                y_wait("dn", s, first + c)

        for width in (1, 2):
            @pl.when((kind == 0) & (size == width))
            def _():
                project(i, s, first, width)

            @pl.when((kind == 1) & (size == width))
            def _():
                finish(i, s, first, width)
        return 0

    slots = (far + 1) * NB

    def dn_step(n, _):
        def one(now, _):
            m = n - 1 + now
            slot, q = m // 2, lax.rem(m, 2)
            d, first = slot // NB, lax.rem(slot, NB) * UD
            last = helper & (d == far)
            s = jnp.where(q == 0, f - d, f + d)
            s = jnp.where(last, jnp.where(q == 0, F - 1 - helped, helped), s)
            wanted = ((m >= 0) & (slot < slots) & (s >= 0) & (s < F) & ((q == 0) | (d > 0))
                      & (last | ~(helper & (s == helped))))

            @pl.when(wanted & (now == 1) & (s != f))
            def _():
                for c in range(UD):
                    y_wait("dn", s, first + c)

            def rows(i, _):
                @pl.when(wanted & (now == 0))
                def _():
                    finish(i, s, first, UD)

                @pl.when(wanted & (now == 1))
                def _():
                    project(i, s, first, UD)
                return 0
            lax.fori_loop(0, jnp.where(helper, 2, 1), rows, 0)
            return 0
        lax.fori_loop(0, 2, one, 0)
        slot = n // 2

        @pl.when(n == 2 * NB - 1)
        def _():
            for c in later:
                pump("dn", 1, c)

        @pl.when((lax.rem(n, 2) == 1) & (slot >= NB) & (slot < far * NB))
        def _():
            for c in range(UD):
                pump("dn", slot // NB + 1, lax.rem(slot, NB) * UD + c)
        return 0

    @pl.when(mid_plane)
    def _():
        gather_finish(own_rows, sems2)
        lax.fori_loop(0, (2 if off else 1) * NU, up_step, 0)
        if tuned:
            lax.fori_loop(0, len(codes + tails[0]), dn_op, 0)
        else:
            lax.fori_loop(0, 2 * slots + 1, dn_step, 0)

    def landed(k):
        return tp_copy(rp2.at[k // 2], rp2.at[k // 2], p2s.at[0], p2r.at[k // 2], 2)

    for k in range(2, T, 2):
        landed(k).wait_recv()
    if off:
        @pl.when(end)
        def _():
            landed(0).wait_recv()

    @pl.when(mid_plane)
    def _():
        rp2[0] = sp2[0, place, t // 2]
    total = jnp.zeros((R, D), jnp.float32)
    for k in range(half_t):
        total = total + rp2[k].astype(jnp.float32)
    channel_out = total.astype(jnp.bfloat16)
    out[...] = (mid[...].astype(jnp.float32) + normalize(channel_out, gains[3:4, :])).astype(jnp.bfloat16)

    def sent(kind, sem):
        rows = (mi if kind == 0 else up).at[pl.ds(0, 2 * (K // G)), :]
        pltpu.make_async_remote_copy(
            src_ref=rows, dst_ref=rows, send_sem=sem, recv_sem=zr.at[0, 0],
            device_id=(g, f, sibling), device_id_type=MESH).wait_send()

    def swapped(buf, sem):
        pltpu.make_async_remote_copy(
            src_ref=buf, dst_ref=buf, send_sem=sem, recv_sem=w1r.at[0],
            device_id=(g, f, sibling), device_id_type=MESH).wait_send()

    if tuned:
        large = 2 * (K // G)
        small = large * PWt // Ht

        def gone(amount, sem):
            swapped(up.at[pl.ds(0, amount[0] * small + amount[1] * large), :], sem)

        for side, plans in enumerate((((0, (1, 1)), (1, (2, 2)), (2, (3, 0))), ((3, (1, 1)), (2, (2, 2)), (1, (3, 0))))):
            for place_f, amount in plans:
                @pl.when(f == place_f)
                def _():
                    gone(amount, zsem(side, 0, 0))
        for k in range(1, G):
            @pl.when(mid_plane)
            def _():
                gone((3, 2), ysem(k, 0, 0))

            @pl.when(end)
            def _():
                gone((3, 1), ysem(k, 0, 0))

    for kind, w in () if tuned else ((0, "mi"), (1, "up")):
        def drain(s, _):
            moved = True if kind == 0 else (mid_plane | (s == f))

            @pl.when((s <= f) & to_right_ok(w) & moved)
            def _():
                sent(kind, zs.at[0, kind, s])

            @pl.when((s >= f) & to_left_ok(w) & moved)
            def _():
                sent(kind, zs.at[1, kind, s])

            @pl.when((s != f) & moved & shared(w, s))
            def _():
                for k in range(1, G):
                    sent(kind, ys.at[k - 1, kind, s])
            if off and kind == 1:
                @pl.when((s == f) & end)
                def _():
                    for k in range(1, G):
                        sent(kind, ys.at[k - 1, kind, s])
            return 0
        lax.fori_loop(0, F, drain, 0)

    @pl.when(mid_plane)
    def _():
        swapped(rq2.at[0], w2s.at[0])
        for k in range(2, T, 2):
            swapped(rp2.at[0], p2s.at[k // 2 - 1])
        gather_drain(own_rows, sems2)
        if off:
            @pl.when(helper)
            def _():
                gather_drain(end_rows, sems3)
                swapped(rq2.at[1], w2s.at[1])
                for k in range(0, T, 2):
                    swapped(rp2.at[0], p3s.at[k // 2])
    if off:
        @pl.when(end)
        def _():
            end_copy().wait_send()
    gather_drain(g1, sems1)
    swapped(rq1, w1s.at[0])
    for k in range(2, T, 2):
        part1(k).wait_send()


def local_layer(sizes, tokens, mix_in, scale, mix_out, up_w, down_w, gains):
    G, F, T = sizes
    R, D = tokens.shape
    K, PWt = mix_in.shape
    Ht = up_w.shape[1]
    NU = max(1, min(4, Ht // 256))
    ND = max(1, min(4, K // 128))
    NP = 2 + NU + ND
    dims = (G, F, T, R, D, K, PWt, Ht, NU, ND, NP)
    tuned = F == 4 and NU == 4 and ND == 4
    kinds, arrivals = (1, 1) if tuned else (2, F), 2 + NU + (F - 1) * ND if tuned else (F - 1) * NP
    H = T // 2
    vmem, hbm = pl.BlockSpec(memory_space=pltpu.VMEM), pl.BlockSpec(memory_space=pl.ANY)
    bf, dma = jnp.bfloat16, pltpu.SemaphoreType.DMA
    return pl.pallas_call(
        functools.partial(kernel, dims),
        out_shape=pltpu.VMEM((R, D), bf),
        in_specs=[hbm] * 7,
        out_specs=vmem,
        scratch_shapes=[
            pltpu.VMEM((R, D), bf), pltpu.VMEM(gains.shape, jnp.float32), pltpu.VMEM((1, PWt), jnp.float32),
            pltpu.VMEM((D, PWt), bf), pltpu.VMEM((PWt, D), bf),
            pltpu.VMEM((D, Ht), bf), pltpu.VMEM((Ht, D), bf),
            pltpu.VMEM((T, R, D), bf), pltpu.VMEM((2, T, R, D), bf),
            pltpu.VMEM((2, T * R, Ht), bf),
            pltpu.VMEM((2, H, R, D), bf), pltpu.VMEM((H, R, D), bf), pltpu.VMEM((H - 1, R, D), bf),
            pltpu.VMEM((2, 2, H, R, D), bf), pltpu.VMEM((2, H, R, D), bf), pltpu.VMEM((H, R, D), bf),
            pltpu.VMEM((R, D), bf),
            dma((7,)), dma((2,) + kinds), dma((F - 1, NP)),
            dma((G - 1,) + kinds), dma((G - 1, arrivals)),
            dma((3,)), dma((T,)), dma((T,)), dma((T,)),
            dma((1,)), dma((1,)),
            dma((1,)), dma((4,)), dma((2,)), dma((2, 2 * ND + 3 if tuned else F * ND)),
            dma((H - 1,)), dma((H - 1,)),
            dma((H - 1,)), dma((H,)), dma((H,)),
        ],
        compiler_params=pltpu.CompilerParams(
            collective_id=0, has_side_effects=True, vmem_limit_bytes=63 * 1024 * 1024),
    )(tokens, gains, scale.reshape(1, PWt), mix_in, mix_out, up_w, down_w)


def solution(mesh):
    sizes = tuple(mesh.shape[name] for name in ("grp", "fs", "tp"))
    return jax.shard_map(
        functools.partial(local_layer, sizes),
        mesh=mesh,
        in_specs=(
            P(("grp", "fs", "tp"), None),
            P("fs", "tp"),
            P("tp"),
            P("tp", "fs"),
            P("fs", "tp"),
            P("tp", "fs"),
            P(),
        ),
        out_specs=P(("grp", "fs", "tp"), None),
        check_vma=False,
    )
```

```python
import functools

import jax
import jax.numpy as jnp
from jax import lax
from jax.experimental import pallas as pl
from jax.experimental.pallas import tpu as pltpu
from jax.sharding import PartitionSpec as P

GROUPS = 4
EPS = 1e-06
MESH = pl.DeviceIdType.MESH


def normalize(values, gain):
    upcast = values.astype(jnp.float32)
    return upcast * lax.rsqrt(jnp.mean(upcast * upcast, axis=-1, keepdims=True) + EPS) * gain


def pooling(mixed_in, first_channel, group_width):
    length, width = mixed_in.shape
    upcast = mixed_in.astype(jnp.float32)
    row = lax.broadcasted_iota(jnp.int32, (length, width), 0)
    group = (first_channel + lax.broadcasted_iota(jnp.int32, (length, width), 1)) // group_width
    position = (row + 1).astype(jnp.float32)
    total, average = upcast, jnp.zeros_like(upcast)
    for index in range(GROUPS):
        step = 1 << index
        total = total + jnp.where(row >= step, pltpu.roll(total, step, axis=0), 0.0)
        mean = total / jnp.minimum(position, float(2 * step))
        average = jnp.where(group == index, mean, average)
    return average - upcast


def kernel(dims, tok_h, gains_h, scale_h, mi_h, mo_h, up_h, dn_h, out,
           tok, gains, scale, mi, mo, up, dn, g1, g2, hid, sp1, rq1, rp1, sp2, rq2, rp2, mid,
           lsem, zs, zr, ys, yr, gs, g1r, g2r, g3r, es, er,
           w1s, w1r, w2s, w2r, p1s, p1r, p2s, p2r, p3s):
    G, F, T, R, D, K, PWt, Ht, NU, ND, NP = dims
    g, f, t = lax.axis_index("grp"), lax.axis_index("fs"), lax.axis_index("tp")
    cu, cd = Ht // NU, K // ND
    UD = 1 if ND % 2 else 2
    NB = ND // UD
    off = F >= 4
    tuned = F == 4 and NU == 4 and ND == 4
    far = F - 2 if off else F - 1
    first, last = (1, F - 2) if off else (0, F - 1)
    mid_plane = (f >= first) & (f <= last)
    end = (f < first) | (f > last)
    helper = (f == 1) | (f == F - 2) if off else f < 0
    helped = jnp.where(f == 1, 0, F - 1)
    inner = jnp.where(f == 0, 1, F - 2)
    sibling = t + 1 - 2 * lax.rem(t, 2)
    place, half_t = lax.rem(t, 2), T // 2
    step = D // 4

    def to_right_ok(w):
        return f + 1 < F if w in ("mi", "mo") else (f + 1 <= last)

    def to_left_ok(w):
        return f > 0 if w in ("mi", "mo") else (f - 1 >= first)

    def shared(w, s):
        return True if w in ("mi", "mo") or not off else ~(helper & (s == helped))
    NM = 1
    pieces = {"mi": (0, NM), "mo": (NM, 1), "up": (NM + 1, NU), "dn": (NM + 1 + NU, ND)}
    kinds = {"mi": 0, "mo": 0, "up": 1, "dn": 1}
    bufs = {"mi": (mi_h, mi), "mo": (mo_h, mo), "up": (up_h, up), "dn": (dn_h, dn)}

    def slot_of(s, where):
        return s - jnp.where(s > where, 1, 0)

    def zsem(side, kind, s):
        return zs.at[side, 0, 0] if tuned else zs.at[side, kind, s]

    def ysem(k, kind, s):
        return ys.at[k - 1, 0, 0] if tuned else ys.at[k - 1, kind, s]

    def yrsem(k, w, s, c, where):
        slot = slot_of(s, where)
        if not tuned:
            return yr.at[k - 1, slot * NP + pieces[w][0] + c]
        base = {"mi": 0, "mo": 1, "up": 2, "dn": 2 + NU + slot * ND}[w]
        return yr.at[k - 1, base + c]

    def mult(value, by):
        return pl.multiple_of(value, by)

    def span(w, s, c, half):
        base = s * K
        if w == "mi":
            size = K // G // NM
            return pl.ds(mult(base + (half * NM + c) * size, size), size), pl.ds(0, PWt)
        if w == "mo":
            return pl.ds(mult(half * (PWt // G), PWt // G), PWt // G), pl.ds(mult(base, 128), K)
        if w == "up":
            return pl.ds(mult(base + half * (K // G), K // G), K // G), pl.ds(mult(c * cu, cu), cu)
        return pl.ds(mult(half * (Ht // G), Ht // G), Ht // G), pl.ds(mult(base + c * cd, cd), cd)

    def view(w, s, c, half):
        return bufs[w][1].at[span(w, s, c, half)]

    def z_copy(w, s, c, to_right):
        p = pieces[w][0] + c
        target = f + 1 if to_right else f - 1
        side = 0 if to_right else 1
        return pltpu.make_async_remote_copy(
            src_ref=view(w, s, c, g), dst_ref=view(w, s, c, g), send_sem=zsem(side, kinds[w], s), recv_sem=zr.at[s - side, p],
            device_id=(g, target, t), device_id_type=MESH)

    def y_copy(w, s, c, k, half=None):
        half = g if half is None else half
        return pltpu.make_async_remote_copy(
            src_ref=view(w, s, c, half), dst_ref=view(w, s, c, half),
            send_sem=ysem(k, kinds[w], s), recv_sem=yrsem(k, w, s, c, f),
            device_id=(lax.rem(g + k, G), f, t), device_id_type=MESH)

    def send_own(w, c):
        @pl.when(to_right_ok(w))
        def _():
            z_copy(w, f, c, True).start()

        @pl.when(to_left_ok(w))
        def _():
            z_copy(w, f, c, False).start()

    def whole_copy(w, c, k):
        half = lax.rem(g - k + G, G)
        return pltpu.make_async_remote_copy(
            src_ref=view(w, f, c, half), dst_ref=view(w, f, c, half),
            send_sem=ysem(k, kinds[w], f), recv_sem=yrsem(k, w, f, c, inner),
            device_id=(g, inner, t), device_id_type=MESH)

    def send_whole(w):
        if off:
            order = list(range(pieces[w][1]))
            if tuned and w == "dn":
                order = order[:1:-1] + order[:2]

            @pl.when(end)
            def _():
                for c in order:
                    for k in range(1, G):
                        whole_copy(w, c, k).start()

    def pass_on(k):
        half = lax.rem(g - k + G, G)
        block = view("dn", helped, ND - 1, half)
        return pltpu.make_async_remote_copy(
            src_ref=block, dst_ref=block, send_sem=ysem(k, 1, helped), recv_sem=yrsem(k, "dn", helped, ND - 1, F - 1 - f),
            device_id=(g, F - 1 - f, t), device_id_type=MESH)

    def pump(w, d, c, kind=None):
        for to_right in (True, False):
            s = f - d if to_right else f + d
            more = to_right_ok(w) if to_right else to_left_ok(w)
            here = (s >= 0) & (s < F)
            if w in ("up", "dn"):
                here = here & mid_plane
            theirs = helper & (s == helped)
            if kind is not None:
                here = here & (theirs if kind == "relay" else ~theirs)
            spread = shared(w, s)
            if tuned and w == "dn" and c == ND - 1:
                spread = spread & (s > 0) & (s < F - 1)

            @pl.when(here)
            def _():
                z_copy(w, s, c, to_right).wait_recv()

                @pl.when(more)
                def _():
                    z_copy(w, s, c, to_right).start()

                @pl.when(spread)
                def _():
                    for k in range(1, G):
                        y_copy(w, s, c, k).start()

    def y_wait(w, s, c):
        for k in range(1, G):
            y_copy(w, s, c, k, lax.rem(g - k + G, G)).wait_recv()

    def y_wait_rows(w, c):
        size, cols = (F - 1) * (K // G), pl.ds(0, PWt)
        if w == "mo":
            size, cols = PWt // G, pl.ds(0, (F - 1) * K)
        if w == "up":
            cols = pl.ds(mult(c * cu, cu), cu)
        rows = bufs[w][1].at[pl.ds(0, size), cols]
        for k in range(1, G):
            pltpu.make_async_remote_copy(
                src_ref=rows, dst_ref=rows, send_sem=ysem(k, 0, 0), recv_sem=yrsem(k, w, 0, c, f),
                device_id=(lax.rem(g + k, G), f, t), device_id_type=MESH).wait_recv()

    def y_wait_all(w):
        if tuned:
            y_wait_rows(w, 0)
            return

        def body(i, _):
            s, c = i // pieces[w][1], lax.rem(i, pieces[w][1])

            @pl.when(s != f)
            def _():
                y_wait(w, s, c)
            return 0
        lax.fori_loop(0, F * pieces[w][1], body, 0)

    def local(w, index):
        cols, rows = pl.ds(mult(f * K, K), K), pl.ds(mult(f * K, K), K)
        dst = bufs[w][1].at[rows, :] if w in ("mi", "up") else bufs[w][1].at[:, cols]
        return pltpu.make_async_copy(bufs[w][0], dst, lsem.at[index])

    def peer(k):
        return lax.rem(t + k, T)

    def tp_copy(src, dst, send, recv, k):
        return pltpu.make_async_remote_copy(
            src_ref=src, dst_ref=dst, send_sem=send, recv_sem=recv,
            device_id=(g, f, peer(k)), device_id_type=MESH)

    def gather_copy(buf, sems, block, target):
        return pltpu.make_async_remote_copy(
            src_ref=buf.at[block], dst_ref=buf.at[block], send_sem=gs.at[sems[0]],
            recv_sem=sems[1].at[block], device_id=(g, f, target), device_id_type=MESH)

    def gather_start(buf, sems):
        for k in range(2, T, 2):
            gather_copy(buf, sems, t, peer(k)).start()
        gather_copy(buf, sems, t, sibling).start()

    def gather_finish(buf, sems):
        for k in range(2, T, 2):
            block = lax.rem(t - k + T, T)
            gather_copy(buf, sems, block, sibling).wait_recv()
            gather_copy(buf, sems, block, sibling).start()
        for k in range(0, T, 2):
            block = lax.rem(sibling - k + T, T)
            gather_copy(buf, sems, block, sibling).wait_recv()

    def gather_drain(buf, sems):
        sent = buf.at[pl.ds(0, T - 1)]
        pltpu.make_async_remote_copy(
            src_ref=sent, dst_ref=sent, send_sem=gs.at[sems[0]], recv_sem=sems[1].at[0],
            device_id=(g, f, sibling), device_id_type=MESH).wait_send()

    own_rows, end_rows = g2.at[0], g2.at[1]
    sems1, sems2, sems3 = (0, g1r), (1, g2r), (2, g3r)

    def end_copy():
        return pltpu.make_async_remote_copy(
            src_ref=g2.at[0, t], dst_ref=g2.at[1, t], send_sem=es.at[0], recv_sem=er.at[0],
            device_id=(g, inner, t), device_id_type=MESH)

    def swap1(j):
        cols = pl.ds(j * step, step)
        return pltpu.make_async_remote_copy(
            src_ref=sp1.at[1 - place, :, :, cols], dst_ref=rq1.at[:, :, cols],
            send_sem=w1s.at[0], recv_sem=w1r.at[j], device_id=(g, f, sibling), device_id_type=MESH)

    def part1(k):
        return tp_copy(sp1.at[place, peer(k) // 2], rp1.at[k // 2 - 1],
                       p1s.at[k // 2 - 1], p1r.at[k // 2 - 1], k)

    def columns(s, c, n):
        return pl.ds(mult(s * K + c * cd, cd), n * cd)

    def swap_index(s, c):
        if not tuned:
            return s * ND + c
        base = jnp.where(s == f, 2 * ND - 1, 2 * ND + 1) + c // 2
        return jnp.where(s == helped, c, jnp.where(s == F - 1 - helped, ND - 1 + c, base))

    def swap2(i, s, c, n):
        return pltpu.make_async_remote_copy(
            src_ref=sp2.at[i, 1 - place, :, :, columns(s, c, n)], dst_ref=rq2.at[i, :, :, columns(s, c, n)],
            send_sem=w2s.at[i], recv_sem=w2r.at[i, swap_index(s, c)],
            device_id=(g, f, sibling), device_id_type=MESH)

    def part2(s, c, n, k):
        return tp_copy(sp2.at[0, place, peer(k) // 2, :, columns(s, c, n)], rp2.at[k // 2, :, columns(s, c, n)],
                       p2s.at[k // 2 - 1], p2r.at[k // 2], k)

    def part3(s, c, n, k):
        return pltpu.make_async_remote_copy(
            src_ref=sp2.at[1, place, peer(k) // 2, :, columns(s, c, n)], dst_ref=rp2.at[k // 2, :, columns(s, c, n)],
            send_sem=p3s.at[k // 2], recv_sem=p2r.at[k // 2],
            device_id=(g, helped, peer(k)), device_id_type=MESH)

    def merge(a, b):
        return (a.astype(jnp.float32) + b.astype(jnp.float32)).astype(jnp.bfloat16)

    loads = [pltpu.make_async_copy(a, b, lsem.at[4 + i])
             for i, (a, b) in enumerate(((tok_h, tok), (gains_h, gains), (scale_h, scale)))]
    local("mi", 0).start()
    local("mo", 1).start()
    for load in loads:
        load.start()
    local("up", 2).start()
    local("dn", 3).start()

    barrier = pltpu.get_barrier_semaphore()

    @pl.when(f + 1 < F)
    def _():
        pl.semaphore_signal(barrier, inc=1, device_id=(g, f + 1, t), device_id_type=MESH)

    @pl.when(f > 0)
    def _():
        pl.semaphore_signal(barrier, inc=1, device_id=(g, f - 1, t), device_id_type=MESH)

    for k in range(1, G):
        pl.semaphore_signal(barrier, inc=1, device_id=(lax.rem(g + k, G), f, t), device_id_type=MESH)
    for k in range(1, T):
        pl.semaphore_signal(barrier, inc=1, device_id=(g, f, peer(k)), device_id_type=MESH)
    greeted = jnp.where(f + 1 < F, 1, 0) + jnp.where(f > 0, 1, 0) + (G - 1 + T - 1)
    pl.semaphore_wait(barrier, greeted)

    local("mi", 0).wait()
    for c in range(NM):
        send_own("mi", c)
    local("mo", 1).wait()
    send_own("mo", 0)
    local("up", 2).wait()
    send_own("up", 0)

    @pl.when(~mid_plane)
    def _():
        for c in range(1, NU):
            send_own("up", c)
    send_whole("up")
    for load in loads:
        load.wait()
    g1[t] = normalize(tok[...], gains[0:1, :]).astype(jnp.bfloat16)
    gather_start(g1, sems1)
    local("dn", 3).wait()

    for d in range(1, F):
        for kind in ("near", "relay"):
            if kind == "near" or (off and d == 1):
                for c in range(NM):
                    pump("mi", d, c, kind)
                pump("mo", d, 0, kind)
        if d < NU:
            @pl.when(mid_plane)
            def _():
                send_own("up", d)
        if tuned and d == 1:
            pump("up", 1, 0, "near")

    @pl.when(mid_plane)
    def _():
        for c in range(F, NU):
            send_own("up", c)

    for c in range(NU // 2):
        pump("up", 1, c, "relay" if tuned and c == 0 else None)

    y_wait_all("mi")
    gather_finish(g1, sems1)
    mixed_in = jnp.dot(g1[...].reshape(T * R, D), mi[...],
                       preferred_element_type=jnp.float32).astype(jnp.bfloat16)
    scaled = (pooling(mixed_in, t * PWt, PWt * T // GROUPS) * scale[...]).astype(jnp.bfloat16)
    y_wait_all("mo")
    if tuned:
        pump("up", 1, NU // 2)
    for j in range(4):
        cols = pl.ds(j * step, step)
        value = jnp.dot(scaled, mo[:, cols], preferred_element_type=jnp.float32
                        ).astype(jnp.bfloat16).reshape(half_t, 2, R, step)
        for q in range(2):
            sp1[q, :, :, cols] = value[:, q]
        swap1(j).start()
    for j in range(4):
        cols = pl.ds(j * step, step)
        swap1(j).wait_recv()
        sp1[place, :, :, cols] = merge(sp1[place, :, :, cols], rq1[:, :, cols])
    for k in range(2, T, 2):
        part1(k).start()

    def pump_all(w, d, start=0):
        def body(c, _):
            pump(w, d, c)
            return 0
        lax.fori_loop(start, pieces[w][1], body, 0)

    pump_all("up", 1, NU // 2 + 1 if tuned else NU // 2)
    if tuned:
        pump("up", far, 0)
    early = far <= 2

    @pl.when(mid_plane & early)
    def _():
        for c in range(ND):
            send_own("dn", c)

    total = sp1[place, t // 2].astype(jnp.float32)
    for k in range(2, T, 2):
        part1(k).wait_recv()
        total = total + rp1[k // 2 - 1].astype(jnp.float32)
    mixer_out = total.astype(jnp.bfloat16)
    middle = (tok[...].astype(jnp.float32) + normalize(mixer_out, gains[1:2, :])).astype(jnp.bfloat16)
    mid[...] = middle
    g2[0, t] = normalize(middle, gains[2:3, :]).astype(jnp.bfloat16)

    @pl.when(mid_plane)
    def _():
        gather_start(own_rows, sems2)
    if off:
        @pl.when(end)
        def _():
            end_copy().start()

    def pump_mid(d, _):
        pump_all("up", d)
        return 0
    lax.fori_loop(2, far, pump_mid, 0)

    @pl.when(~(mid_plane & early))
    def _():
        for c in range(ND):
            send_own("dn", c)
    send_whole("dn")
    if far > 1:
        pump_all("up", far, 1 if tuned else 0)

    def up_project(i, c):
        cols = pl.ds(mult(c * cu, cu), cu)
        pre = jnp.dot(g2[i].reshape(T * R, D), up[:, cols], preferred_element_type=jnp.float32)
        pre = jnp.maximum(pre, 0.0)
        hid[i, :, cols] = (pre * pre).astype(jnp.bfloat16)

    half_u, half_d = NU // 2, (ND + 1) // 2
    turn = max(half_u - 1, 0)
    soon = [c for c in range(half_d) if half_u + c < NU]
    if off and half_d < ND:
        soon.append(half_d)
    later = [c for c in range(ND) if c not in soon]

    def act(todo):
        for what, d, c in todo:
            if what == "pass":
                y_wait("dn", helped, ND - 1)
                for k in range(1, G):
                    pass_on(k).start()
            else:
                pump("dn", d, c, what)

    up_acts = {2: [("near", 1, 0)], 3: [("near", 1, 1), ("relay", 1, 0), ("near", 1, 2)], 5: [("relay", 1, 1)],
               6: [("near", 1, 3)], 7: [("relay", 1, 2)]}

    def scheduled(acts, n):
        for index, todo in acts.items():
            @pl.when(n == index)
            def _():
                act(todo)

    def up_step(j, _):
        i, c = j // NU, lax.rem(j, NU)

        @pl.when(i == 0)
        def _():
            if tuned:
                y_wait_rows("up", c)
                return

            def landed_rows(s, _):
                @pl.when(s != f)
                def _():
                    y_wait("up", s, c)
                return 0
            lax.fori_loop(0, F, landed_rows, 0)
        if off:
            @pl.when(helper & (i == 1) & (c == 0))
            def _():
                gather_finish(end_rows, sems3)

        @pl.when((i == 0) | helper)
        def _():
            up_project(i, c)
        if off:
            @pl.when(helper & (i == 0) & (c == turn))
            def _():
                end_copy().wait_recv()
                gather_start(end_rows, sems3)
        if tuned:
            scheduled(up_acts, j)
            return 0
        first_pass = (i == 0) & (c >= half_u) & (c - half_u < half_d)
        second_pass = (i == 1) & (c == turn) & (half_d < ND)

        @pl.when(first_pass | second_pass)
        def _():
            pump("dn", 1, jnp.where(i == 0, c - half_u, half_d))
        return 0

    def project(i, s, first, n):
        cols = columns(s, first, n)
        value = jnp.dot(hid[i], dn[:, cols], preferred_element_type=jnp.float32
                        ).astype(jnp.bfloat16).reshape(half_t, 2, R, n * cd)
        for q in range(2):
            sp2[i, q, :, :, cols] = value[:, q]
        swap2(i, s, first, n).start()

    def finish(i, s, first, n):
        cols = columns(s, first, n)
        swap2(i, s, first, n).wait_recv()
        sp2[i, place, :, :, cols] = merge(sp2[i, place, :, :, cols], rq2[i, :, :, cols])

        @pl.when(i == 0)
        def _():
            for k in range(2, T, 2):
                part2(s, first, n, k).start()
        if off:
            @pl.when(i == 1)
            def _():
                for chip in range(half_t):
                    part3(s, first, n, lax.rem(2 * chip + place - t + T, T)).start()

    OWN, NEAR, HELPED, FAR = range(4)
    codes, before = [], {}

    def queue(kind, who, c, n, rows=(1, 0), wait=True):
        for i in rows:
            fresh = kind == 0 and wait and who != OWN and i == rows[0]
            codes.append(kind + 2 * (n - 1) + 4 * i + 8 * fresh + 16 * who + 64 * c)

    def also(*todo):
        before.setdefault(len(codes), []).extend(todo)

    if tuned:
        queue(0, OWN, 0, 2)
        queue(0, OWN, 2, 2)
        queue(1, OWN, 0, 2)
        also(("near", 2, 0), ("relay", 1, 3))
        queue(1, OWN, 2, 2)
        queue(0, NEAR, 0, 2)
        also(("near", 2, 1))
        queue(1, NEAR, 0, 2)
        queue(0, NEAR, 2, 2)
        also(("pass", 0, 0))
        queue(1, NEAR, 2, 2)
        also(("near", 2, 2))
        queue(0, HELPED, 2, 2)
        queue(0, FAR, 0, 1)
        queue(1, HELPED, 2, 2)
        queue(1, FAR, 0, 1)
        queue(0, FAR, 1, 1, (1,))
        also(("near", 2, 3))
        queue(0, HELPED, 0, 1, (1,))
        queue(0, FAR, 1, 1, (0,), False)
        queue(1, FAR, 1, 1, (1,))
        queue(0, HELPED, 0, 1, (0,), False)
        queue(1, HELPED, 0, 1, (1,))
        queue(1, FAR, 1, 1, (0,))
        tails = []
        split = len(codes)
        for second in (False, True):
            if second:
                queue(0, HELPED, 1, 1, (1,))
                queue(0, FAR, 2, 2, (1,))
                queue(1, HELPED, 1, 1, (1,))
                queue(0, HELPED, 1, 1, (0,), False)
                queue(1, FAR, 2, 2, (1,))
                queue(0, FAR, 2, 2, (0,), False)
                queue(1, HELPED, 0, 1, (0,))
                queue(1, HELPED, 1, 1, (0,))
                queue(1, FAR, 2, 2, (0,))
            else:
                queue(0, HELPED, 1, 1, (1,))
                queue(0, FAR, 2, 2, (1,))
                queue(1, HELPED, 1, 1, (1,))
                queue(0, HELPED, 1, 1, (0,), False)
                queue(1, FAR, 2, 2, (1,))
                queue(0, FAR, 2, 2, (0,), False)
                queue(1, HELPED, 0, 1, (0,))
                queue(1, HELPED, 1, 1, (0,))
                queue(1, FAR, 2, 2, (0,))
            tails.append(codes[split:])
            del codes[split:]

    def choose(n, values):
        out = jnp.int32(values[0])
        for index, value in enumerate(values[1:]):
            out = jnp.where(n == index + 1, value, out)
        return out

    def dn_op(n, _):
        scheduled(before, n)
        code = jnp.where(place == 0, choose(n, codes + tails[0]), choose(n, codes + tails[1]))
        kind, size, i = lax.rem(code, 2), lax.rem(code // 2, 2) + 1, lax.rem(code // 4, 2)
        fresh, who, first = lax.rem(code // 8, 2), lax.rem(code // 16, 4), code // 64
        s = jnp.where(who == OWN, f, jnp.where(who == NEAR, F - 1 - f, jnp.where(who == HELPED, helped, F - 1 - helped)))
        for c in range(2):
            passed = (who == HELPED) & (first + c == ND - 1)

            @pl.when((fresh == 1) & (c < size) & ~passed)
            def _():
                y_wait("dn", s, first + c)

        for width in (1, 2):
            @pl.when((kind == 0) & (size == width))
            def _():
                project(i, s, first, width)

            @pl.when((kind == 1) & (size == width))
            def _():
                finish(i, s, first, width)
        return 0

    slots = (far + 1) * NB

    def dn_step(n, _):
        def one(now, _):
            m = n - 1 + now
            slot, q = m // 2, lax.rem(m, 2)
            d, first = slot // NB, lax.rem(slot, NB) * UD
            last = helper & (d == far)
            s = jnp.where(q == 0, f - d, f + d)
            s = jnp.where(last, jnp.where(q == 0, F - 1 - helped, helped), s)
            wanted = ((m >= 0) & (slot < slots) & (s >= 0) & (s < F) & ((q == 0) | (d > 0))
                      & (last | ~(helper & (s == helped))))

            @pl.when(wanted & (now == 1) & (s != f))
            def _():
                for c in range(UD):
                    y_wait("dn", s, first + c)

            def rows(i, _):
                @pl.when(wanted & (now == 0))
                def _():
                    finish(i, s, first, UD)

                @pl.when(wanted & (now == 1))
                def _():
                    project(i, s, first, UD)
                return 0
            lax.fori_loop(0, jnp.where(helper, 2, 1), rows, 0)
            return 0
        lax.fori_loop(0, 2, one, 0)
        slot = n // 2

        @pl.when(n == 2 * NB - 1)
        def _():
            for c in later:
                pump("dn", 1, c)

        @pl.when((lax.rem(n, 2) == 1) & (slot >= NB) & (slot < far * NB))
        def _():
            for c in range(UD):
                pump("dn", slot // NB + 1, lax.rem(slot, NB) * UD + c)
        return 0

    @pl.when(mid_plane)
    def _():
        gather_finish(own_rows, sems2)
        lax.fori_loop(0, (2 if off else 1) * NU, up_step, 0)
        if tuned:
            lax.fori_loop(0, len(codes + tails[0]), dn_op, 0)
        else:
            lax.fori_loop(0, 2 * slots + 1, dn_step, 0)

    def landed(k):
        return tp_copy(rp2.at[k // 2], rp2.at[k // 2], p2s.at[0], p2r.at[k // 2], 2)

    for k in range(2, T, 2):
        landed(k).wait_recv()
    if off:
        @pl.when(end)
        def _():
            landed(0).wait_recv()

    @pl.when(mid_plane)
    def _():
        rp2[0] = sp2[0, place, t // 2]
    total = jnp.zeros((R, D), jnp.float32)
    for k in range(half_t):
        total = total + rp2[k].astype(jnp.float32)
    channel_out = total.astype(jnp.bfloat16)
    out[...] = (mid[...].astype(jnp.float32) + normalize(channel_out, gains[3:4, :])).astype(jnp.bfloat16)

    def sent(kind, sem):
        rows = (mi if kind == 0 else up).at[pl.ds(0, 2 * (K // G)), :]
        pltpu.make_async_remote_copy(
            src_ref=rows, dst_ref=rows, send_sem=sem, recv_sem=zr.at[0, 0],
            device_id=(g, f, sibling), device_id_type=MESH).wait_send()

    def swapped(buf, sem):
        pltpu.make_async_remote_copy(
            src_ref=buf, dst_ref=buf, send_sem=sem, recv_sem=w1r.at[0],
            device_id=(g, f, sibling), device_id_type=MESH).wait_send()

    if tuned:
        large = 2 * (K // G)
        small = large * PWt // Ht

        def gone(amount, sem):
            swapped(up.at[pl.ds(0, amount[0] * small + amount[1] * large), :], sem)

        for side, plans in enumerate((((0, (1, 1)), (1, (2, 2)), (2, (3, 0))), ((3, (1, 1)), (2, (2, 2)), (1, (3, 0))))):
            for place_f, amount in plans:
                @pl.when(f == place_f)
                def _():
                    gone(amount, zsem(side, 0, 0))
        for k in range(1, G):
            @pl.when(mid_plane)
            def _():
                gone((3, 2), ysem(k, 0, 0))

            @pl.when(end)
            def _():
                gone((3, 1), ysem(k, 0, 0))

    for kind, w in () if tuned else ((0, "mi"), (1, "up")):
        def drain(s, _):
            moved = True if kind == 0 else (mid_plane | (s == f))

            @pl.when((s <= f) & to_right_ok(w) & moved)
            def _():
                sent(kind, zs.at[0, kind, s])

            @pl.when((s >= f) & to_left_ok(w) & moved)
            def _():
                sent(kind, zs.at[1, kind, s])

            @pl.when((s != f) & moved & shared(w, s))
            def _():
                for k in range(1, G):
                    sent(kind, ys.at[k - 1, kind, s])
            if off and kind == 1:
                @pl.when((s == f) & end)
                def _():
                    for k in range(1, G):
                        sent(kind, ys.at[k - 1, kind, s])
            return 0
        lax.fori_loop(0, F, drain, 0)

    @pl.when(mid_plane)
    def _():
        swapped(rq2.at[0], w2s.at[0])
        for k in range(2, T, 2):
            swapped(rp2.at[0], p2s.at[k // 2 - 1])
        gather_drain(own_rows, sems2)
        if off:
            @pl.when(helper)
            def _():
                gather_drain(end_rows, sems3)
                swapped(rq2.at[1], w2s.at[1])
                for k in range(0, T, 2):
                    swapped(rp2.at[0], p3s.at[k // 2])
    if off:
        @pl.when(end)
        def _():
            end_copy().wait_send()
    gather_drain(g1, sems1)
    swapped(rq1, w1s.at[0])
    for k in range(2, T, 2):
        part1(k).wait_send()


def local_layer(sizes, tokens, mix_in, scale, mix_out, up_w, down_w, gains):
    G, F, T = sizes
    R, D = tokens.shape
    K, PWt = mix_in.shape
    Ht = up_w.shape[1]
    NU = max(1, min(4, Ht // 256))
    ND = max(1, min(4, K // 128))
    NP = 2 + NU + ND
    dims = (G, F, T, R, D, K, PWt, Ht, NU, ND, NP)
    tuned = F == 4 and NU == 4 and ND == 4
    kinds, arrivals = (1, 1) if tuned else (2, F), 2 + NU + (F - 1) * ND if tuned else (F - 1) * NP
    H = T // 2
    vmem, hbm = pl.BlockSpec(memory_space=pltpu.VMEM), pl.BlockSpec(memory_space=pl.ANY)
    bf, dma = jnp.bfloat16, pltpu.SemaphoreType.DMA
    return pl.pallas_call(
        functools.partial(kernel, dims),
        out_shape=pltpu.VMEM((R, D), bf),
        in_specs=[hbm] * 7,
        out_specs=vmem,
        scratch_shapes=[
            pltpu.VMEM((R, D), bf), pltpu.VMEM(gains.shape, jnp.float32), pltpu.VMEM((1, PWt), jnp.float32),
            pltpu.VMEM((D, PWt), bf), pltpu.VMEM((PWt, D), bf),
            pltpu.VMEM((D, Ht), bf), pltpu.VMEM((Ht, D), bf),
            pltpu.VMEM((T, R, D), bf), pltpu.VMEM((2, T, R, D), bf),
            pltpu.VMEM((2, T * R, Ht), bf),
            pltpu.VMEM((2, H, R, D), bf), pltpu.VMEM((H, R, D), bf), pltpu.VMEM((H - 1, R, D), bf),
            pltpu.VMEM((2, 2, H, R, D), bf), pltpu.VMEM((2, H, R, D), bf), pltpu.VMEM((H, R, D), bf),
            pltpu.VMEM((R, D), bf),
            dma((7,)), dma((2,) + kinds), dma((F - 1, NP)),
            dma((G - 1,) + kinds), dma((G - 1, arrivals)),
            dma((3,)), dma((T,)), dma((T,)), dma((T,)),
            dma((1,)), dma((1,)),
            dma((1,)), dma((4,)), dma((2,)), dma((2, 2 * ND + 3 if tuned else F * ND)),
            dma((H - 1,)), dma((H - 1,)),
            dma((H - 1,)), dma((H,)), dma((H,)),
        ],
        compiler_params=pltpu.CompilerParams(
            collective_id=0, has_side_effects=True, vmem_limit_bytes=63 * 1024 * 1024),
    )(tokens, gains, scale.reshape(1, PWt), mix_in, mix_out, up_w, down_w)


def solution(mesh):
    sizes = tuple(mesh.shape[name] for name in ("grp", "fs", "tp"))
    return jax.shard_map(
        functools.partial(local_layer, sizes),
        mesh=mesh,
        in_specs=(
            P(("grp", "fs", "tp"), None),
            P("fs", "tp"),
            P("tp"),
            P("tp", "fs"),
            P("fs", "tp"),
            P("tp", "fs"),
            P(),
        ),
        out_specs=P(("grp", "fs", "tp"), None),
        check_vma=False,
    )
```
